128 devices in a mesh: sp: 16 (over z, y), tp: 8 (over x, core).
Axes of the slice: x: 4, y: 4, z: 4, core: 2. Of those that a mesh axis runs over, the one named last changes fastest.
Arguments:
- hidden: bfloat16 [16, 1024, 1024], P(None, 'sp'), may hold values from -0.09375 to 0.09375
- value_weight: bfloat16 [1024, 1024], P(None, 'tp'), may hold values from -0.75 to 0.75
- queries: bfloat16 [16, 8, 1024, 64], P(None, 'tp', 'sp'), may hold values from -0.1875 to 0.1875
- key_vectors: bfloat16 [16, 8, 1024, 64], P(None, 'tp', 'sp'), may hold values from -0.1875 to 0.1875
- forward_decay: float32 [16, 8, 1024, 64], P(None, 'tp', 'sp'), may hold values from -0.0029296875 to -9.765625e-06
- backward_decay: float32 [16, 8, 1024, 64], P(None, 'tp', 'sp'), may hold values from -0.0029296875 to -9.765625e-06
- cotangent: bfloat16 [16, 1024, 1024], P(None, 'sp', 'tp'), may hold values from -6 to 6
Outputs:
- grad_queries: bfloat16 [16, 8, 1024, 64], P(None, 'tp', 'sp')
- grad_keys: bfloat16 [16, 8, 1024, 64], P(None, 'tp', 'sp')
- grad_forward: float32 [16, 8, 1024, 64], P(None, 'tp', 'sp')
- grad_backward: float32 [16, 8, 1024, 64], P(None, 'tp', 'sp')
- grad_hidden: bfloat16 [16, 1024, 1024], P(None, 'sp', 'tp')
- grad_weight: float32 [1024, 1024], P('sp', 'tp')
The draws below stay inside these ranges and needn't reach their ends.
All inputs are finite; a program needn't handle non-finite values.
Results may differ from the reference program's by a relative error of at most 0.015.
Values may be sent and summed in bfloat16 or wider, within the bound.
A program may use at most 128 MiB of HBM per device.

```python
import jax
import jax.numpy as jnp
from jax import lax

D = 1024
HEADS = 8
DK = 64
DV = 128
BATCH = 16
TOK_DEV = 64
TOKENS = 1024


def steps_of(rng, shape, cuts, smallest, high):
    level, own = 1.0, jax.random.fold_in(rng, 6)
    for axis_at, parts in cuts:
        heights = jnp.exp(jax.random.uniform(jax.random.fold_in(own, axis_at), (parts,), jnp.float32, smallest / len(cuts), high / len(cuts)))
        level = level * jnp.repeat(heights, shape[axis_at] // parts).reshape([-1 if axis == axis_at else 1 for axis in range(len(shape))])
    return level


def normal_values(key, dims, spread, reach, split=(), kind=jnp.bfloat16):
    values = jax.random.normal(key, dims, jnp.float32) * spread
    if len(split) > 0:
        values = steps_of(key, dims, split, -0.22, 0.18) * values
    return jnp.clip(values, min=-reach, max=reach).astype(kind)


def setup_inputs(seed: int = 0) -> dict:
    keys = jax.random.split(jax.random.key(seed), 8)
    hidden = normal_values(keys[0], (BATCH, TOKENS, D), 0.016, 0.09375, ((1, 16),))
    value_weight = normal_values(keys[1], (D, HEADS * DV), (D // 16) ** -0.5, 0.75, ((1, 8),))
    queries = normal_values(keys[2], (BATCH, HEADS, TOKENS, DK), 0.03, 0.1875, ((1, 8), (2, 16)))
    key_vectors = normal_values(keys[3], (BATCH, HEADS, TOKENS, DK), 0.03, 0.1875, ((1, 8), (2, 16)))
    forward_decay = jnp.clip(-0.0029296875 + 0.002919922 * jax.random.uniform(keys[4], (BATCH, HEADS, TOKENS, DK), jnp.float32) ** steps_of(keys[4], (BATCH, HEADS, TOKENS, DK), ((1, 8), (2, 16)), -0.2, 0.2), -0.0029296875, -9.765624781721272e-06)
    backward_decay = jnp.clip(-0.0029296875 + 0.002919922 * jax.random.uniform(keys[5], (BATCH, HEADS, TOKENS, DK), jnp.float32) ** steps_of(keys[5], (BATCH, HEADS, TOKENS, DK), ((1, 8), (2, 16)), -0.2, 0.2), -0.0029296875, -9.765624781721272e-06)
    cotangent = normal_values(keys[6], (BATCH, TOKENS, HEADS * DV), 1.0, 6.0, ((1, 16), (2, 8)))
    return dict(hidden=hidden, value_weight=value_weight, queries=queries, key_vectors=key_vectors, forward_decay=forward_decay, backward_decay=backward_decay, cotangent=cotangent)


EXACT_DOTS = lax.Precision.HIGHEST


def rounded(tensor):
    return lax.optimization_barrier(tensor.astype(jnp.bfloat16)).astype(jnp.float32)


def elements(query_heads, key_heads, value_heads, decay_heads, seed_heads):
    cumulative = jnp.cumsum(decay_heads, axis=2)
    final_sum = cumulative[:, :, -1, :]
    to_end = jnp.exp(final_sum[:, :, None, :] - cumulative)
    factor = jnp.exp(final_sum)
    state_part = jnp.einsum('bhjd,bhje->bhde', key_heads * to_end, value_heads, precision=EXACT_DOTS)
    grad_part = jnp.einsum('bhcd,bhce->bhde', query_heads * jnp.exp(cumulative), seed_heads, precision=EXACT_DOTS)
    return factor, state_part, grad_part


def block_grads(query_part, key_part, value_part, decay_part, seed_part, state_in, grad_in):
    length = query_part.shape[1]
    value_real = value_part.astype(jnp.float32)
    seed_real = seed_part.astype(jnp.float32)
    cumulative = jnp.cumsum(decay_part, axis=1)
    final_sum = cumulative[:, -1, :]
    growth = jnp.exp(cumulative)
    shrink = jnp.exp(-cumulative)
    to_end = jnp.exp(final_sum[:, None, :] - cumulative)
    query_hat = rounded(query_part * growth)
    key_hat = rounded(key_part * shrink)
    below_mask = jnp.tril(jnp.ones((length, length), dtype=bool))[None]
    scores = rounded(jnp.where(below_mask, jnp.einsum('hid,hjd->hij', query_hat, key_hat, precision=EXACT_DOTS), 0.0))
    seed_scores = rounded(jnp.where(below_mask, jnp.einsum('hie,hje->hij', seed_real, value_real, precision=EXACT_DOTS), 0.0))
    grad_query = growth * (jnp.einsum('hij,hjd->hid', seed_scores, key_hat, precision=EXACT_DOTS)
                           + jnp.einsum('hce,hde->hcd', seed_real, state_in, precision=EXACT_DOTS))
    grad_key = shrink * jnp.einsum('hij,hid->hjd', seed_scores, query_hat, precision=EXACT_DOTS)
    grad_key = grad_key + to_end * jnp.einsum('hde,hje->hjd', grad_in, value_real, precision=EXACT_DOTS)
    grad_value = jnp.einsum('hij,hie->hje', scores, seed_real, precision=EXACT_DOTS)
    grad_value = grad_value + jnp.einsum('hjd,hde->hje', key_part * to_end, grad_in, precision=EXACT_DOTS)
    grad_cumul = query_part * grad_query - key_part * grad_key
    return grad_query, grad_key, grad_value, grad_cumul


def direction(query_seq, key_seq, value_seq, decay_seq, seed_seq):
    head_count, length, key_width = query_seq.shape
    value_width = value_seq.shape[2]
    block_count = length // TOK_DEV

    def to_blocks(tensor):
        return tensor.reshape(head_count, block_count, TOK_DEV, tensor.shape[2]).transpose(1, 0, 2, 3)

    def from_blocks(tensor):
        return tensor.transpose(1, 0, 2, 3).reshape(head_count, length, tensor.shape[3])

    query_blocks, key_blocks = to_blocks(query_seq), to_blocks(key_seq)
    value_blocks, decay_blocks, seed_blocks = to_blocks(value_seq), to_blocks(decay_seq), to_blocks(seed_seq)
    factor, state_part, grad_part = elements(query_blocks, key_blocks, value_blocks.astype(jnp.float32),
                                             decay_blocks, seed_blocks.astype(jnp.float32))

    def advance(carried, pieces):
        return pieces[0][:, :, None] * carried + pieces[1], carried

    zero_state = jnp.zeros((head_count, key_width, value_width), jnp.float32)
    _, state_in = lax.scan(advance, zero_state, (factor, state_part))
    _, grad_in = lax.scan(advance, zero_state, (factor, grad_part), reverse=True)
    results = lax.map(lambda pieces: block_grads(*pieces),
                      (query_blocks, key_blocks, value_blocks, decay_blocks, seed_blocks, state_in, grad_in))
    return tuple(from_blocks(result) for result in results)


def reverse_tokens(tensor):
    return jnp.flip(tensor, axis=1)


def reference(hidden, value_weight, queries, key_vectors, forward_decay, backward_decay, cotangent):
    hidden_rows = hidden.reshape(BATCH * TOKENS, D)
    values_flat = jnp.dot(hidden_rows, value_weight, preferred_element_type=jnp.float32).astype(jnp.bfloat16)
    value_heads = values_flat.reshape(BATCH, TOKENS, HEADS, DV).transpose(0, 2, 1, 3)
    seed_heads = cotangent.reshape(BATCH, TOKENS, HEADS, DV).transpose(0, 2, 1, 3)

    def per_sequence(inputs):
        query_seq, key_seq, value_seq, ahead_decay, behind_decay, seed_seq = inputs
        ahead = direction(query_seq, key_seq, value_seq, ahead_decay, seed_seq)
        behind = direction(reverse_tokens(query_seq), reverse_tokens(key_seq), reverse_tokens(value_seq),
                           reverse_tokens(behind_decay), reverse_tokens(seed_seq))
        cumul_ahead = ahead[3]
        cumul_behind = reverse_tokens(behind[3])
        grad_ahead = -(jnp.cumsum(cumul_ahead, axis=1) - cumul_ahead)
        grad_behind = jnp.cumsum(cumul_behind, axis=1)
        return (ahead[0] + reverse_tokens(behind[0]), ahead[1] + reverse_tokens(behind[1]),
                ahead[2] + reverse_tokens(behind[2]), grad_ahead, grad_behind)

    grad_query, grad_key, grad_value, grad_ahead, grad_behind = lax.map(
        per_sequence, (queries.astype(jnp.float32), key_vectors.astype(jnp.float32), value_heads,
                       forward_decay, backward_decay, seed_heads))
    value_rows = grad_value.transpose(0, 2, 1, 3).reshape(BATCH * TOKENS, HEADS * DV).astype(jnp.bfloat16)
    grad_hidden = lax.dot_general(value_rows, value_weight, (((1,), (1,)), ((), ())),
                                  preferred_element_type=jnp.float32).astype(jnp.bfloat16).reshape(BATCH, TOKENS, D)
    grad_weight = lax.dot_general(hidden_rows, value_rows, (((0,), (0,)), ((), ())),
                                  preferred_element_type=jnp.float32)
    return (grad_query.astype(jnp.bfloat16), grad_key.astype(jnp.bfloat16), grad_ahead, grad_behind,
            grad_hidden, grad_weight)
```

```python
import functools

import jax
import jax.numpy as jnp
from jax import lax
from jax.experimental import pallas as pl
from jax.experimental.pallas import tpu as pltpu
from jax.sharding import PartitionSpec as P

F32, BF16 = jnp.float32, jnp.bfloat16
MESH = pl.DeviceIdType.MESH
LAG = 2
EXTRA = 4


def dot(a, b, ca=1, cb=0):
    return lax.dot_general(a, b, (((ca,), (cb,)), ((), ())), preferred_element_type=F32)


def split(x):
    high = x.astype(BF16)
    return high, (x - high.astype(F32)).astype(BF16)


def plan(sp, batch, heads):
    outer = 4 if sp % 4 == 0 and batch % (sp // 4) == 0 else sp
    inner = sp // outer
    own = batch // inner
    return outer, inner, own, own * heads


def kernel(dims, hid, wgt, qry, key, fdec, bdec, cot,
           o_q, o_k, o_f, o_b, o_h, o_w,
           val, cum, intra_q, intra_k, intra_v,
           a_out, a_in, b_out, b_in, c_out, c_in, d_all, w_in, g_out, g_in,
           a_ss, a_rs, b_ss, b_rs, c_ss, c_rs, d_ss, d_rs, w_ss, w_rs, g_ss, g_rs):
    sp, tp, batch, heads, length, dk, dv, width = dims
    outer, inner, own, units = plan(sp, batch, heads)
    pack = 2 * dk
    feat = width // tp
    rows_sp = width // sp
    group = d_group(own)
    spi, tpi = lax.axis_index("sp"), lax.axis_index("tp")
    z, y = spi // inner, lax.rem(spi, inner)

    barrier = pltpu.get_barrier_semaphore()
    for r in range(1, sp):
        pl.semaphore_signal(barrier, inc=1, device_id={"sp": lax.rem(spi + r, sp)}, device_id_type=MESH)
    for r in range(1, tp):
        pl.semaphore_signal(barrier, inc=1, device_id={"tp": lax.rem(tpi + r, tp)}, device_id_type=MESH)
    pl.semaphore_wait(barrier, sp + tp - 2)

    def remote(src, dst, ss, rs, **where):
        return pltpu.make_async_remote_copy(src_ref=src, dst_ref=dst, send_sem=ss, recv_sem=rs,
                                            device_id=where, device_id_type=MESH)

    def w_copy(r):
        to = lax.rem(tpi + r, tp)
        return remote(wgt.at[pl.ds(pl.multiple_of(to * feat, feat), feat), :], w_in.at[r],
                      w_ss.at[r - 1], w_rs.at[r - 1], tp=to)

    def member(r):
        return lax.rem(y + r, inner)

    def a_copy(side, r, u):
        return remote(a_out.at[side, r - 1, u], a_in.at[side, r, u], a_ss.at[side, r - 1, u],
                      a_rs.at[side, r - 1, u], sp=z * inner + member(r))

    def b_copy(side, u):
        to = z + 1 if side == 0 else z - 1
        to = jnp.clip(to, 0, outer - 1)
        return remote(b_out.at[side, u], b_in.at[side, u], b_ss.at[side, u], b_rs.at[side, u],
                      sp=to * inner + y)

    def c_copy(side, r, u):
        return remote(c_out.at[side, r, u], c_in.at[side, r, u], c_ss.at[side, r - 1, u],
                      c_rs.at[side, r - 1, u], sp=z * inner + member(r))

    messages = own // group

    def d_copy(t, r, h, m):
        owner = lax.rem(y - r + inner, inner)
        first = pl.multiple_of((owner * own + m * group) * length, length)
        return remote(d_all.at[0, h, pl.ds(first, group * length), :],
                      d_all.at[t, h, pl.ds(first, group * length), :],
                      d_ss.at[t - 1, r, h, m], d_rs.at[t - 1, r, h, m], tp=lax.rem(tpi + t, tp))

    def d_wait(t, r, h, m):
        d_copy(t, r, h, m).wait_recv()

    def g_copy(r, h):
        to = lax.rem(spi + r, sp)
        return remote(g_out.at[h, to], g_in.at[h, r], g_ss.at[h, r - 1], g_rs.at[h, r - 1], sp=to)

    for r in range(1, tp):
        w_copy(r).start()
    w_in[0] = wgt[pl.ds(pl.multiple_of(tpi * feat, feat), feat), :]

    chunk = 4 * length
    total = batch * length

    def values(i, _):
        at = pl.ds(pl.multiple_of(i * chunk, chunk), chunk)
        val[at, :] = dot(hid[at, :], wgt[...]).astype(BF16)
        return 0

    mine = own * length // chunk if own * length % chunk == 0 else 0

    def values_of(r):
        lax.fori_loop(0, mine, lambda i, _: values(member(r) * mine + i, 0), 0)

    if mine:
        for r in range(1, inner):
            values_of(r)
    else:
        lax.fori_loop(0, total // chunk, values, 0)

    row = lax.broadcasted_iota(jnp.int32, (length, length), 0)
    col = lax.broadcasted_iota(jnp.int32, (length, length), 1)
    lower, upper = row >= col, row <= col
    ones_lower, ones_upper = jnp.where(lower, 1.0, 0.0), jnp.where(upper, 1.0, 0.0)
    sums = jnp.concatenate([ones_lower, ones_upper], 0).astype(BF16)
    strict = jnp.concatenate([jnp.where(row > col, 1.0, 0.0), jnp.where(row < col, 1.0, 0.0)], 0).astype(BF16)
    left = lax.broadcasted_iota(jnp.int32, (length, pack), 1) < dk
    tail_row = lax.broadcasted_iota(jnp.int32, (16, pack), 0)
    ones_tail = jnp.ones((16, dv), BF16)
    ones_dv = jnp.ones((16, dv), BF16)

    def both(matrix, x):
        high, low = split(x)
        out = dot(matrix, high) + dot(matrix, low)
        return jnp.where(left, out[:length], out[length:])

    def head_cols(ref, b, h):
        at = pl.ds(pl.multiple_of(b * length, length), length)
        return ref[at, pl.ds(pl.multiple_of(h * dv, dv), dv)]

    def twice(ref, b, h):
        x = ref[b, h].astype(F32)
        return jnp.concatenate([x, x], 1)

    def parts(b, h):
        c = both(sums, jnp.concatenate([fdec[b, h], bdec[b, h]], 1))
        cum[b, h] = c
        end = jnp.where(left[:1], c[length - 1:length], c[0:1])
        grow = (twice(qry, b, h) * jnp.exp(c)).astype(BF16)
        decay_key = (twice(key, b, h) * jnp.exp(end - c)).astype(BF16)
        state = dot(decay_key, head_cols(val, b, h), 0, 0)
        grad = dot(grow, head_cols(cot, b, h), 0, 0)
        high = end.astype(BF16).astype(F32)
        tail = jnp.where(tail_row == 0, high, jnp.where(tail_row == 1, end - high, 0.0))
        low = jnp.concatenate([state[:dk], grad[dk:], tail], 0).astype(BF16)
        up = jnp.concatenate([grad[:dk], state[dk:], tail], 0).astype(BF16)
        return low, up

    pair = 2 if units % 2 == 0 else 1

    def phase_one(i, _):
        todo = [(r, i * pair + n) for n in range(pair) for r in range(1, inner)]
        made = [parts(member(r) * own + lax.rem(u, own), u // own) for r, u in todo]
        for (r, u), sides in zip(todo, made):
            for side in range(2):
                a_out[side, r - 1, u] = sides[side]
        for r, u in todo:
            for side in range(2):
                a_copy(side, r, u).start()
        return 0

    lax.fori_loop(0, units // pair, phase_one, 0)
    if mine:
        values_of(0)

    def intra(b, h):
        c = cum[b, h]
        q_hat = (twice(qry, b, h) * jnp.exp(c)).astype(BF16)
        k_hat = (twice(key, b, h) * jnp.exp(-c)).astype(BF16)
        v, seed = head_cols(val, b, h), head_cols(cot, b, h)
        seed_scores = dot(seed, v, 1, 1)
        zero = jnp.zeros_like(q_hat)
        q_left, q_right = jnp.where(left, q_hat, zero), jnp.where(left, zero, q_hat)
        k_left, k_right = jnp.where(left, k_hat, zero), jnp.where(left, zero, k_hat)
        score = (jnp.where(lower, dot(q_left, k_hat, 1, 1), 0.0)
                 + jnp.where(upper, dot(q_right, k_hat, 1, 1), 0.0)).astype(BF16)
        seed_low = jnp.where(lower, seed_scores, 0.0).astype(BF16)
        seed_up = jnp.where(upper, seed_scores, 0.0).astype(BF16)
        intra_q[b, h] = dot(seed_low, k_left) + dot(seed_up, k_right)
        intra_k[b, h] = dot(seed_low, q_left, 0, 0) + dot(seed_up, q_right, 0, 0)
        intra_v[b, h] = dot(score, seed, 0, 0)

    def combine(side, u):
        @pl.when((z > 0) if side == 0 else (z < outer - 1))
        def _():
            b_copy(side, u).wait_recv()

        first = (z == 0) if side == 0 else (z == outer - 1)

        @pl.when(first)
        def _():
            b_in[side, u] = jnp.zeros((pack, dv), BF16)

        for r in range(1, inner):
            a_copy(side, r, u).wait_recv()
        running = b_in[side, u].astype(F32)
        order = range(inner) if side == 0 else range(inner - 1, -1, -1)
        for person in order:
            r = lax.rem(person - y + inner, inner)
            source = lax.rem(y - person + inner, inner)
            c_out[side, r, u] = running.astype(BF16)
            message = a_in[side, source, u]
            factor = jnp.exp(dot(message[pack:], ones_tail, 0, 0))
            running = factor * running + message[:pack].astype(F32)
        b_out[side, u] = running.astype(BF16)

        @pl.when((z < outer - 1) if side == 0 else (z > 0))
        def _():
            b_copy(side, u).start()

        c_in[side, 0, u] = c_out[side, 0, u]
        for r in range(1, inner):
            c_copy(side, r, u).start()

    def finish(r, u, h, step):
        b = lax.rem(y - r + inner, inner) * own + step
        low, up = c_in[0, r, u], c_in[1, r, u]
        state = jnp.concatenate([low[:dk], up[dk:]], 0)
        grad = jnp.concatenate([up[:dk], low[dk:]], 0)
        c = cum[b, h]
        end = jnp.where(left[:1], c[length - 1:length], c[0:1])
        grow, shrink, to_end = jnp.exp(c), jnp.exp(-c), jnp.exp(end - c)
        q, k = twice(qry, b, h), twice(key, b, h)
        v, seed = head_cols(val, b, h), head_cols(cot, b, h)
        cross = dot(seed, state, 1, 1)
        dq = grow * (intra_q[b, h] + cross)
        dk_ = shrink * intra_k[b, h] + to_end * dot(v, grad, 1, 1)
        dv_ = intra_v[b, h] + dot((k * to_end).astype(BF16), grad)
        g = q * dq - k * dk_
        pair = (state.astype(F32) * grad.astype(F32)).astype(BF16)
        start = (jnp.sum(q * grow * cross, axis=0, keepdims=True)
                 + jnp.exp(end) * dot(ones_dv, pair, 1, 1)[:1])
        decay_grad = start - both(strict, g)
        o_q[b, h] = (dq[:, :dk] + dq[:, dk:]).astype(BF16)
        o_k[b, h] = (dk_[:, :dk] + dk_[:, dk:]).astype(BF16)
        o_f[b, h] = decay_grad[:, :dk]
        o_b[b, h] = decay_grad[:, dk:]
        d_all[0, h, pl.ds(pl.multiple_of(b * length, length), length), :] = dv_.astype(BF16)

    def weight_term(h):
        full = dot(d_all[0, h], hid[...], 0, 0)
        for p in range(sp):
            g_out[h, p] = full[:, p * rows_sp:(p + 1) * rows_sp].astype(BF16)
        for r in range(1, sp):
            g_copy(r, h).start()

    delay = (outer - 1) * LAG + 1 + EXTRA

    def phase_two(s, _):
        for side in range(2):
            at = s - 1 - (z if side == 0 else outer - 1 - z) * LAG

            @pl.when((at >= 0) & (at < units))
            def _():
                combine(side, at)

        @pl.when(s < units)
        def _():
            h, step = s // own, lax.rem(s, own)
            low, up = parts(y * own + step, h)
            a_in[0, 0, s] = low
            a_in[1, 0, s] = up
            for r in range(inner):
                intra(member(r) * own + step, h)

        last = s - delay

        @pl.when(last >= 0)
        def _():
            h, step = last // own, lax.rem(last, own)
            for side in range(2):
                for r in range(1, inner):
                    c_copy(side, r, last).wait_recv()
            for r in range(inner):
                finish(r, last, h, step)

            @pl.when(lax.rem(step + 1, group) == 0)
            def _():
                m = step // group
                for r in range(inner):
                    for t in range(1, tp):
                        d_copy(t, r, h, m).start()

            @pl.when(step == own - 1)
            def _():
                weight_term(h)
        return 0

    lax.fori_loop(0, units + delay, phase_two, 0)

    for t in range(1, tp):
        w_copy(t).wait_recv()
        for r in range(inner):
            for h in range(heads):
                for m in range(messages):
                    d_wait(t, r, h, m)

    def features(i, _):
        at = pl.ds(pl.multiple_of(i * chunk, chunk), chunk)
        acc = jnp.zeros((chunk, feat), F32)
        for t in range(tp):
            for h in range(heads):
                acc = acc + dot(d_all[t, h, at, :], w_in[t, :, h * dv:(h + 1) * dv], 1, 1)
        o_h[at, :] = acc.astype(BF16)
        return 0

    lax.fori_loop(0, total // chunk, features, 0)

    for h in range(heads):
        acc = g_out[h, spi].astype(F32)
        for r in range(1, sp):
            g_copy(r, h).wait_recv()
            acc = acc + g_in[h, r].astype(F32)
        o_w[:, h * dv:(h + 1) * dv] = acc.T

    for r in range(1, tp):
        w_copy(r).wait_send()
    for h in range(heads):
        for r in range(1, sp):
            g_copy(r, h).wait_send()
        for m in range(messages):
            for t in range(1, tp):
                for r in range(inner):
                    d_copy(t, r, h, m).wait_send()

    def drain(u, _):
        for side in range(2):
            for r in range(1, inner):
                a_copy(side, r, u).wait_send()
                c_copy(side, r, u).wait_send()

            @pl.when((z < outer - 1) if side == 0 else (z > 0))
            def _():
                b_copy(side, u).wait_send()
        return 0

    lax.fori_loop(0, units, drain, 0)


def d_group(own):
    return 4 if own % 4 == 0 else 1


def shards(sp, tp, hidden, value_weight, queries, key_vectors, forward_decay, backward_decay, cotangent):
    batch, length, width = hidden.shape
    heads, dk = queries.shape[1], queries.shape[3]
    cols = value_weight.shape[1]
    dv = cols // heads
    outer, inner, own, units = plan(sp, batch, heads)
    pack, rows, feat, rows_sp = 2 * dk, batch * length, width // tp, width // sp
    group = d_group(own)
    dims = (sp, tp, batch, heads, length, dk, dv, width)
    vmem, dma = pltpu.VMEM, pltpu.SemaphoreType.DMA
    peers = max(inner - 1, 1)
    scratch = [
        vmem((rows, cols), BF16),
        vmem((batch, heads, length, pack), F32),
        vmem((batch, heads, length, pack), F32),
        vmem((batch, heads, length, pack), F32),
        vmem((batch, heads, length, dv), F32),
        vmem((2, peers, units, pack + 16, dv), BF16),
        vmem((2, inner, units, pack + 16, dv), BF16),
        vmem((2, units, pack, dv), BF16),
        vmem((2, units, pack, dv), BF16),
        vmem((2, inner, units, pack, dv), BF16),
        vmem((2, inner, units, pack, dv), BF16),
        vmem((tp, heads, rows, dv), BF16),
        vmem((tp, feat, cols), BF16),
        vmem((heads, sp, dv, rows_sp), BF16),
        vmem((heads, sp, dv, rows_sp), BF16),
        dma((2, peers, units)), dma((2, peers, units)),
        dma((2, units)), dma((2, units)),
        dma((2, peers, units)), dma((2, peers, units)),
        dma((tp - 1, inner, heads, own // group)), dma((tp - 1, inner, heads, own // group)),
        dma((tp - 1,)), dma((tp - 1,)),
        dma((heads, sp - 1)), dma((heads, sp - 1)),
    ]
    whole = pl.BlockSpec(memory_space=vmem)
    outs = pl.pallas_call(
        functools.partial(kernel, dims),
        out_shape=(
            vmem((batch, heads, length, dk), BF16),
            vmem((batch, heads, length, dk), BF16),
            vmem((batch, heads, length, dk), F32),
            vmem((batch, heads, length, dk), F32),
            vmem((rows, feat), BF16),
            vmem((rows_sp, cols), F32),
        ),
        in_specs=[whole] * 7,
        out_specs=(whole,) * 6,
        scratch_shapes=scratch,
        compiler_params=pltpu.CompilerParams(
            collective_id=0, has_side_effects=True, vmem_limit_bytes=40 * 1024 * 1024
        ),
    )(hidden.reshape(rows, width), value_weight, queries, key_vectors, forward_decay, backward_decay,
      cotangent.reshape(rows, cols))
    outs = store(outs)
    return outs[:4] + (outs[4].reshape(batch, length, feat), outs[5])


def store_kernel(*refs):
    n = len(refs) // 2
    sems = refs[-1]
    copies = [pltpu.make_async_copy(refs[i], refs[n + i], sems.at[i]) for i in range(n)]
    for copy in copies:
        copy.start()
    for copy in copies:
        copy.wait()


def store(arrays):
    n = len(arrays)
    return pl.pallas_call(
        store_kernel,
        out_shape=tuple(jax.ShapeDtypeStruct(a.shape, a.dtype) for a in arrays),
        in_specs=[pl.BlockSpec(memory_space=pltpu.VMEM)] * n,
        out_specs=(pl.BlockSpec(memory_space=pl.ANY),) * n,
        scratch_shapes=[pltpu.SemaphoreType.DMA((n,))],
        compiler_params=pltpu.CompilerParams(has_side_effects=True, vmem_limit_bytes=1024 * 1024),
    )(*arrays)


def solution(mesh):
    heads = P(None, "tp", "sp", None)
    return jax.shard_map(
        functools.partial(shards, mesh.shape["sp"], mesh.shape["tp"]),
        mesh=mesh,
        in_specs=(P(None, "sp", None), P(None, "tp"), heads, heads, heads, heads, P(None, "sp", "tp")),
        out_specs=(heads, heads, heads, heads, P(None, "sp", "tp"), P("sp", "tp")),
        check_vma=False,
    )
```

```python
import functools

import jax
import jax.numpy as jnp
from jax import lax
from jax.experimental import pallas as pl
from jax.experimental.pallas import tpu as pltpu
from jax.sharding import PartitionSpec as P

F32, BF16 = jnp.float32, jnp.bfloat16
MESH = pl.DeviceIdType.MESH
CORES = 2
INNER = 4


def dot(a, b, ca=1, cb=0):
    return lax.dot_general(a, b, (((ca,), (cb,)), ((), ())), preferred_element_type=F32)


def halves(x):
    high = x.astype(BF16)
    return jnp.concatenate([high, (x - high.astype(F32)).astype(BF16)], 0)


def kernel(dims, hid, wgt, qry, key, fdec, bdec, cot,
           o_q, o_k, o_f, o_b, o_h, o_w,
           hid_v, wgt_v, q_v, k_v, f_v, b_v, cot_v,
           val, cum, q_hats, k_ends, intra_q, intra_k, intra_v,
           a_out, a_in, e_out, e_in, local, b_out, b_in, c_out, c_in,
           d_all, w_in, w_acc, g_out, g_in,
           i_s, h_s, a_ss, a_rs, e_ss, e_rs, b_ss, b_rs, c_ss, c_rs,
           d_ss, d_rs, p_ss, p_rs, f_ss, f_rs, w_ss, w_rs, g_ss, g_rs):
    sp, tp, batch, length, dk, dv, width = dims
    inner, outer, own, xs = INNER, sp // INNER, batch // INNER, tp // CORES
    pack, feat, rows_sp, group = 2 * dk, width // tp, width // sp, INNER * length
    spi, tpi = lax.axis_index("sp"), lax.axis_index("tp")
    z, y = spi // inner, lax.rem(spi, inner)
    x, core = tpi // CORES, lax.rem(tpi, CORES)

    barrier = pltpu.get_barrier_semaphore()
    for r in range(1, sp):
        pl.semaphore_signal(barrier, inc=1, device_id={"sp": lax.rem(spi + r, sp)}, device_id_type=MESH)
    for r in range(1, tp):
        pl.semaphore_signal(barrier, inc=1, device_id={"tp": lax.rem(tpi + r, tp)}, device_id_type=MESH)

    def owner(r):
        return lax.rem(y + r, inner)

    def batch_of(r, u):
        return owner(r) * own + u

    def slot(r, u):
        return u * inner + r

    def rows(r, u, count=1):
        return pl.ds(pl.multiple_of(slot(r, u) * length, length), count * length)

    small = [pltpu.make_async_copy(src, dst, i_s.at[i]) for i, (src, dst) in enumerate(
        ((fdec, f_v), (bdec, b_v), (qry, q_v), (cot, cot_v), (wgt, wgt_v), (key, k_v)))]

    def load_hidden(r, u):
        return pltpu.make_async_copy(hid.at[batch_of(r, u)], hid_v.at[rows(r, u)], h_s.at[slot(r, u)])

    for copy in small[:5]:
        copy.start()
    for u in range(own):
        for r in range(inner):
            load_hidden(r, u).start()
        if u == 0:
            small[5].start()

    def remote(src, dst, ss, rs, **where):
        return pltpu.make_async_remote_copy(src_ref=src, dst_ref=dst, send_sem=ss, recv_sem=rs,
                                            device_id=where, device_id_type=MESH)

    def w_copy(r):
        to = lax.rem(tpi + r, tp)
        return remote(wgt_v.at[pl.ds(pl.multiple_of(to * feat, feat), feat), :], w_in.at[tpi],
                      w_ss.at[r - 1], w_rs.at[r - 1], tp=to)

    def a_copy(kind, r, u):
        return remote(a_out.at[kind, r - 1, u], a_in.at[kind, r, u], a_ss.at[kind, r - 1, u],
                      a_rs.at[kind, r - 1, u], sp=z * inner + owner(r))

    def e_copy(r):
        to = lax.rem(spi + r, sp)
        return remote(e_out.at[lax.rem(to, inner)], e_in.at[r], e_ss.at[r - 1], e_rs.at[r - 1], sp=to)

    def b_copy(side, r, u):
        to = jnp.clip(z + r if side == 0 else z - r, 0, outer - 1)
        return remote(b_out.at[side, u], b_in.at[side, r - 1, u], b_ss.at[side, r - 1, u],
                      b_rs.at[side, r - 1, u], sp=to * inner + y)

    def above(r):
        return z + r < outer

    def below(r):
        return z >= r

    def c_copy(side, r, u):
        return remote(c_out.at[side, r, u], c_in.at[side, r - 1, u], c_ss.at[side, r - 1, u],
                      c_rs.at[side, r - 1, u], sp=z * inner + lax.rem(y - r + inner, inner))

    def part_rows(u, part):
        return rows(0, u) if part == 0 else rows(1, u, inner - 1)

    def d_copy(r, u, part):
        at = part_rows(u, part)
        return remote(d_all.at[tpi, at], d_all.at[tpi, at], d_ss.at[r - 1, u, part],
                      d_rs.at[r - 1, u, part], tp=lax.rem(x + r, xs) * CORES + core)

    mate = x * CORES + 1 - core

    def p_copy(u, part):
        at = part_rows(u, part)
        return remote(d_all.at[tpi, at], d_all.at[tpi, at], p_ss.at[u, part], p_rs.at[u, part], tp=mate)

    def f_copy(r, u):
        source = lax.rem(x - r + xs, xs) * CORES + core
        at = rows(0, u, inner)
        return remote(d_all.at[source, at], d_all.at[source, at], f_ss.at[r - 1, u], f_rs.at[r - 1, u], tp=mate)

    def g_copy(r):
        to = lax.rem(spi + r, sp)
        return remote(g_out.at[to], g_in.at[r - 1], g_ss.at[r - 1], g_rs.at[r - 1], sp=to)

    row = lax.broadcasted_iota(jnp.int32, (length, length), 0)
    col = lax.broadcasted_iota(jnp.int32, (length, length), 1)
    lower, upper = row >= col, row <= col

    def matrix(first, second):
        both = jnp.concatenate([jnp.where(first, 1.0, 0.0), jnp.where(second, 1.0, 0.0)], 0)
        return jnp.concatenate([both, both], 1).astype(BF16)

    sums, strict = matrix(lower, upper), matrix(row > col, row < col)
    left = lax.broadcasted_iota(jnp.int32, (length, pack), 1) < dk
    left_tall = lax.broadcasted_iota(jnp.int32, (dv, pack), 1) < dk

    def directed(tri, blocks):
        made = []
        for i in range(0, len(blocks), 2):
            pair = blocks[i:i + 2]
            out = dot(tri, halves(jnp.concatenate(pair, 1) if len(pair) > 1 else pair[0]))
            for n in range(len(pair)):
                part = out[:, n * pack:(n + 1) * pack]
                made.append(jnp.where(left, part[:length], part[length:]))
        return made

    def twice(ref, b):
        v = ref[b].astype(F32)
        return jnp.concatenate([v, v], 1)

    def ends(c):
        return jnp.where(left[:1], c[length - 1:length], c[0:1])

    for side in range(2):
        for r in range(1, outer):
            @pl.when(jnp.logical_not(below(r) if side == 0 else above(r)))
            def _():
                b_in[side, r - 1] = jnp.zeros((own, dv, pack), BF16)

    for copy in small[:2]:
        copy.wait()

    def decays(u, _):
        blocks = [jnp.concatenate([f_v[batch_of(r, u)], b_v[batch_of(r, u)]], 1) for r in range(inner)]
        made = directed(sums, blocks)
        for r in range(inner):
            cum[slot(r, u)] = made[r]
        for r in range(inner):
            e_out[owner(r), pl.ds(u, 1), :] = ends(made[r])
        return 0

    lax.fori_loop(0, own, decays, 0)

    def grads(todo):
        hats = [(twice(q_v, batch_of(r, u)) * jnp.exp(cum[slot(r, u)])).astype(BF16) for r, u in todo]
        made = [dot(cot_v[batch_of(r, u)], hat, 0, 0).astype(BF16) for (r, u), hat in zip(todo, hats)]
        return hats, made

    def states(todo):
        keys = []
        for r, u in todo:
            c = cum[slot(r, u)]
            keys.append((twice(k_v, batch_of(r, u)) * jnp.exp(ends(c) - c)).astype(BF16))
        made = [dot(val[rows(r, u)], k_end, 0, 0).astype(BF16) for (r, u), k_end in zip(todo, keys)]
        return keys, made

    def place(kind, r, u, value):
        if r == 0:
            a_in[kind, 0, u] = value
        else:
            a_out[kind, r - 1, u] = value

    def emit(kind, todo):
        kept, made = (grads if kind == 0 else states)(todo)
        keep = q_hats if kind == 0 else k_ends
        for (r, u), value, block in zip(todo, kept, made):
            keep[slot(r, u)] = value
            place(kind, r, u, block)

    def values(u):
        at = rows(0, u, inner)
        val[at] = dot(hid_v[at], wgt_v[...]).astype(BF16)

    for copy in small[2:4]:
        copy.wait()

    bunch = 2 if own % 2 == 0 else 1
    for first in range(0, own, bunch):
        todo = [(r, first + n) for n in range(bunch) for r in range(1, inner)]
        emit(0, todo)
        if first == 0:
            pl.semaphore_wait(barrier, sp + tp - 2)
            for r in range(1, sp):
                e_copy(r).start()
        for r, u in todo:
            a_copy(0, r, u).start()
        if first == 0:
            for copy in small[4:]:
                copy.wait()
            for r in range(1, tp):
                w_copy(r).start()
            w_in[tpi] = wgt_v[pl.ds(pl.multiple_of(tpi * feat, feat), feat), :]
            e_in[0] = e_out[y]
        for n in range(bunch):
            for r in range(inner):
                load_hidden(r, first + n).wait()
            values(first + n)
        emit(1, todo)
        for r, u in todo:
            a_copy(1, r, u).start()

    mine = [(0, u) for u in range(own)]
    emit(0, mine)
    emit(1, mine)
    w_acc[...] = jnp.zeros((dv, width), F32)
    for r in range(1, sp):
        e_copy(r).wait_recv()

    def ending(plane, person, u):
        source = lax.rem(spi - (plane * inner + person) + sp, sp)
        return e_in[source, pl.ds(u, 1), :]

    people = (tuple(range(inner)), tuple(range(inner - 1, -1, -1)))

    def offset(person):
        return lax.rem(y - person + inner, inner)

    def combine_plane(u):
        for kind in range(2):
            for r in range(1, inner):
                a_copy(kind, r, u).wait_recv()
        for side in range(2):
            running = jnp.zeros((dv, pack), F32)
            for n, person in enumerate(people[side]):
                grad, state = a_in[0, offset(person), u], a_in[1, offset(person), u]
                block = jnp.where(left_tall, state, grad) if side == 0 else jnp.where(left_tall, grad, state)
                if n == 0:
                    running = block.astype(F32)
                else:
                    local[side, person, u] = running
                    running = jnp.exp(ending(z, person, u)) * running + block.astype(F32)
            b_out[side, u] = running.astype(BF16)
        for side in range(2):
            for r in range(1, outer):
                @pl.when(above(r) if side == 0 else below(r))
                def _():
                    b_copy(side, r, u).start()

    def combine_all(u):
        for side in range(2):
            for r in range(1, outer):
                @pl.when(below(r) if side == 0 else above(r))
                def _():
                    b_copy(side, r, u).wait_recv()
        for side in range(2):
            carried = b_in[side, 0, u].astype(F32)
            passed = jnp.zeros((1, pack), F32)
            for r in range(2, outer):
                plane = lax.rem(z - r + 1 + outer, outer) if side == 0 else lax.rem(z + r - 1, outer)
                for person in range(inner):
                    passed = passed + ending(plane, person, u)
                carried = carried + jnp.exp(passed) * b_in[side, r - 1, u].astype(F32)
            passed = jnp.zeros((1, pack), F32)
            for n, person in enumerate(people[side]):
                if n == 0:
                    c_out[side, offset(person), u] = carried.astype(BF16)
                else:
                    out = jnp.exp(passed) * carried + local[side, person, u]
                    c_out[side, offset(person), u] = out.astype(BF16)
                passed = passed + ending(z, person, u)
        for side in range(2):
            for r in range(1, inner):
                c_copy(side, r, u).start()

    def intra(todo):
        made = []
        for r, u in todo:
            b, s = batch_of(r, u), slot(r, u)
            q_hat = q_hats[s]
            k_hat = (twice(k_v, b) * jnp.exp(-cum[s])).astype(BF16)
            v, seed = val[rows(r, u)], cot_v[b]
            seed_scores = dot(seed, v, 1, 1)
            zero = jnp.zeros_like(q_hat)
            q_left, q_right = jnp.where(left, q_hat, zero), jnp.where(left, zero, q_hat)
            k_left, k_right = jnp.where(left, k_hat, zero), jnp.where(left, zero, k_hat)
            score = (jnp.where(lower, dot(q_left, k_hat, 1, 1), 0.0)
                     + jnp.where(upper, dot(q_right, k_hat, 1, 1), 0.0)).astype(BF16)
            seed_low = jnp.where(lower, seed_scores, 0.0).astype(BF16)
            seed_up = jnp.where(upper, seed_scores, 0.0).astype(BF16)
            made.append((dot(seed_low, k_left) + dot(seed_up, k_right),
                         dot(seed_low, q_left, 0, 0) + dot(seed_up, q_right, 0, 0),
                         dot(score, seed, 0, 0)))
        for (r, u), (for_q, for_k, for_v) in zip(todo, made):
            intra_q[slot(r, u)] = for_q
            intra_k[slot(r, u)] = for_k
            intra_v[slot(r, u)] = for_v

    def arrived(r, u):
        low, up = (c_out[0, 0, u], c_out[1, 0, u]) if r == 0 else (c_in[0, r - 1, u], c_in[1, r - 1, u])
        return jnp.where(left_tall, low, up), jnp.where(left_tall, up, low)

    def finish_values(todo):
        made = [intra_v[slot(r, u)] + dot(k_ends[slot(r, u)], arrived(r, u)[1], 1, 1) for r, u in todo]
        for (r, u), block in zip(todo, made):
            d_all[tpi, rows(r, u)] = block.astype(BF16)

    def finish_rest(todo):
        kept, terms = [], []
        for r, u in todo:
            b, s = batch_of(r, u), slot(r, u)
            state, grad = arrived(r, u)
            c = cum[s]
            end = ends(c)
            grow, shrink, to_end = jnp.exp(c), jnp.exp(-c), jnp.exp(end - c)
            q, k = twice(q_v, b), twice(k_v, b)
            cross = dot(cot_v[b], state)
            dq = grow * (intra_q[s] + cross)
            dk_ = shrink * intra_k[s] + to_end * dot(val[rows(r, u)], grad)
            terms.append(q * dq - k * dk_)
            start = (jnp.sum(q * grow * cross, axis=0, keepdims=True)
                     + jnp.exp(end) * jnp.sum(state.astype(F32) * grad.astype(F32), axis=0, keepdims=True))
            kept.append((dq, dk_, start))
        for (r, u), (dq, dk_, start), sums_ in zip(todo, kept, directed(strict, terms)):
            b = batch_of(r, u)
            decay_grad = start - sums_
            o_q[b] = (dq[:, :dk] + dq[:, dk:]).astype(BF16)
            o_k[b] = (dk_[:, :dk] + dk_[:, dk:]).astype(BF16)
            o_f[b] = decay_grad[:, :dk]
            o_b[b] = decay_grad[:, dk:]

    def send_rows(u, part):
        for r in range(1, xs):
            d_copy(r, u, part).start()
        p_copy(u, part).start()

    def finish_own(u):
        finish_values([(0, u)])
        send_rows(u, 0)
        finish_rest([(0, u)])

    def first_steps(s, _):
        combine_plane(s)
        intra([(r, s) for r in range(inner)])

        @pl.when(s > 0)
        def _():
            combine_all(s - 1)
            finish_own(s - 1)
        return 0

    lax.fori_loop(0, own, first_steps, 0)
    combine_all(own - 1)
    finish_own(own - 1)

    def forward(u):
        for r in range(1, xs):
            for part in range(2):
                d_copy(r, u, part).wait_recv()
            f_copy(r, u).start()

    def features(u):
        for part in range(2):
            p_copy(u, part).wait_recv()
        for r in range(1, xs):
            f_copy(r, u).wait_recv()
        at = rows(0, u, inner)
        wide = jnp.concatenate([d_all[t, at] for t in range(tp)], 1)
        weights = jnp.concatenate([w_in[t] for t in range(tp)], 1)
        out = dot(wide, weights, 1, 1).astype(BF16)
        for r in range(inner):
            o_h[batch_of(r, u)] = out[r * length:(r + 1) * length]

    for r in range(1, tp):
        w_copy(r).wait_recv()

    def last_steps(u, _):
        others = [(r, u) for r in range(1, inner)]
        for side in range(2):
            for r in range(1, inner):
                c_copy(side, r, u).wait_recv()
        finish_values(others)
        send_rows(u, 1)
        at = rows(0, u, inner)
        w_acc[...] += dot(d_all[tpi, at], hid_v[at], 0, 0)

        @pl.when(u == own - 1)
        def _():
            for p in range(0, sp, 2):
                block = w_acc[:, p * rows_sp:(p + 2) * rows_sp].T.astype(BF16)
                g_out[p] = block[:rows_sp]
                g_out[p + 1] = block[rows_sp:]
            for r in range(1, sp):
                g_copy(r).start()

        finish_rest(others)

        @pl.when(u > 0)
        def _():
            forward(u - 1)

        @pl.when(u > 1)
        def _():
            features(u - 2)
        return 0

    lax.fori_loop(0, own, last_steps, 0)
    forward(own - 1)
    features(own - 2)
    features(own - 1)

    acc = g_out[spi].astype(F32)
    for r in range(1, sp):
        g_copy(r).wait_recv()
        acc = acc + g_in[r - 1].astype(F32)
    o_w[...] = acc

    for r in range(1, tp):
        w_copy(r).wait_send()
    for r in range(1, sp):
        e_copy(r).wait_send()
        g_copy(r).wait_send()

    def drain(u, _):
        for r in range(1, inner):
            for kind in range(2):
                a_copy(kind, r, u).wait_send()
                c_copy(kind, r, u).wait_send()
        for side in range(2):
            for r in range(1, outer):
                @pl.when(above(r) if side == 0 else below(r))
                def _():
                    b_copy(side, r, u).wait_send()
        for part in range(2):
            p_copy(u, part).wait_send()
            for r in range(1, xs):
                d_copy(r, u, part).wait_send()
        for r in range(1, xs):
            f_copy(r, u).wait_send()
        return 0

    lax.fori_loop(0, own, drain, 0)


def store_kernel(*refs):
    n = len(refs) // 2
    copies = [pltpu.make_async_copy(refs[i], refs[n + i], refs[-1].at[i]) for i in range(n)]
    for copy in copies:
        copy.start()
    for copy in copies:
        copy.wait()


def store(arrays):
    n = len(arrays)
    return pl.pallas_call(
        store_kernel,
        out_shape=tuple(jax.ShapeDtypeStruct(a.shape, a.dtype) for a in arrays),
        in_specs=[pl.BlockSpec(memory_space=pltpu.VMEM)] * n,
        out_specs=(pl.BlockSpec(memory_space=pl.ANY),) * n,
        scratch_shapes=[pltpu.SemaphoreType.DMA((n,))],
        compiler_params=pltpu.CompilerParams(has_side_effects=True, vmem_limit_bytes=1024 * 1024),
    )(*arrays)


def shards(sp, tp, hidden, value_weight, queries, key_vectors, forward_decay, backward_decay, cotangent):
    batch, length, width = hidden.shape
    heads, dk = queries.shape[1], queries.shape[3]
    dv = value_weight.shape[1]
    assert heads == 1
    inner, outer, own, xs = INNER, sp // INNER, batch // INNER, tp // CORES
    pack, rows, feat, rows_sp = 2 * dk, batch * length, width // tp, width // sp
    dims = (sp, tp, batch, length, dk, dv, width)
    vmem, dma = pltpu.VMEM, pltpu.SemaphoreType.DMA
    scratch = [
        vmem((rows, width), BF16), vmem((width, dv), BF16),
        vmem((batch, length, dk), BF16), vmem((batch, length, dk), BF16),
        vmem((batch, length, dk), F32), vmem((batch, length, dk), F32),
        vmem((batch, length, dv), BF16),
        vmem((rows, dv), BF16),
        vmem((batch, length, pack), F32),
        vmem((batch, length, pack), BF16), vmem((batch, length, pack), BF16),
        vmem((batch, length, pack), F32), vmem((batch, length, pack), F32),
        vmem((batch, length, dv), F32),
        vmem((2, inner - 1, own, dv, pack), BF16), vmem((2, inner, own, dv, pack), BF16),
        vmem((inner, own, pack), F32), vmem((sp, own, pack), F32),
        vmem((2, inner, own, dv, pack), F32),
        vmem((2, own, dv, pack), BF16), vmem((2, outer - 1, own, dv, pack), BF16),
        vmem((2, inner, own, dv, pack), BF16), vmem((2, inner - 1, own, dv, pack), BF16),
        vmem((tp, rows, dv), BF16), vmem((tp, feat, dv), BF16),
        vmem((dv, width), F32),
        vmem((sp, rows_sp, dv), BF16), vmem((sp - 1, rows_sp, dv), BF16),
        dma((6,)), dma((batch,)),
        dma((2, inner - 1, own)), dma((2, inner - 1, own)),
        dma((sp - 1,)), dma((sp - 1,)),
        dma((2, outer - 1, own)), dma((2, outer - 1, own)),
        dma((2, inner - 1, own)), dma((2, inner - 1, own)),
        dma((xs - 1, own, 2)), dma((xs - 1, own, 2)),
        dma((own, 2)), dma((own, 2)),
        dma((xs - 1, own)), dma((xs - 1, own)),
        dma((tp - 1,)), dma((tp - 1,)),
        dma((sp - 1,)), dma((sp - 1,)),
    ]
    whole = pl.BlockSpec(memory_space=vmem)
    flat = (batch, length, dk)
    args = (hidden, value_weight, queries.reshape(flat), key_vectors.reshape(flat),
            forward_decay.reshape(flat), backward_decay.reshape(flat), cotangent)
    outs = pl.pallas_call(
        functools.partial(kernel, dims),
        out_shape=(
            vmem(flat, BF16), vmem(flat, BF16), vmem(flat, F32), vmem(flat, F32),
            vmem((batch, length, feat), BF16), vmem((rows_sp, dv), F32),
        ),
        in_specs=[pl.BlockSpec(memory_space=pltpu.HBM)] * 7,
        out_specs=(whole,) * 6,
        scratch_shapes=scratch,
        compiler_params=pltpu.CompilerParams(
            collective_id=0, has_side_effects=True, vmem_limit_bytes=48 * 1024 * 1024
        ),
    )(*(pltpu.with_memory_space_constraint(a, pltpu.HBM) for a in args))
    outs = store(outs)
    return tuple(a.reshape(queries.shape) for a in outs[:4]) + tuple(outs[4:])


def solution(mesh):
    heads = P(None, "tp", "sp", None)
    return jax.shard_map(
        functools.partial(shards, mesh.shape["sp"], mesh.shape["tp"]),
        mesh=mesh,
        in_specs=(P(None, "sp", None), P(None, "tp"), heads, heads, heads, heads, P(None, "sp", "tp")),
        out_specs=(heads, heads, heads, heads, P(None, "sp", "tp"), P("sp", "tp")),
        check_vma=False,
    )
```

```python
import functools

import jax
import jax.numpy as jnp
from jax import lax
from jax.experimental import pallas as pl
from jax.experimental.pallas import tpu as pltpu
from jax.sharding import PartitionSpec as P

F32, BF16 = jnp.float32, jnp.bfloat16
MESH = pl.DeviceIdType.MESH
CORES = 2
INNER = 4
PLACE = (0, 2, 1, 3)
FAR_FIRST = (2, 1, 3)
OFFSETS = sorted(((dz, dy) for dz in range(4) for dy in range(4) if dz or dy),
                 key=lambda d: -sum(min(v, 4 - v) for v in d))


def dot(a, b, ca=1, cb=0):
    return lax.dot_general(a, b, (((ca,), (cb,)), ((), ())), preferred_element_type=F32)


def halves(x):
    high = x.astype(BF16)
    return jnp.concatenate([high, (x - high.astype(F32)).astype(BF16)], 0)


def kernel(dims, hid, wgt, qry, key, fdec, bdec, cot,
           o_q, o_k, o_f, o_b, o_h, o_w,
           hid_v, wgt_v, q_v, k_v, decay_v, cot_v,
           val, cum, q_hats, k_ends, intra_q, intra_k, intra_v,
           a_out, a_in, e_out, e_in, local, b_out, b_in, c_out, c_in,
           d_all, w_in, w_acc, g_out, g_in,
           i_s, h_s, a_ss, a_rs, e_ss, e_rs, b_ss, b_rs, c_ss, c_rs,
           d_ss, d_rs, f_ss, f_rs, w_ss, w_rs, g_ss, g_rs):
    sp, tp, batch, length, dk, dv, width = dims
    inner, outer, own, xs = INNER, sp // INNER, batch // INNER, tp // CORES
    pack, feat, rows_sp, group = 2 * dk, width // tp, width // sp, INNER * length
    spi, tpi = lax.axis_index("sp"), lax.axis_index("tp")
    z, y = spi // inner, lax.rem(spi, inner)
    x, core = tpi // CORES, lax.rem(tpi, CORES)

    barrier = pltpu.get_barrier_semaphore()
    for r in range(1, sp):
        pl.semaphore_signal(barrier, inc=1, device_id={"sp": lax.rem(spi + r, sp)}, device_id_type=MESH)
    for r in range(1, tp):
        pl.semaphore_signal(barrier, inc=1, device_id={"tp": lax.rem(tpi + r, tp)}, device_id_type=MESH)

    def owner(r):
        return lax.rem(y + r, inner)

    def batch_of(r, u):
        return owner(r) * own + u

    def slot(r, u):
        return u * inner + PLACE[r]

    def rows(r, u, count=1):
        return pl.ds(pl.multiple_of(slot(r, u) * length, length), count * length)

    def away(dz, dy):
        return lax.rem(z + dz, outer) * inner + lax.rem(y + dy, inner)

    bunch = 2 if own % 2 == 0 else 1

    def take(ref, sem):
        pltpu.make_async_copy(ref, ref, sem).wait()

    for i, (src, dst) in enumerate(((fdec, decay_v.at[0]), (bdec, decay_v.at[1]), (qry, q_v), (cot, cot_v),
                                    (wgt, wgt_v))):
        pltpu.make_async_copy(src, dst, i_s.at[max(i - 1, 0)]).start()
    for u in range(own):
        for r in range(inner):
            pltpu.make_async_copy(hid.at[batch_of(r, u)], hid_v.at[rows(r, u)], h_s.at[u // bunch]).start()
        if u == 0:
            pltpu.make_async_copy(key, k_v, i_s.at[4]).start()

    def remote(src, dst, ss, rs, **where):
        return pltpu.make_async_remote_copy(src_ref=src, dst_ref=dst, send_sem=ss, recv_sem=rs,
                                            device_id=where, device_id_type=MESH)

    def w_copy(r):
        to = lax.rem(tpi + r, tp)
        return remote(wgt_v.at[pl.ds(pl.multiple_of(to * feat, feat), feat), :], w_in.at[tpi],
                      w_ss.at[0], w_rs.at[0], tp=to)

    def a_copy(kind, r, u):
        return remote(a_out.at[u, kind, r - 1], a_in.at[u, kind, r], a_ss.at[0], a_rs.at[u],
                      sp=z * inner + owner(r))

    def e_copy(dz, dy):
        return remote(e_out.at[lax.rem(y + dy, inner)], e_in.at[dz * inner + dy], e_ss.at[0], e_rs.at[0],
                      sp=away(dz, dy))

    def b_copy(side, r, u):
        to = jnp.clip(z + r if side == 0 else z - r, 0, outer - 1)
        return remote(b_out.at[side, u], b_in.at[side, u, r - 1], b_ss.at[0], b_rs.at[side, u],
                      sp=to * inner + y)

    def above(r):
        return z + r < outer

    def below(r):
        return z >= r

    def c_copy(side, r, u):
        return remote(c_out.at[u, r, side], c_in.at[u, PLACE[r] - 1, side], c_ss.at[0],
                      c_rs.at[u, PLACE[r] // 2], sp=z * inner + lax.rem(y - r + inner, inner))

    mate = x * CORES + 1 - core

    def d_copies(r, u, count):
        at, half = rows(r, u, count), PLACE[r] // 2
        for k in FAR_FIRST:
            remote(d_all.at[tpi, at], d_all.at[tpi, at], d_ss.at[0], d_rs.at[k - 1, u, half],
                   tp=lax.rem(x + k, xs) * CORES + core).start()
        remote(d_all.at[tpi, at], d_all.at[tpi, at], f_ss.at[0], f_rs.at[u], tp=mate).start()

    def forward(u):
        for half in range(2):
            at = rows(half, u, 2)
            for k in (1, 3, 2):
                mine = d_all.at[lax.rem(x - k + xs, xs) * CORES + core, at]
                take(mine, d_rs.at[k - 1, u, half])
                remote(mine, mine, f_ss.at[0], f_rs.at[u], tp=mate).start()

    def g_copy(dz, dy):
        to = away(dz, dy)
        return remote(g_out.at[to], g_in.at[dz * inner + dy - 1], g_ss.at[0], g_rs.at[0], sp=to)

    row = lax.broadcasted_iota(jnp.int32, (length, length), 0)
    col = lax.broadcasted_iota(jnp.int32, (length, length), 1)
    lower, upper = row >= col, row <= col

    def matrix(first, second):
        both = jnp.concatenate([jnp.where(first, 1.0, 0.0), jnp.where(second, 1.0, 0.0)], 0)
        return jnp.concatenate([both, both], 1).astype(BF16)

    sums, strict = matrix(lower, upper), matrix(row > col, row < col)
    left = lax.broadcasted_iota(jnp.int32, (length, pack), 1) < dk
    left_tall = lax.broadcasted_iota(jnp.int32, (dv, pack), 1) < dk

    def directed(tri, blocks):
        made = []
        for i in range(0, len(blocks), 2):
            pair = blocks[i:i + 2]
            out = dot(tri, halves(jnp.concatenate(pair, 1) if len(pair) > 1 else pair[0]))
            for n in range(len(pair)):
                part = out[:, n * pack:(n + 1) * pack]
                made.append(jnp.where(left, part[:length], part[length:]))
        return made

    def twice(ref, b):
        v = ref[b].astype(F32)
        return jnp.concatenate([v, v], 1)

    def ends(c):
        return jnp.where(left[:1], c[length - 1:length], c[0:1])

    for side in range(2):
        for r in range(1, outer):
            @pl.when(jnp.logical_not(below(r) if side == 0 else above(r)))
            def _():
                b_in[side, :, r - 1] = jnp.zeros((own, dv, pack), BF16)

    def decays(todo):
        blocks = [jnp.concatenate([decay_v[0, batch_of(r, u)], decay_v[1, batch_of(r, u)]], 1) for r, u in todo]
        made = directed(sums, blocks)
        for (r, u), c in zip(todo, made):
            cum[slot(r, u)] = c
        for (r, u), c in zip(todo, made):
            e_out[owner(r), pl.ds(u, 1), :] = ends(c)

    take(decay_v, i_s.at[0])
    decays([(r, u) for u in range(own) for r in range(inner)])

    def grads(todo):
        hats = [(twice(q_v, batch_of(r, u)) * jnp.exp(cum[slot(r, u)])).astype(BF16) for r, u in todo]
        made = [dot(cot_v[batch_of(r, u)], hat, 0, 0).astype(BF16) for (r, u), hat in zip(todo, hats)]
        return hats, made

    def states(todo):
        keys = []
        for r, u in todo:
            c = cum[slot(r, u)]
            keys.append((twice(k_v, batch_of(r, u)) * jnp.exp(ends(c) - c)).astype(BF16))
        made = [dot(val[rows(r, u)], k_end, 0, 0).astype(BF16) for (r, u), k_end in zip(todo, keys)]
        return keys, made

    def place(kind, r, u, value):
        if r == 0:
            a_in[u, kind, 0] = value
        else:
            a_out[u, kind, r - 1] = value

    def emit(kind, todo):
        kept, made = (grads if kind == 0 else states)(todo)
        keep = q_hats if kind == 0 else k_ends
        for (r, u), value, block in zip(todo, kept, made):
            keep[slot(r, u)] = value
            place(kind, r, u, block)

    def values(u):
        at = rows(0, u, inner)
        val[at] = dot(hid_v[at], wgt_v[...]).astype(BF16)

    take(q_v, i_s.at[1])
    take(cot_v, i_s.at[2])

    for first in range(0, own, bunch):
        todo = [(r, first + n) for n in range(bunch) for r in FAR_FIRST]
        emit(0, todo)
        if first == 0:
            pl.semaphore_wait(barrier, sp + tp - 2)
            for offset in OFFSETS:
                e_copy(*offset).start()
        for r, u in todo:
            a_copy(0, r, u).start()
        if first == 0:
            take(wgt_v, i_s.at[3])
            for r in range(1, tp):
                w_copy(r).start()
            w_in[tpi] = wgt_v[pl.ds(pl.multiple_of(tpi * feat, feat), feat), :]
            e_in[0] = e_out[y]
            take(k_v, i_s.at[4])
        take(hid_v.at[rows(0, first, bunch * inner)], h_s.at[first // bunch])
        for n in range(bunch):
            values(first + n)
        emit(1, todo)
        for r, u in todo:
            a_copy(1, r, u).start()

    mine = [(0, u) for u in range(own)]
    emit(0, mine)
    emit(1, mine)
    w_acc[...] = jnp.zeros((dv, width), F32)

    def ending(plane, person, u):
        source = lax.rem(z - plane + outer, outer) * inner + lax.rem(y - person + inner, inner)
        return e_in[source, pl.ds(u, 1), :]

    people = (tuple(range(inner)), tuple(range(inner - 1, -1, -1)))

    def offset(person):
        return lax.rem(y - person + inner, inner)

    def combine_plane(u):
        take(a_in.at[u, :, pl.ds(1, inner - 1)], a_rs.at[u])
        for side in range(2):
            running = jnp.zeros((dv, pack), F32)
            for n, person in enumerate(people[side]):
                grad, state = a_in[u, 0, offset(person)], a_in[u, 1, offset(person)]
                block = jnp.where(left_tall, state, grad) if side == 0 else jnp.where(left_tall, grad, state)
                if n == 0:
                    running = block.astype(F32)
                else:
                    local[side, person, u] = running
                    running = jnp.exp(ending(z, person, u)) * running + block.astype(F32)
            b_out[side, u] = running.astype(BF16)
        for side in range(2):
            for r in range(1, outer):
                @pl.when(above(r) if side == 0 else below(r))
                def _():
                    b_copy(side, r, u).start()

    def combine_all(u):
        for side in range(2):
            for n in range(1, outer):
                @pl.when((z if side == 0 else outer - 1 - z) == n)
                def _():
                    take(b_in.at[side, u, pl.ds(0, n)], b_rs.at[side, u])
        for side in range(2):
            carried = b_in[side, u, 0].astype(F32)
            passed = jnp.zeros((1, pack), F32)
            for r in range(2, outer):
                plane = lax.rem(z - r + 1 + outer, outer) if side == 0 else lax.rem(z + r - 1, outer)
                for person in range(inner):
                    passed = passed + ending(plane, person, u)
                carried = carried + jnp.exp(passed) * b_in[side, u, r - 1].astype(F32)
            passed = jnp.zeros((1, pack), F32)
            for n, person in enumerate(people[side]):
                if n == 0:
                    c_out[u, offset(person), side] = carried.astype(BF16)
                else:
                    out = jnp.exp(passed) * carried + local[side, person, u]
                    c_out[u, offset(person), side] = out.astype(BF16)
                passed = passed + ending(z, person, u)
        for r in FAR_FIRST:
            for side in range(2):
                c_copy(side, r, u).start()

    def intra(todo):
        made = []
        for r, u in todo:
            b, s = batch_of(r, u), slot(r, u)
            q_hat = q_hats[s]
            k_hat = (twice(k_v, b) * jnp.exp(-cum[s])).astype(BF16)
            v, seed = val[rows(r, u)], cot_v[b]
            seed_scores = dot(seed, v, 1, 1)
            zero = jnp.zeros_like(q_hat)
            q_left, q_right = jnp.where(left, q_hat, zero), jnp.where(left, zero, q_hat)
            k_left, k_right = jnp.where(left, k_hat, zero), jnp.where(left, zero, k_hat)
            score = (jnp.where(lower, dot(q_left, k_hat, 1, 1), 0.0)
                     + jnp.where(upper, dot(q_right, k_hat, 1, 1), 0.0)).astype(BF16)
            seed_low = jnp.where(lower, seed_scores, 0.0).astype(BF16)
            seed_up = jnp.where(upper, seed_scores, 0.0).astype(BF16)
            made.append((dot(seed_low, k_left) + dot(seed_up, k_right),
                         dot(seed_low, q_left, 0, 0) + dot(seed_up, q_right, 0, 0),
                         dot(score, seed, 0, 0)))
        for (r, u), (for_q, for_k, for_v) in zip(todo, made):
            intra_q[slot(r, u)] = for_q
            intra_k[slot(r, u)] = for_k
            intra_v[slot(r, u)] = for_v

    def arrived(r, u):
        low, up = (c_out[u, 0, 0], c_out[u, 0, 1]) if r == 0 else (c_in[u, PLACE[r] - 1, 0], c_in[u, PLACE[r] - 1, 1])
        return jnp.where(left_tall, low, up), jnp.where(left_tall, up, low)

    def finish_values(todo):
        made = [intra_v[slot(r, u)] + dot(k_ends[slot(r, u)], arrived(r, u)[1], 1, 1) for r, u in todo]
        for (r, u), block in zip(todo, made):
            d_all[tpi, rows(r, u)] = block.astype(BF16)

    def finish_rest(todo):
        kept, terms = [], []
        for r, u in todo:
            b, s = batch_of(r, u), slot(r, u)
            state, grad = arrived(r, u)
            c = cum[s]
            end = ends(c)
            grow, shrink, to_end = jnp.exp(c), jnp.exp(-c), jnp.exp(end - c)
            q, k = twice(q_v, b), twice(k_v, b)
            cross = dot(cot_v[b], state)
            dq = grow * (intra_q[s] + cross)
            dk_ = shrink * intra_k[s] + to_end * dot(val[rows(r, u)], grad)
            terms.append(q * dq - k * dk_)
            start = (jnp.sum(q * grow * cross, axis=0, keepdims=True)
                     + jnp.exp(end) * jnp.sum(state.astype(F32) * grad.astype(F32), axis=0, keepdims=True))
            kept.append((dq, dk_, start))
        for (r, u), (dq, dk_, start), sums_ in zip(todo, kept, directed(strict, terms)):
            b = batch_of(r, u)
            decay_grad = start - sums_
            o_q[b] = (dq[:, :dk] + dq[:, dk:]).astype(BF16)
            o_k[b] = (dk_[:, :dk] + dk_[:, dk:]).astype(BF16)
            o_f[b] = decay_grad[:, :dk]
            o_b[b] = decay_grad[:, dk:]

    def finish_own(u):
        finish_values([(0, u)])
        d_copies(0, u, 1)
        finish_rest([(0, u)])

    def features(u):
        take(d_all.at[pl.ds(0, xs), rows(0, u, inner)], f_rs.at[u])
        at = rows(0, u, inner)
        wide = jnp.concatenate([d_all[t, at] for t in range(tp)], 1)
        weights = jnp.concatenate([w_in[t] for t in range(tp)], 1)
        out = dot(wide, weights, 1, 1).astype(BF16)
        for r in range(inner):
            o_h[batch_of(r, u)] = out[PLACE[r] * length:(PLACE[r] + 1) * length]

    def finish_others(todo, u):
        first = PLACE[todo[0]] - 1
        take(c_in.at[u, pl.ds(first, len(todo))], c_rs.at[u, (first + 1) // 2])
        todo = [(r, u) for r in todo]
        finish_values(todo)
        d_copies(*todo[0], len(todo))

    def weight_terms(r, u):
        at = rows(r, u, 2)
        return dot(d_all[tpi, at], hid_v[at], 0, 0)

    def others(u):
        finish_others([2], u)
        finish_others([1, 3], u)
        at = rows(0, u, inner)
        w_acc[...] += dot(d_all[tpi, at], hid_v[at], 0, 0)
        finish_rest([(r, u) for r in range(1, inner)])

    def combine_and_finish(u):
        combine_all(u)
        finish_own(u)

    def loop(first, last, step):
        lax.fori_loop(first, last, lambda u, _: step(u) or 0, 0)

    def intra_all(u):
        intra([(r, u) for r in range(inner)])

    def late_steps(u):
        combine_and_finish(u)
        others(u - own // 2)

    loop(0, own - 1, intra_all)
    take(e_in.at[pl.ds(1, sp - 1)], e_rs.at[0])
    combine_plane(0)
    intra_all(own - 1)
    loop(1, own // 2, combine_plane)
    loop(0, own // 2, combine_and_finish)
    loop(own // 2, own, combine_plane)
    loop(own // 2, own, late_steps)
    loop(own - own // 2, own - 1, others)
    take(w_in.at[pl.ds(0, tp - 1)], w_rs.at[0])
    loop(0, own - 2, forward)
    loop(0, own - 3, features)

    end = own - 1
    finish_others([2], end)
    w_acc[...] += weight_terms(0, end)
    finish_others([1, 3], end)
    full = w_acc[...] + weight_terms(1, end)
    for p in range(0, sp, 2):
        block = full[:, p * rows_sp:(p + 2) * rows_sp].T.astype(BF16)
        g_out[p] = block[:rows_sp]
        g_out[p + 1] = block[rows_sp:]
    for offset in OFFSETS:
        g_copy(*offset).start()
    finish_rest([(r, end) for r in range(1, inner)])
    forward(end - 1)
    loop(own - 3, own - 2, features)
    forward(end)
    loop(own - 2, own, features)

    take(g_in, g_rs.at[0])
    acc = g_out[spi].astype(F32)
    for r in range(sp - 1):
        acc = acc + g_in[r].astype(F32)
    o_w[...] = acc

    take(w_in.at[pl.ds(0, tp - 1)], w_ss.at[0])
    take(e_in.at[pl.ds(1, sp - 1)], e_ss.at[0])
    take(a_out, a_ss.at[0])
    take(b_in.at[0], b_ss.at[0])
    take(c_in, c_ss.at[0])
    take(d_all.at[pl.ds(0, xs - 1)], d_ss.at[0])
    take(d_all.at[pl.ds(0, xs)], f_ss.at[0])
    take(g_in, g_ss.at[0])


def store_kernel(*refs):
    n = len(refs) // 2
    copies = [pltpu.make_async_copy(refs[i], refs[n + i], refs[-1].at[i]) for i in range(n)]
    for copy in copies:
        copy.start()
    for copy in copies:
        copy.wait()


def store(arrays):
    n = len(arrays)
    return pl.pallas_call(
        store_kernel,
        out_shape=tuple(jax.ShapeDtypeStruct(a.shape, a.dtype) for a in arrays),
        in_specs=[pl.BlockSpec(memory_space=pltpu.VMEM)] * n,
        out_specs=(pl.BlockSpec(memory_space=pl.ANY),) * n,
        scratch_shapes=[pltpu.SemaphoreType.DMA((n,))],
        compiler_params=pltpu.CompilerParams(has_side_effects=True, vmem_limit_bytes=1024 * 1024),
    )(*arrays)


def shards(sp, tp, hidden, value_weight, queries, key_vectors, forward_decay, backward_decay, cotangent):
    batch, length, width = hidden.shape
    heads, dk = queries.shape[1], queries.shape[3]
    dv = value_weight.shape[1]
    assert heads == 1
    inner, outer, own, xs = INNER, sp // INNER, batch // INNER, tp // CORES
    pack, rows, feat, rows_sp = 2 * dk, batch * length, width // tp, width // sp
    dims = (sp, tp, batch, length, dk, dv, width)
    vmem, dma = pltpu.VMEM, pltpu.SemaphoreType.DMA
    scratch = [
        vmem((rows, width), BF16), vmem((width, dv), BF16),
        vmem((batch, length, dk), BF16), vmem((batch, length, dk), BF16),
        vmem((2, batch, length, dk), F32), vmem((batch, length, dv), BF16),
        vmem((rows, dv), BF16),
        vmem((batch, length, pack), F32),
        vmem((batch, length, pack), BF16), vmem((batch, length, pack), BF16),
        vmem((batch, length, pack), F32), vmem((batch, length, pack), F32),
        vmem((batch, length, dv), F32),
        vmem((own, 2, inner - 1, dv, pack), BF16), vmem((own, 2, inner, dv, pack), BF16),
        vmem((inner, own, pack), F32), vmem((sp, own, pack), F32),
        vmem((2, inner, own, dv, pack), F32),
        vmem((2, own, dv, pack), BF16), vmem((2, own, outer - 1, dv, pack), BF16),
        vmem((own, inner, 2, dv, pack), BF16), vmem((own, inner - 1, 2, dv, pack), BF16),
        vmem((tp, rows, dv), BF16), vmem((tp, feat, dv), BF16),
        vmem((dv, width), F32),
        vmem((sp, rows_sp, dv), BF16), vmem((sp - 1, rows_sp, dv), BF16),
        dma((5,)), dma((2,)),
        dma((1,)), dma((own,)),
        dma((1,)), dma((1,)),
        dma((1,)), dma((2, own)),
        dma((1,)), dma((own, 2)),
        dma((1,)), dma((xs - 1, own, 2)),
        dma((1,)), dma((own,)),
        dma((1,)), dma((1,)),
        dma((1,)), dma((1,)),
    ]
    whole = pl.BlockSpec(memory_space=vmem)
    flat = (batch, length, dk)
    args = (hidden, value_weight, queries.reshape(flat), key_vectors.reshape(flat),
            forward_decay.reshape(flat), backward_decay.reshape(flat), cotangent)
    outs = pl.pallas_call(
        functools.partial(kernel, dims),
        out_shape=(
            vmem(flat, BF16), vmem(flat, BF16), vmem(flat, F32), vmem(flat, F32),
            vmem((batch, length, feat), BF16), vmem((rows_sp, dv), F32),
        ),
        in_specs=[pl.BlockSpec(memory_space=pltpu.HBM)] * 7,
        out_specs=(whole,) * 6,
        scratch_shapes=scratch,
        compiler_params=pltpu.CompilerParams(
            collective_id=0, has_side_effects=True, vmem_limit_bytes=48 * 1024 * 1024
        ),
    )(*(pltpu.with_memory_space_constraint(a, pltpu.HBM) for a in args))
    outs = store(outs)
    return tuple(a.reshape(queries.shape) for a in outs[:4]) + tuple(outs[4:])


def solution(mesh):
    heads = P(None, "tp", "sp", None)
    return jax.shard_map(
        functools.partial(shards, mesh.shape["sp"], mesh.shape["tp"]),
        mesh=mesh,
        in_specs=(P(None, "sp", None), P(None, "tp"), heads, heads, heads, heads, P(None, "sp", "tp")),
        out_specs=(heads, heads, heads, heads, P(None, "sp", "tp"), P("sp", "tp")),
        check_vma=False,
    )
```

```python
import functools

import jax
import jax.numpy as jnp
from jax import lax
from jax.experimental import pallas as pl
from jax.experimental.pallas import tpu as pltpu
from jax.sharding import PartitionSpec as P

F32, BF16 = jnp.float32, jnp.bfloat16
MESH = pl.DeviceIdType.MESH
CORES = 2
INNER = 4
PLACE = (0, 2, 1, 3)
FAR_FIRST = (2, 1, 3)
OFFSETS = sorted(((dz, dy) for dz in range(4) for dy in range(4) if dz or dy),
                 key=lambda d: -sum(min(v, 4 - v) for v in d))


def dot(a, b, ca=1, cb=0):
    return lax.dot_general(a, b, (((ca,), (cb,)), ((), ())), preferred_element_type=F32)


def halves(x):
    high = x.astype(BF16)
    return jnp.concatenate([high, (x - high.astype(F32)).astype(BF16)], 0)


def kernel(dims, hid, wgt, qry, key, fdec, bdec, cot,
           o_q, o_k, o_f, o_b, o_h, o_w,
           hid_v, wgt_v, q_v, k_v, decay_v, cot_v,
           val, cum, q_hats, k_ends, intra_q, intra_k, intra_v,
           a_out, a_in, e_out, e_in, local, b_out, b_in, c_out, c_in,
           d_all, w_in, w_acc, g_out, g_in,
           i_s, h_s, a_ss, a_rs, e_ss, e_rs, b_ss, b_rs, c_ss, c_rs,
           d_ss, d_rs, f_ss, f_rs, w_ss, w_rs, g_ss, g_rs):
    sp, tp, batch, length, dk, dv, width = dims
    inner, outer, own, xs = INNER, sp // INNER, batch // INNER, tp // CORES
    pack, feat, rows_sp, group = 2 * dk, width // tp, width // sp, INNER * length
    spi, tpi = lax.axis_index("sp"), lax.axis_index("tp")
    z, y = spi // inner, lax.rem(spi, inner)
    x, core = tpi // CORES, lax.rem(tpi, CORES)

    barrier = pltpu.get_barrier_semaphore()
    def owner(r):
        return lax.rem(y + r, inner)

    def batch_of(r, u):
        return owner(r) * own + u

    def slot(r, u):
        return u * inner + PLACE[r]

    def rows(r, u, count=1):
        return pl.ds(pl.multiple_of(slot(r, u) * length, length), count * length)

    def away(dz, dy):
        return lax.rem(z + dz, outer) * inner + lax.rem(y + dy, inner)

    def take(ref, sem):
        pltpu.make_async_copy(ref, ref, sem).wait()

    def load(first, count):
        at, n = pl.ds(first, count), min(first, 1)
        for i in range(2):
            pltpu.make_async_copy((fdec, bdec)[i].at[:, at], decay_v.at[i, :, at], i_s.at[n]).start()
        pltpu.make_async_copy(qry.at[:, at], q_v.at[:, at], i_s.at[2 + n]).start()
        pltpu.make_async_copy(cot.at[:, at], cot_v.at[:, at], i_s.at[4 + n]).start()

    def loaded(first, count):
        at, n = pl.ds(first, count), min(first, 1)
        take(decay_v.at[:, :, at], i_s.at[n])
        take(q_v.at[:, at], i_s.at[2 + n])
        take(cot_v.at[:, at], i_s.at[4 + n])

    def load_hidden(u):
        for r in range(inner):
            pltpu.make_async_copy(hid.at[owner(r), u], hid_v.at[rows(r, u)], h_s.at[u]).start()

    load(0, 1)
    for r in range(1, sp):
        pl.semaphore_signal(barrier, inc=1, device_id={"sp": lax.rem(spi + r, sp)}, device_id_type=MESH)
    for r in range(1, tp):
        pl.semaphore_signal(barrier, inc=1, device_id={"tp": lax.rem(tpi + r, tp)}, device_id_type=MESH)

    pltpu.make_async_copy(wgt, wgt_v, i_s.at[6]).start()
    load_hidden(0)
    pltpu.make_async_copy(key, k_v, i_s.at[7]).start()
    load(1, own - 1)
    for u in range(1, own):
        load_hidden(u)

    def remote(src, dst, ss, rs, **where):
        return pltpu.make_async_remote_copy(src_ref=src, dst_ref=dst, send_sem=ss, recv_sem=rs,
                                            device_id=where, device_id_type=MESH)

    def w_copy(r):
        to = lax.rem(tpi + r, tp)
        return remote(wgt_v.at[pl.ds(pl.multiple_of(to * feat, feat), feat), :], w_in.at[tpi],
                      w_ss.at[0], w_rs.at[0], tp=to)

    def a_copy(kind, r, u):
        return remote(a_out.at[u, kind, r - 1], a_in.at[u, kind, r], a_ss.at[0], a_rs.at[u],
                      sp=z * inner + owner(r))

    def e_copy(dz, dy):
        return remote(e_out.at[lax.rem(y + dy, inner)], e_in.at[dz * inner + dy], e_ss.at[0], e_rs.at[0],
                      sp=away(dz, dy))

    def b_copy(side, r, u):
        to = jnp.clip(z + r if side == 0 else z - r, 0, outer - 1)
        return remote(b_out.at[side, u], b_in.at[side, u, r - 1], b_ss.at[0], b_rs.at[u],
                      sp=to * inner + y)

    def above(r):
        return z + r < outer

    def below(r):
        return z >= r

    def c_copy(side, r, u):
        return remote(c_out.at[u, r, side], c_in.at[u, PLACE[r] - 1, side], c_ss.at[0],
                      c_rs.at[u, PLACE[r] // 2], sp=z * inner + lax.rem(y - r + inner, inner))

    mate = x * CORES + 1 - core

    def d_copies(r, u, count):
        at, half = rows(r, u, count), PLACE[r] // 2
        for k in FAR_FIRST:
            remote(d_all.at[tpi, at], d_all.at[tpi, at], d_ss.at[0], d_rs.at[u, half],
                   tp=lax.rem(x + k, xs) * CORES + core).start()
        remote(d_all.at[tpi, at], d_all.at[tpi, at], f_ss.at[0], f_rs.at[u], tp=mate).start()

    def forward(u):
        for half in range(2):
            at = rows(half, u, 2)
            take(d_all.at[pl.ds(0, xs - 1), at], d_rs.at[u, half])
            for k in range(1, xs):
                mine = d_all.at[lax.rem(x - k + xs, xs) * CORES + core, at]
                remote(mine, mine, f_ss.at[0], f_rs.at[u], tp=mate).start()

    def g_copy(dz, dy):
        to = away(dz, dy)
        return remote(g_out.at[to], g_in.at[dz * inner + dy - 1], g_ss.at[0], g_rs.at[0], sp=to)

    row = lax.broadcasted_iota(jnp.int32, (length, length), 0)
    col = lax.broadcasted_iota(jnp.int32, (length, length), 1)
    lower, upper = row >= col, row <= col

    def matrix(first, second):
        both = jnp.concatenate([jnp.where(first, 1.0, 0.0), jnp.where(second, 1.0, 0.0)], 0)
        return jnp.concatenate([both, both], 1).astype(BF16)

    sums, strict = matrix(lower, upper), matrix(row > col, row < col)
    left = lax.broadcasted_iota(jnp.int32, (length, pack), 1) < dk
    left_tall = lax.broadcasted_iota(jnp.int32, (dv, pack), 1) < dk

    def directed(tri, blocks):
        made = []
        for i in range(0, len(blocks), 2):
            pair = blocks[i:i + 2]
            out = dot(tri, halves(jnp.concatenate(pair, 1) if len(pair) > 1 else pair[0]))
            for n in range(len(pair)):
                part = out[:, n * pack:(n + 1) * pack]
                made.append(jnp.where(left, part[:length], part[length:]))
        return made

    def twice(ref, r, u):
        v = ref[owner(r), u].astype(F32)
        return jnp.concatenate([v, v], 1)

    def ends(c):
        return jnp.where(left[:1], c[length - 1:length], c[0:1])

    for side in range(2):
        for r in range(1, outer):
            @pl.when(jnp.logical_not(below(r) if side == 0 else above(r)))
            def _():
                b_in[side, :, r - 1] = jnp.zeros((own, dv, pack), BF16)

    def decays(todo):
        blocks = [jnp.concatenate([decay_v[0, owner(r), u], decay_v[1, owner(r), u]], 1) for r, u in todo]
        made = directed(sums, blocks)
        for (r, u), c in zip(todo, made):
            cum[slot(r, u)] = c
        for (r, u), c in zip(todo, made):
            e_out[owner(r), pl.ds(u, 1), :] = ends(c)

    def grads(todo):
        hats = [(twice(q_v, r, u) * jnp.exp(cum[slot(r, u)])).astype(BF16) for r, u in todo]
        made = [dot(cot_v[owner(r), u], hat, 0, 0).astype(BF16) for (r, u), hat in zip(todo, hats)]
        return hats, made

    def states(todo):
        keys = []
        for r, u in todo:
            c = cum[slot(r, u)]
            keys.append((twice(k_v, r, u) * jnp.exp(ends(c) - c)).astype(BF16))
        made = [dot(val[rows(r, u)], k_end, 0, 0).astype(BF16) for (r, u), k_end in zip(todo, keys)]
        return keys, made

    def place(kind, r, u, value):
        if r == 0:
            a_in[u, kind, 0] = value
        else:
            a_out[u, kind, r - 1] = value

    def emit(kind, todo):
        kept, made = (grads if kind == 0 else states)(todo)
        keep = q_hats if kind == 0 else k_ends
        for (r, u), value, block in zip(todo, kept, made):
            keep[slot(r, u)] = value
            place(kind, r, u, block)

    def values(u):
        at = rows(0, u, inner)
        val[at] = dot(hid_v[at], wgt_v[...]).astype(BF16)

    everyone = tuple(range(inner))
    for u in range(own):
        todo = [(r, u) for r in FAR_FIRST]
        if u == 0:
            loaded(0, 1)
            decays([(r, u) for r in everyone])
        emit(0, todo)
        if u == 0:
            pl.semaphore_wait(barrier, sp + tp - 2)
        for r, u in todo:
            a_copy(0, r, u).start()
        if u == 0:
            loaded(1, own - 1)
            decays([(r, n) for n in range(1, own) for r in everyone])
            for offset in OFFSETS:
                e_copy(*offset).start()
            take(wgt_v, i_s.at[6])
            take(k_v, i_s.at[7])
        take(hid_v.at[rows(0, u, inner)], h_s.at[u])
        values(u)
        emit(1, todo)
        for r, u in todo:
            a_copy(1, r, u).start()

    for r in range(1, tp):
        w_copy(r).start()
    w_in[tpi] = wgt_v[pl.ds(pl.multiple_of(tpi * feat, feat), feat), :]
    e_in[0] = e_out[y]
    mine = [(0, u) for u in range(own)]
    emit(0, mine)
    emit(1, mine)
    w_acc[...] = jnp.zeros((dv, width), F32)

    def ending(plane, person, u):
        source = lax.rem(z - plane + outer, outer) * inner + lax.rem(y - person + inner, inner)
        return e_in[source, pl.ds(u, 1), :]

    people = (tuple(range(inner)), tuple(range(inner - 1, -1, -1)))

    def offset(person):
        return lax.rem(y - person + inner, inner)

    def combine_plane(u):
        take(a_in.at[u, :, pl.ds(1, inner - 1)], a_rs.at[u])
        for side in range(2):
            running = jnp.zeros((dv, pack), F32)
            for n, person in enumerate(people[side]):
                grad, state = a_in[u, 0, offset(person)], a_in[u, 1, offset(person)]
                block = jnp.where(left_tall, state, grad) if side == 0 else jnp.where(left_tall, grad, state)
                if n == 0:
                    running = block.astype(F32)
                else:
                    local[side, person, u] = running
                    running = jnp.exp(ending(z, person, u)) * running + block.astype(F32)
            b_out[side, u] = running.astype(BF16)
        for side in range(2):
            for r in range(1, outer):
                @pl.when(above(r) if side == 0 else below(r))
                def _():
                    b_copy(side, r, u).start()

    def combine_all(u):
        take(b_in.at[0, u], b_rs.at[u])
        for side in range(2):
            carried = b_in[side, u, 0].astype(F32)
            passed = jnp.zeros((1, pack), F32)
            for r in range(2, outer):
                plane = lax.rem(z - r + 1 + outer, outer) if side == 0 else lax.rem(z + r - 1, outer)
                for person in range(inner):
                    passed = passed + ending(plane, person, u)
                carried = carried + jnp.exp(passed) * b_in[side, u, r - 1].astype(F32)
            passed = jnp.zeros((1, pack), F32)
            for n, person in enumerate(people[side]):
                if n == 0:
                    c_out[u, offset(person), side] = carried.astype(BF16)
                else:
                    out = jnp.exp(passed) * carried + local[side, person, u]
                    c_out[u, offset(person), side] = out.astype(BF16)
                passed = passed + ending(z, person, u)
        for r in FAR_FIRST:
            for side in range(2):
                c_copy(side, r, u).start()

    def intra(todo):
        made = []
        for r, u in todo:
            s = slot(r, u)
            q_hat = q_hats[s]
            k_hat = (twice(k_v, r, u) * jnp.exp(-cum[s])).astype(BF16)
            v, seed = val[rows(r, u)], cot_v[owner(r), u]
            seed_scores = dot(seed, v, 1, 1)
            zero = jnp.zeros_like(q_hat)
            q_left, q_right = jnp.where(left, q_hat, zero), jnp.where(left, zero, q_hat)
            k_left, k_right = jnp.where(left, k_hat, zero), jnp.where(left, zero, k_hat)
            score = (jnp.where(lower, dot(q_left, k_hat, 1, 1), 0.0)
                     + jnp.where(upper, dot(q_right, k_hat, 1, 1), 0.0)).astype(BF16)
            seed_low = jnp.where(lower, seed_scores, 0.0).astype(BF16)
            seed_up = jnp.where(upper, seed_scores, 0.0).astype(BF16)
            made.append((dot(seed_low, k_left) + dot(seed_up, k_right),
                         dot(seed_low, q_left, 0, 0) + dot(seed_up, q_right, 0, 0),
                         dot(score, seed, 0, 0)))
        for (r, u), (for_q, for_k, for_v) in zip(todo, made):
            intra_q[slot(r, u)] = for_q
            intra_k[slot(r, u)] = for_k
            intra_v[slot(r, u)] = for_v

    def arrived(r, u):
        low, up = (c_out[u, 0, 0], c_out[u, 0, 1]) if r == 0 else (c_in[u, PLACE[r] - 1, 0], c_in[u, PLACE[r] - 1, 1])
        return jnp.where(left_tall, low, up), jnp.where(left_tall, up, low)

    def finish_values(todo):
        made = [intra_v[slot(r, u)] + dot(k_ends[slot(r, u)], arrived(r, u)[1], 1, 1) for r, u in todo]
        for (r, u), block in zip(todo, made):
            d_all[tpi, rows(r, u)] = block.astype(BF16)

    def finish_rest(todo):
        kept, terms = [], []
        for r, u in todo:
            s = slot(r, u)
            state, grad = arrived(r, u)
            c = cum[s]
            end = ends(c)
            grow, shrink, to_end = jnp.exp(c), jnp.exp(-c), jnp.exp(end - c)
            q, k = twice(q_v, r, u), twice(k_v, r, u)
            cross = dot(cot_v[owner(r), u], state)
            dq = grow * (intra_q[s] + cross)
            dk_ = shrink * intra_k[s] + to_end * dot(val[rows(r, u)], grad)
            terms.append(q * dq - k * dk_)
            start = (jnp.sum(q * grow * cross, axis=0, keepdims=True)
                     + jnp.exp(end) * jnp.sum(state.astype(F32) * grad.astype(F32), axis=0, keepdims=True))
            kept.append((dq, dk_, start))
        for (r, u), (dq, dk_, start), sums_ in zip(todo, kept, directed(strict, terms)):
            b = batch_of(r, u)
            decay_grad = start - sums_
            o_q[b] = (dq[:, :dk] + dq[:, dk:]).astype(BF16)
            o_k[b] = (dk_[:, :dk] + dk_[:, dk:]).astype(BF16)
            o_f[b] = decay_grad[:, :dk]
            o_b[b] = decay_grad[:, dk:]

    def finish_own(u):
        finish_values([(0, u)])
        d_copies(0, u, 1)
        finish_rest([(0, u)])

    def features(u):
        take(d_all.at[pl.ds(0, xs), rows(0, u, inner)], f_rs.at[u])
        at = rows(0, u, inner)
        wide = jnp.concatenate([d_all[t, at] for t in range(tp)], 1)
        weights = jnp.concatenate([w_in[t] for t in range(tp)], 1)
        out = dot(wide, weights, 1, 1).astype(BF16)
        for r in range(inner):
            o_h[batch_of(r, u)] = out[PLACE[r] * length:(PLACE[r] + 1) * length]

    def finish_others(todo, u):
        first = PLACE[todo[0]] - 1
        take(c_in.at[u, pl.ds(first, len(todo))], c_rs.at[u, (first + 1) // 2])
        todo = [(r, u) for r in todo]
        finish_values(todo)
        d_copies(*todo[0], len(todo))

    def weight_terms(r, u):
        at = rows(r, u, 2)
        return dot(d_all[tpi, at], hid_v[at], 0, 0)

    def others(u):
        finish_others([2], u)
        finish_others([1, 3], u)
        at = rows(0, u, inner)
        w_acc[...] += dot(d_all[tpi, at], hid_v[at], 0, 0)
        finish_rest([(r, u) for r in range(1, inner)])

    def loop(first, last, step):
        lax.fori_loop(first, last, lambda u, _: step(u) or 0, 0)

    def intra_all(u):
        intra([(r, u) for r in range(inner)])

    def middle_steps(u):
        combine_all(u)
        finish_own(u)
        combine_plane(u + half_own)

    def late_steps(u):
        combine_all(u)
        finish_own(u)
        others(u - half_own)

    half_own, end = own // 2, own - 1
    loop(0, half_own, intra_all)
    take(e_in.at[pl.ds(1, sp - 1)], e_rs.at[0])
    combine_plane(0)
    loop(half_own, own, intra_all)
    loop(1, half_own, combine_plane)
    loop(0, half_own, middle_steps)
    loop(half_own, own, late_steps)
    loop(half_own, end, others)

    finish_others([2], end)
    w_acc[...] += weight_terms(0, end)
    finish_others([1, 3], end)
    full = w_acc[...] + weight_terms(1, end)
    for p in range(0, sp, 2):
        block = full[:, p * rows_sp:(p + 2) * rows_sp].T.astype(BF16)
        g_out[p] = block[:rows_sp]
        g_out[p + 1] = block[rows_sp:]
    for offset in OFFSETS:
        g_copy(*offset).start()
    finish_rest([(r, end) for r in range(1, inner)])
    loop(0, end, forward)
    take(w_in.at[pl.ds(0, tp - 1)], w_rs.at[0])
    loop(0, half_own, features)
    forward(end)
    loop(half_own, own, features)

    take(g_in, g_rs.at[0])
    acc = g_out[spi].astype(F32)
    for r in range(sp - 1):
        acc = acc + g_in[r].astype(F32)
    o_w[...] = acc

    take(w_in.at[pl.ds(0, tp - 1)], w_ss.at[0])
    take(e_in.at[pl.ds(1, sp - 1)], e_ss.at[0])
    take(a_out, a_ss.at[0])
    take(b_in.at[0], b_ss.at[0])
    take(c_in, c_ss.at[0])
    take(d_all.at[pl.ds(0, xs - 1)], d_ss.at[0])
    take(d_all.at[pl.ds(0, xs)], f_ss.at[0])
    take(g_in, g_ss.at[0])


def store_kernel(*refs):
    n = len(refs) // 2
    copies = [pltpu.make_async_copy(refs[i], refs[n + i], refs[-1].at[i]) for i in range(n)]
    for copy in copies:
        copy.start()
    for copy in copies:
        copy.wait()


def store(arrays):
    n = len(arrays)
    return pl.pallas_call(
        store_kernel,
        out_shape=tuple(jax.ShapeDtypeStruct(a.shape, a.dtype) for a in arrays),
        in_specs=[pl.BlockSpec(memory_space=pltpu.VMEM)] * n,
        out_specs=(pl.BlockSpec(memory_space=pl.ANY),) * n,
        scratch_shapes=[pltpu.SemaphoreType.DMA((n,))],
        compiler_params=pltpu.CompilerParams(has_side_effects=True, vmem_limit_bytes=1024 * 1024),
    )(*arrays)


def shards(sp, tp, hidden, value_weight, queries, key_vectors, forward_decay, backward_decay, cotangent):
    batch, length, width = hidden.shape
    heads, dk = queries.shape[1], queries.shape[3]
    dv = value_weight.shape[1]
    assert heads == 1
    inner, outer, own, xs = INNER, sp // INNER, batch // INNER, tp // CORES
    pack, rows, feat, rows_sp = 2 * dk, batch * length, width // tp, width // sp
    dims = (sp, tp, batch, length, dk, dv, width)
    vmem, dma = pltpu.VMEM, pltpu.SemaphoreType.DMA
    scratch = [
        vmem((rows, width), BF16), vmem((width, dv), BF16),
        vmem((inner, own, length, dk), BF16), vmem((inner, own, length, dk), BF16),
        vmem((2, inner, own, length, dk), F32), vmem((inner, own, length, dv), BF16),
        vmem((rows, dv), BF16),
        vmem((batch, length, pack), F32),
        vmem((batch, length, pack), BF16), vmem((batch, length, pack), BF16),
        vmem((batch, length, pack), F32), vmem((batch, length, pack), F32),
        vmem((batch, length, dv), F32),
        vmem((own, 2, inner - 1, dv, pack), BF16), vmem((own, 2, inner, dv, pack), BF16),
        vmem((inner, own, pack), F32), vmem((sp, own, pack), F32),
        vmem((2, inner, own, dv, pack), F32),
        vmem((2, own, dv, pack), BF16), vmem((2, own, outer - 1, dv, pack), BF16),
        vmem((own, inner, 2, dv, pack), BF16), vmem((own, inner - 1, 2, dv, pack), BF16),
        vmem((tp, rows, dv), BF16), vmem((tp, feat, dv), BF16),
        vmem((dv, width), F32),
        vmem((sp, rows_sp, dv), BF16), vmem((sp - 1, rows_sp, dv), BF16),
        dma((8,)), dma((own,)),
        dma((1,)), dma((own,)),
        dma((1,)), dma((1,)),
        dma((1,)), dma((own,)),
        dma((1,)), dma((own, 2)),
        dma((1,)), dma((own, 2)),
        dma((1,)), dma((own,)),
        dma((1,)), dma((1,)),
        dma((1,)), dma((1,)),
    ]
    whole = pl.BlockSpec(memory_space=vmem)
    flat, split = (batch, length, dk), (inner, own, length, dk)
    args = (hidden.reshape(inner, own, length, width), value_weight, queries.reshape(split),
            key_vectors.reshape(split), forward_decay.reshape(split), backward_decay.reshape(split),
            cotangent.reshape(inner, own, length, dv))
    outs = pl.pallas_call(
        functools.partial(kernel, dims),
        out_shape=(
            vmem(flat, BF16), vmem(flat, BF16), vmem(flat, F32), vmem(flat, F32),
            vmem((batch, length, feat), BF16), vmem((rows_sp, dv), F32),
        ),
        in_specs=[pl.BlockSpec(memory_space=pltpu.HBM)] * 7,
        out_specs=(whole,) * 6,
        scratch_shapes=scratch,
        compiler_params=pltpu.CompilerParams(
            collective_id=0, has_side_effects=True, vmem_limit_bytes=48 * 1024 * 1024
        ),
    )(*(pltpu.with_memory_space_constraint(a, pltpu.HBM) for a in args))
    outs = store(outs)
    return tuple(a.reshape(queries.shape) for a in outs[:4]) + tuple(outs[4:])


def solution(mesh):
    heads = P(None, "tp", "sp", None)
    return jax.shard_map(
        functools.partial(shards, mesh.shape["sp"], mesh.shape["tp"]),
        mesh=mesh,
        in_specs=(P(None, "sp", None), P(None, "tp"), heads, heads, heads, heads, P(None, "sp", "tp")),
        out_specs=(heads, heads, heads, heads, P(None, "sp", "tp"), P("sp", "tp")),
        check_vma=False,
    )
```

```python
import functools

import jax
import jax.numpy as jnp
from jax import lax
from jax.experimental import pallas as pl
from jax.experimental.pallas import tpu as pltpu
from jax.sharding import PartitionSpec as P

F32, BF16 = jnp.float32, jnp.bfloat16
MESH = pl.DeviceIdType.MESH
CORES = 2
INNER = 4
TAIL = 16
GRAD, STATE = 0, 1
FAR_FIRST = (2, 1, 3)
OFFSETS = sorted(((dz, dy) for dz in range(4) for dy in range(4) if dz or dy),
                 key=lambda d: -sum(min(v, 4 - v) for v in d))


def dot(a, b, ca=1, cb=0):
    return lax.dot_general(a, b, (((ca,), (cb,)), ((), ())), preferred_element_type=F32)


def halves(x):
    high = x.astype(BF16)
    return jnp.concatenate([high, (x - high.astype(F32)).astype(BF16)], 0)


def kernel(dims, hid, wgt, qry, key, fdec, bdec, cot,
           o_q, o_k, o_f, o_b, o_h, o_w,
           hid_v, wgt_v, q_v, k_v, decay_v, cot_v,
           val, cum, q_hats, k_ends, intra_q, intra_k, intra_v,
           a_out, a_in, e_out, e_in, local, b_out, b_in, c_out, c_in,
           d_all, w_in, w_acc, g_out, g_in,
           i_s, h_s, a_ss, a_rs, e_ss, e_rs, b_ss, b_rs, c_ss, c_rs,
           d_ss, d_rs, f_ss, f_rs, w_ss, w_rs, g_ss, g_rs):
    sp, tp, batch, length, dk, dv, width = dims
    inner, outer, own, xs = INNER, sp // INNER, batch // INNER, tp // CORES
    pack, feat, rows_sp, group = 2 * dk, width // tp, width // sp, INNER * length
    spi, tpi = lax.axis_index("sp"), lax.axis_index("tp")
    z, y = spi // inner, lax.rem(spi, inner)
    x, core = tpi // CORES, lax.rem(tpi, CORES)

    barrier = pltpu.get_barrier_semaphore()
    def owner(r):
        return lax.rem(y + r, inner)

    def batch_of(r, u):
        return owner(r) * own + u

    def slot(r, u):
        return u * inner + r

    def rows(r, u, count=1):
        return pl.ds(pl.multiple_of(slot(r, u) * length, length), count * length)

    def away(dz, dy):
        return lax.rem(z + dz, outer) * inner + lax.rem(y + dy, inner)

    def take(ref, sem):
        pltpu.make_async_copy(ref, ref, sem).wait()

    def load(first, count):
        at, n = pl.ds(first, count), min(first, 1)
        for i in range(2):
            pltpu.make_async_copy((fdec, bdec)[i].at[:, at], decay_v.at[i, :, at], i_s.at[n]).start()
        pltpu.make_async_copy(qry.at[:, at], q_v.at[:, at], i_s.at[2 + n]).start()
        pltpu.make_async_copy(cot.at[:, at], cot_v.at[:, at], i_s.at[4 + n]).start()

    def loaded(first, count):
        at, n = pl.ds(first, count), min(first, 1)
        take(decay_v.at[:, :, at], i_s.at[n])
        take(q_v.at[:, at], i_s.at[2 + n])
        take(cot_v.at[:, at], i_s.at[4 + n])

    def load_hidden(u):
        for r in range(inner):
            pltpu.make_async_copy(hid.at[owner(r), u], hid_v.at[rows(r, u)], h_s.at[u]).start()

    load(0, 1)
    for r in range(1, sp):
        pl.semaphore_signal(barrier, inc=1, device_id={"sp": lax.rem(spi + r, sp)}, device_id_type=MESH)
    for r in range(1, tp):
        pl.semaphore_signal(barrier, inc=1, device_id={"tp": lax.rem(tpi + r, tp)}, device_id_type=MESH)

    pltpu.make_async_copy(wgt, wgt_v, i_s.at[6]).start()
    load_hidden(0)
    pltpu.make_async_copy(key, k_v, i_s.at[7]).start()
    load(1, own - 1)
    for u in range(1, own):
        load_hidden(u)

    def remote(src, dst, ss, rs, **where):
        return pltpu.make_async_remote_copy(src_ref=src, dst_ref=dst, send_sem=ss, recv_sem=rs,
                                            device_id=where, device_id_type=MESH)

    def w_copy(r):
        to = lax.rem(tpi + r, tp)
        return remote(wgt_v.at[pl.ds(pl.multiple_of(to * feat, feat), feat), :], w_in.at[tpi],
                      w_ss.at[0], w_rs.at[0], tp=to)

    def a_copy(kind, r, u):
        return remote(a_out.at[kind, u, r - 1], a_in.at[kind, u, r], a_ss.at[0], a_rs.at[kind, u],
                      sp=z * inner + owner(r))

    def e_copy(r):
        return remote(e_out.at[owner(r)], e_in.at[r], e_ss.at[0], e_rs.at[0], sp=z * inner + owner(r))

    def b_part(ref, kind):
        return ref if kind == GRAD else ref.at[pl.ds(0, dv)]

    def b_copy(kind, r, u):
        return remote(b_part(b_out.at[kind, u], kind), b_part(b_in.at[kind, u, r - 1], kind), b_ss.at[kind],
                      b_rs.at[kind, u], sp=lax.rem(z + r, outer) * inner + y)

    def c_copy(kind, r, u):
        return remote(c_out.at[kind, u, r], c_in.at[kind, u, r - 1], c_ss.at[0], c_rs.at[kind, u],
                      sp=z * inner + lax.rem(y - r + inner, inner))

    mate = x * CORES + 1 - core

    def d_copies(r, u, count):
        at = rows(r, u, count)
        for k in FAR_FIRST:
            remote(d_all.at[tpi, at], d_all.at[tpi, at], d_ss.at[0], d_rs.at[u],
                   tp=lax.rem(x + k, xs) * CORES + core).start()
        remote(d_all.at[tpi, at], d_all.at[tpi, at], f_ss.at[0], f_rs.at[u], tp=mate).start()

    def forward(u):
        at = rows(0, u, inner)
        take(d_all.at[pl.ds(0, xs - 1), at], d_rs.at[u])
        for k in range(1, xs):
            mine = d_all.at[lax.rem(x - k + xs, xs) * CORES + core, at]
            remote(mine, mine, f_ss.at[0], f_rs.at[u], tp=mate).start()

    def g_copy(dz, dy):
        to = away(dz, dy)
        return remote(g_out.at[to], g_in.at[dz * inner + dy - 1], g_ss.at[0], g_rs.at[0], sp=to)

    row = lax.broadcasted_iota(jnp.int32, (length, length), 0)
    col = lax.broadcasted_iota(jnp.int32, (length, length), 1)
    lower, upper = row >= col, row <= col

    def matrix(first, second):
        both = jnp.concatenate([jnp.where(first, 1.0, 0.0), jnp.where(second, 1.0, 0.0)], 0)
        return jnp.concatenate([both, both], 1).astype(BF16)

    sums, strict = matrix(lower, upper), matrix(row > col, row < col)
    left = lax.broadcasted_iota(jnp.int32, (length, pack), 1) < dk
    tail_row = lax.broadcasted_iota(jnp.int32, (TAIL, pack), 0)
    left_tall = lax.broadcasted_iota(jnp.int32, (dv, pack), 1) < dk

    def directed(tri, blocks):
        made = []
        for i in range(0, len(blocks), 2):
            pair = blocks[i:i + 2]
            out = dot(tri, halves(jnp.concatenate(pair, 1) if len(pair) > 1 else pair[0]))
            for n in range(len(pair)):
                part = out[:, n * pack:(n + 1) * pack]
                made.append(jnp.where(left, part[:length], part[length:]))
        return made

    def twice(ref, r, u):
        v = ref[owner(r), u].astype(F32)
        return jnp.concatenate([v, v], 1)

    def ends(c):
        return jnp.where(left[:1], c[length - 1:length], c[0:1])

    def decays(todo):
        blocks = [jnp.concatenate([decay_v[0, owner(r), u], decay_v[1, owner(r), u]], 1) for r, u in todo]
        made = directed(sums, blocks)
        for (r, u), c in zip(todo, made):
            cum[slot(r, u)] = c
        for (r, u), c in zip(todo, made):
            e_out[owner(r), pl.ds(u, 1), :] = ends(c)

    def grads(todo):
        hats = [(twice(q_v, r, u) * jnp.exp(cum[slot(r, u)])).astype(BF16) for r, u in todo]
        made = [dot(cot_v[owner(r), u], hat, 0, 0).astype(BF16) for (r, u), hat in zip(todo, hats)]
        return hats, made

    def states(todo):
        keys = []
        for r, u in todo:
            c = cum[slot(r, u)]
            keys.append((twice(k_v, r, u) * jnp.exp(ends(c) - c)).astype(BF16))
        made = [dot(val[rows(r, u)], k_end, 0, 0).astype(BF16) for (r, u), k_end in zip(todo, keys)]
        return keys, made

    def place(kind, r, u, value):
        if r == 0:
            a_in[kind, u, 0] = value
        else:
            a_out[kind, u, r - 1] = value

    def emit(kind, todo):
        kept, made = (grads if kind == 0 else states)(todo)
        keep = q_hats if kind == 0 else k_ends
        for (r, u), value, block in zip(todo, kept, made):
            keep[slot(r, u)] = value
            place(kind, r, u, block)

    def values(u):
        at = rows(0, u, inner)
        val[at] = dot(hid_v[at], wgt_v[...]).astype(BF16)

    everyone, visitors = tuple(range(inner)), tuple(range(1, inner))

    def send(kind, u):
        for r in FAR_FIRST:
            a_copy(kind, r, u).start()

    loaded(0, 1)
    decays([(r, 0) for r in everyone])
    emit(GRAD, [(r, 0) for r in visitors])
    pl.semaphore_wait(barrier, sp + tp - 2)
    send(GRAD, 0)
    loaded(1, own - 1)
    decays([(r, u) for u in range(1, own) for r in everyone])
    for r in FAR_FIRST:
        e_copy(r).start()
    e_in[0] = e_out[y]
    for u in range(1, own):
        emit(GRAD, [(r, u) for r in visitors])
        send(GRAD, u)

    half_own, end = own // 2, own - 1
    take(wgt_v, i_s.at[6])
    take(k_v, i_s.at[7])
    for u in range(own):
        take(hid_v.at[rows(0, u, inner)], h_s.at[u])
        values(u)
        emit(STATE, [(r, u) for r in visitors])
        if u < half_own:
            send(STATE, u)

    for r in range(1, tp):
        w_copy(r).start()
    w_in[tpi] = wgt_v[pl.ds(pl.multiple_of(tpi * feat, feat), feat), :]
    mine = [(0, u) for u in range(own)]
    emit(GRAD, mine)
    emit(STATE, mine)
    w_acc[...] = jnp.zeros((dv, width), F32)

    def offset(person):
        return lax.rem(y - person + inner, inner)

    def endings(u):
        return [e_in[offset(person), pl.ds(u, 1), :] for person in everyone]

    def pick(kind, ahead, behind):
        at = left_tall if ahead.shape[0] == dv else left[:1]
        return jnp.where(at, ahead, behind) if kind == STATE else jnp.where(at, behind, ahead)

    def running(blocks, factors, order):
        total, before = None, [None] * inner
        for person in order:
            before[person] = jnp.zeros((dv, pack), F32) if total is None else total
            total = blocks[person] if total is None else factors[person] * total + blocks[person]
        return before, total

    def combine_plane(kind, u):
        take(a_in.at[kind, u, pl.ds(1, inner - 1)], a_rs.at[kind, u])
        blocks = [a_in[kind, u, offset(person)].astype(F32) for person in everyone]
        ends_ = endings(u)
        factors = [jnp.exp(e) for e in ends_]
        before, total = running(blocks, factors, everyone)
        after, total_back = running(blocks, factors, everyone[::-1])
        for person in everyone:
            local[kind, u, person] = pick(kind, before[person], after[person])
        b_out[kind, u, pl.ds(0, dv)] = pick(kind, total, total_back).astype(BF16)
        if kind == GRAD:
            whole = sum(ends_[1:], ends_[0])
            high = whole.astype(BF16).astype(F32)
            tail = jnp.where(tail_row == 0, high, jnp.where(tail_row == 1, whole - high, 0.0))
            b_out[kind, u, pl.ds(dv, TAIL)] = tail.astype(BF16)
        for r in FAR_FIRST:
            b_copy(kind, r, u).start()

    def combine_all(kind, u):
        take(b_in.at[GRAD, u] if kind == GRAD else b_in.at[STATE, u, :, pl.ds(0, dv)], b_rs.at[kind, u])
        planes = [None]
        for r in range(1, outer):
            tail = b_in[GRAD, u, r - 1, pl.ds(dv, TAIL)].astype(F32)
            planes.append(tail[0:1] + tail[1:2])
        zero = jnp.zeros((1, pack), F32)
        carried = jnp.zeros((dv, pack), F32)
        for r in range(1, outer):
            q = outer - r
            ahead = jnp.where(z >= r, jnp.exp(sum(planes[1:r], zero)), 0.0)
            behind = jnp.where(z + q < outer, jnp.exp(sum(planes[r + 1:], zero)), 0.0)
            carried = carried + pick(kind, ahead, behind) * b_in[kind, u, r - 1, pl.ds(0, dv)].astype(F32)
        ends_ = endings(u)
        for person in everyone:
            factor = jnp.exp(pick(kind, sum(ends_[:person], zero), sum(ends_[person + 1:], zero)))
            c_out[kind, u, offset(person)] = (factor * carried + local[kind, u, person]).astype(BF16)
        for r in FAR_FIRST:
            c_copy(kind, r, u).start()

    def intra(todo):
        made = []
        for r, u in todo:
            s = slot(r, u)
            q_hat = q_hats[s]
            k_hat = (twice(k_v, r, u) * jnp.exp(-cum[s])).astype(BF16)
            v, seed = val[rows(r, u)], cot_v[owner(r), u]
            seed_scores = dot(seed, v, 1, 1)
            zero = jnp.zeros_like(q_hat)
            q_left, q_right = jnp.where(left, q_hat, zero), jnp.where(left, zero, q_hat)
            k_left, k_right = jnp.where(left, k_hat, zero), jnp.where(left, zero, k_hat)
            score = (jnp.where(lower, dot(q_left, k_hat, 1, 1), 0.0)
                     + jnp.where(upper, dot(q_right, k_hat, 1, 1), 0.0)).astype(BF16)
            seed_low = jnp.where(lower, seed_scores, 0.0).astype(BF16)
            seed_up = jnp.where(upper, seed_scores, 0.0).astype(BF16)
            made.append((dot(seed_low, k_left) + dot(seed_up, k_right),
                         dot(seed_low, q_left, 0, 0) + dot(seed_up, q_right, 0, 0),
                         dot(score, seed, 0, 0)))
        for (r, u), (for_q, for_k, for_v) in zip(todo, made):
            intra_q[slot(r, u)] = for_q
            intra_k[slot(r, u)] = for_k
            intra_v[slot(r, u)] = for_v

    def arrived(kind, r, u):
        return c_out[kind, u, 0] if r == 0 else c_in[kind, u, r - 1]

    def finish_values(todo):
        made = [intra_v[slot(r, u)] + dot(k_ends[slot(r, u)], arrived(GRAD, r, u), 1, 1) for r, u in todo]
        for (r, u), block in zip(todo, made):
            d_all[tpi, rows(r, u)] = block.astype(BF16)

    def finish_rest(todo):
        kept, terms = [], []
        for r, u in todo:
            s = slot(r, u)
            state, grad = arrived(STATE, r, u), arrived(GRAD, r, u)
            c = cum[s]
            end = ends(c)
            grow, shrink, to_end = jnp.exp(c), jnp.exp(-c), jnp.exp(end - c)
            q, k = twice(q_v, r, u), twice(k_v, r, u)
            cross = dot(cot_v[owner(r), u], state)
            dq = grow * (intra_q[s] + cross)
            dk_ = shrink * intra_k[s] + to_end * dot(val[rows(r, u)], grad)
            terms.append(q * dq - k * dk_)
            start = (jnp.sum(q * grow * cross, axis=0, keepdims=True)
                     + jnp.exp(end) * jnp.sum(state.astype(F32) * grad.astype(F32), axis=0, keepdims=True))
            kept.append((dq, dk_, start))
        for (r, u), (dq, dk_, start), sums_ in zip(todo, kept, directed(strict, terms)):
            b = batch_of(r, u)
            decay_grad = start - sums_
            o_q[b] = (dq[:, :dk] + dq[:, dk:]).astype(BF16)
            o_k[b] = (dk_[:, :dk] + dk_[:, dk:]).astype(BF16)
            o_f[b] = decay_grad[:, :dk]
            o_b[b] = decay_grad[:, dk:]

    def features(u):
        take(d_all.at[pl.ds(0, xs), rows(0, u, inner)], f_rs.at[u])
        at = rows(0, u, inner)
        wide = jnp.concatenate([d_all[t, at] for t in range(tp)], 1)
        weights = jnp.concatenate([w_in[t] for t in range(tp)], 1)
        out = dot(wide, weights, 1, 1).astype(BF16)
        for r in range(inner):
            o_h[batch_of(r, u)] = out[r * length:(r + 1) * length]

    def finish_own(u):
        finish_values([(0, u)])
        d_copies(0, u, 1)

    def finish_others(u):
        take(c_in.at[GRAD, u], c_rs.at[GRAD, u])
        finish_values([(r, u) for r in visitors])
        d_copies(1, u, inner - 1)

    def weight_terms(u):
        at = rows(0, u, inner)
        return dot(d_all[tpi, at], hid_v[at], 0, 0)

    def rest_others(u):
        take(c_in.at[STATE, u], c_rs.at[STATE, u])
        finish_rest([(r, u) for r in visitors])

    def loop(first, last, step):
        lax.fori_loop(first, last, lambda u, _: step(u) or 0, 0)

    def intra_all(u):
        intra([(r, u) for r in everyone])

    def first_steps(u):
        combine_plane(GRAD, u)
        intra_all(u)

    def second_steps(u):
        combine_all(GRAD, u)
        finish_own(u)

        @pl.when(u < end)
        def _():
            combine_plane(STATE, u - 1)

    def weigh(u):
        finish_others(u)
        w_acc[...] += weight_terms(u)

    def third_steps(u):
        weigh(u)
        combine_all(STATE, u)
        finish_rest([(0, u)])

    def fourth_steps(u):
        forward(u)
        rest_others(u)
        combine_all(STATE, u + half_own)
        finish_rest([(0, u + half_own)])

    take(e_in.at[pl.ds(1, inner - 1)], e_rs.at[0])
    loop(0, end, first_steps)
    combine_plane(GRAD, end)
    combine_all(GRAD, 0)
    finish_own(0)
    intra_all(end)
    loop(1, own, second_steps)
    loop(half_own, own, lambda u: send(STATE, u))
    loop(0, half_own, third_steps)
    loop(half_own, end, weigh)

    finish_others(end)
    full = w_acc[...] + weight_terms(end)
    for p in range(0, sp, 2):
        block = full[:, p * rows_sp:(p + 2) * rows_sp].T.astype(BF16)
        g_out[p] = block[:rows_sp]
        g_out[p + 1] = block[rows_sp:]
    for away_by in OFFSETS:
        g_copy(*away_by).start()

    loop(half_own, own, lambda u: combine_plane(STATE, u))
    loop(0, half_own, fourth_steps)
    loop(half_own, own, forward)
    take(w_in.at[pl.ds(0, tp - 1)], w_rs.at[0])
    loop(0, end, features)
    loop(half_own, end, rest_others)
    features(end)
    rest_others(end)

    take(g_in, g_rs.at[0])
    acc = g_out[spi].astype(F32)
    for r in range(sp - 1):
        acc = acc + g_in[r].astype(F32)
    o_w[...] = acc

    take(w_in.at[pl.ds(0, tp - 1)], w_ss.at[0])
    take(e_in.at[pl.ds(1, inner - 1)], e_ss.at[0])
    take(a_out, a_ss.at[0])
    take(b_in.at[GRAD], b_ss.at[GRAD])
    take(b_in.at[STATE, :, :, pl.ds(0, dv)], b_ss.at[STATE])
    take(c_in, c_ss.at[0])
    take(d_all.at[pl.ds(0, xs - 1)], d_ss.at[0])
    take(d_all.at[pl.ds(0, xs)], f_ss.at[0])
    take(g_in, g_ss.at[0])


def store_kernel(*refs):
    n = len(refs) // 2
    copies = [pltpu.make_async_copy(refs[i], refs[n + i], refs[-1].at[i]) for i in range(n)]
    for copy in copies:
        copy.start()
    for copy in copies:
        copy.wait()


def store(arrays):
    n = len(arrays)
    return pl.pallas_call(
        store_kernel,
        out_shape=tuple(jax.ShapeDtypeStruct(a.shape, a.dtype) for a in arrays),
        in_specs=[pl.BlockSpec(memory_space=pltpu.VMEM)] * n,
        out_specs=(pl.BlockSpec(memory_space=pl.ANY),) * n,
        scratch_shapes=[pltpu.SemaphoreType.DMA((n,))],
        compiler_params=pltpu.CompilerParams(has_side_effects=True, vmem_limit_bytes=1024 * 1024),
    )(*arrays)


def shards(sp, tp, hidden, value_weight, queries, key_vectors, forward_decay, backward_decay, cotangent):
    batch, length, width = hidden.shape
    heads, dk = queries.shape[1], queries.shape[3]
    dv = value_weight.shape[1]
    assert heads == 1
    inner, outer, own, xs = INNER, sp // INNER, batch // INNER, tp // CORES
    pack, rows, feat, rows_sp = 2 * dk, batch * length, width // tp, width // sp
    dims = (sp, tp, batch, length, dk, dv, width)
    vmem, dma = pltpu.VMEM, pltpu.SemaphoreType.DMA
    scratch = [
        vmem((rows, width), BF16), vmem((width, dv), BF16),
        vmem((inner, own, length, dk), BF16), vmem((inner, own, length, dk), BF16),
        vmem((2, inner, own, length, dk), F32), vmem((inner, own, length, dv), BF16),
        vmem((rows, dv), BF16),
        vmem((batch, length, pack), F32),
        vmem((batch, length, pack), BF16), vmem((batch, length, pack), BF16),
        vmem((batch, length, pack), F32), vmem((batch, length, pack), F32),
        vmem((batch, length, dv), F32),
        vmem((2, own, inner - 1, dv, pack), BF16), vmem((2, own, inner, dv, pack), BF16),
        vmem((inner, own, pack), F32), vmem((inner, own, pack), F32),
        vmem((2, own, inner, dv, pack), F32),
        vmem((2, own, dv + TAIL, pack), BF16), vmem((2, own, outer - 1, dv + TAIL, pack), BF16),
        vmem((2, own, inner, dv, pack), BF16), vmem((2, own, inner - 1, dv, pack), BF16),
        vmem((tp, rows, dv), BF16), vmem((tp, feat, dv), BF16),
        vmem((dv, width), F32),
        vmem((sp, rows_sp, dv), BF16), vmem((sp - 1, rows_sp, dv), BF16),
        dma((8,)), dma((own,)),
        dma((1,)), dma((2, own)),
        dma((1,)), dma((1,)),
        dma((2,)), dma((2, own)),
        dma((1,)), dma((2, own)),
        dma((1,)), dma((own,)),
        dma((1,)), dma((own,)),
        dma((1,)), dma((1,)),
        dma((1,)), dma((1,)),
    ]
    whole = pl.BlockSpec(memory_space=vmem)
    flat, split = (batch, length, dk), (inner, own, length, dk)
    args = (hidden.reshape(inner, own, length, width), value_weight, queries.reshape(split),
            key_vectors.reshape(split), forward_decay.reshape(split), backward_decay.reshape(split),
            cotangent.reshape(inner, own, length, dv))
    outs = pl.pallas_call(
        functools.partial(kernel, dims),
        out_shape=(
            vmem(flat, BF16), vmem(flat, BF16), vmem(flat, F32), vmem(flat, F32),
            vmem((batch, length, feat), BF16), vmem((rows_sp, dv), F32),
        ),
        in_specs=[pl.BlockSpec(memory_space=pltpu.HBM)] * 7,
        out_specs=(whole,) * 6,
        scratch_shapes=scratch,
        compiler_params=pltpu.CompilerParams(
            collective_id=0, has_side_effects=True, vmem_limit_bytes=48 * 1024 * 1024
        ),
    )(*(pltpu.with_memory_space_constraint(a, pltpu.HBM) for a in args))
    outs = store(outs)
    return tuple(a.reshape(queries.shape) for a in outs[:4]) + tuple(outs[4:])


def solution(mesh):
    heads = P(None, "tp", "sp", None)
    return jax.shard_map(
        functools.partial(shards, mesh.shape["sp"], mesh.shape["tp"]),
        mesh=mesh,
        in_specs=(P(None, "sp", None), P(None, "tp"), heads, heads, heads, heads, P(None, "sp", "tp")),
        out_specs=(heads, heads, heads, heads, P(None, "sp", "tp"), P("sp", "tp")),
        check_vma=False,
    )
```

```python
import functools

import jax
import jax.numpy as jnp
from jax import lax
from jax.experimental import pallas as pl
from jax.experimental.pallas import tpu as pltpu
from jax.sharding import PartitionSpec as P

F32, BF16 = jnp.float32, jnp.bfloat16
MESH = pl.DeviceIdType.MESH
CORES = 2
INNER = 4
TAIL = 16
GRAD, STATE = 0, 1
FAR_FIRST = (2, 1, 3)
OFFSETS = sorted(((dz, dy) for dz in range(4) for dy in range(4) if dz or dy),
                 key=lambda d: -sum(min(v, 4 - v) for v in d))


def dot(a, b, ca=1, cb=0):
    return lax.dot_general(a, b, (((ca,), (cb,)), ((), ())), preferred_element_type=F32)


def halves(x):
    high = x.astype(BF16)
    return jnp.concatenate([high, (x - high.astype(F32)).astype(BF16)], 0)


def kernel(dims, hid, wgt, qry, key, fdec, bdec, cot,
           o_q, o_k, o_f, o_b, o_h, o_w,
           hid_v, wgt_v, q_v, k_v, decay_v, cot_v,
           val, cum, q_hats, k_ends, intra_q, intra_k, intra_v,
           a_out, a_in, e_out, e_in, local, b_out, b_in, c_out, c_in,
           d_all, w_in, w_acc, g_out, g_in,
           i_s, h_s, a_ss, a_rs, e_ss, e_rs, b_ss, b_rs, c_ss, c_rs,
           d_ss, d_rs, f_ss, f_rs, w_ss, w_rs, g_ss, g_rs):
    sp, tp, batch, length, dk, dv, width = dims
    inner, outer, own, xs = INNER, sp // INNER, batch // INNER, tp // CORES
    pack, feat, rows_sp, group = 2 * dk, width // tp, width // sp, INNER * length
    spi, tpi = lax.axis_index("sp"), lax.axis_index("tp")
    z, y = spi // inner, lax.rem(spi, inner)
    x, core = tpi // CORES, lax.rem(tpi, CORES)

    barrier = pltpu.get_barrier_semaphore()
    def owner(r):
        return lax.rem(y + r, inner)

    def batch_of(r, u):
        return owner(r) * own + u

    def slot(r, u):
        return u * inner + r

    def rows(r, u, count=1):
        return pl.ds(pl.multiple_of(slot(r, u) * length, length), count * length)

    def away(dz, dy):
        return lax.rem(z + dz, outer) * inner + lax.rem(y + dy, inner)

    def take(ref, sem):
        pltpu.make_async_copy(ref, ref, sem).wait()

    def load(first, count):
        at, n = pl.ds(first, count), min(first, 1)
        for i in range(2):
            pltpu.make_async_copy((fdec, bdec)[i].at[:, at], decay_v.at[i, :, at], i_s.at[n]).start()
        pltpu.make_async_copy(qry.at[:, at], q_v.at[:, at], i_s.at[2 + n]).start()
        pltpu.make_async_copy(cot.at[:, at], cot_v.at[:, at], i_s.at[4 + n]).start()

    def loaded(first, count):
        at, n = pl.ds(first, count), min(first, 1)
        take(decay_v.at[:, :, at], i_s.at[n])
        take(q_v.at[:, at], i_s.at[2 + n])
        take(cot_v.at[:, at], i_s.at[4 + n])

    def load_hidden(u):
        for r in range(inner):
            pltpu.make_async_copy(hid.at[owner(r), u], hid_v.at[rows(r, u)], h_s.at[u]).start()

    load(0, 1)
    for r in range(1, sp):
        pl.semaphore_signal(barrier, inc=1, device_id={"sp": lax.rem(spi + r, sp)}, device_id_type=MESH)
    for r in range(1, tp):
        pl.semaphore_signal(barrier, inc=1, device_id={"tp": lax.rem(tpi + r, tp)}, device_id_type=MESH)

    pltpu.make_async_copy(wgt, wgt_v, i_s.at[6]).start()
    load_hidden(0)
    pltpu.make_async_copy(key, k_v, i_s.at[7]).start()
    load(1, own - 1)
    for u in range(1, own):
        load_hidden(u)

    def remote(src, dst, ss, rs, **where):
        return pltpu.make_async_remote_copy(src_ref=src, dst_ref=dst, send_sem=ss, recv_sem=rs,
                                            device_id=where, device_id_type=MESH)

    def w_copy(r):
        to = lax.rem(tpi + r, tp)
        return remote(wgt_v.at[pl.ds(pl.multiple_of(to * feat, feat), feat), :], w_in.at[tpi],
                      w_ss.at[0], w_rs.at[0], tp=to)

    def a_copy(kind, r, u):
        return remote(a_out.at[kind, u, r - 1], a_in.at[kind, u, r], a_ss.at[0], a_rs.at[kind, u],
                      sp=z * inner + owner(r))

    def e_copy(r):
        return remote(e_out.at[owner(r)], e_in.at[r], e_ss.at[0], e_rs.at[0], sp=z * inner + owner(r))

    def b_part(ref, kind):
        return ref if kind == GRAD else ref.at[pl.ds(0, dv)]

    def b_copy(kind, r, u):
        return remote(b_part(b_out.at[kind, u], kind), b_part(b_in.at[kind, u, r - 1], kind), b_ss.at[kind],
                      b_rs.at[kind, u], sp=lax.rem(z + r, outer) * inner + y)

    def c_copy(kind, r, u):
        return remote(c_out.at[kind, u, r], c_in.at[kind, u, r - 1], c_ss.at[0], c_rs.at[kind, u],
                      sp=z * inner + lax.rem(y - r + inner, inner))

    mate = x * CORES + 1 - core

    def d_copies(r, u, count):
        at = rows(r, u, count)
        for k in FAR_FIRST:
            remote(d_all.at[tpi, at], d_all.at[tpi, at], d_ss.at[0], d_rs.at[u],
                   tp=lax.rem(x + k, xs) * CORES + core).start()
        remote(d_all.at[tpi, at], d_all.at[tpi, at], f_ss.at[0], f_rs.at[u], tp=mate).start()

    def forward(u):
        at = rows(0, u, inner)
        take(d_all.at[pl.ds(0, xs - 1), at], d_rs.at[u])
        for k in range(1, xs):
            mine = d_all.at[lax.rem(x - k + xs, xs) * CORES + core, at]
            remote(mine, mine, f_ss.at[0], f_rs.at[u], tp=mate).start()

    def g_copy(dz, dy):
        to = away(dz, dy)
        return remote(g_out.at[to], g_in.at[dz * inner + dy - 1], g_ss.at[0], g_rs.at[0], sp=to)

    row = lax.broadcasted_iota(jnp.int32, (length, length), 0)
    col = lax.broadcasted_iota(jnp.int32, (length, length), 1)
    lower, upper = row >= col, row <= col

    def matrix(first, second):
        both = jnp.concatenate([jnp.where(first, 1.0, 0.0), jnp.where(second, 1.0, 0.0)], 0)
        return jnp.concatenate([both, both], 1).astype(BF16)

    sums, strict = matrix(lower, upper), matrix(row > col, row < col)
    left = lax.broadcasted_iota(jnp.int32, (length, pack), 1) < dk
    tail_row = lax.broadcasted_iota(jnp.int32, (TAIL, pack), 0)
    left_tall = lax.broadcasted_iota(jnp.int32, (dv, pack), 1) < dk

    def directed(tri, blocks):
        made = []
        for i in range(0, len(blocks), 2):
            pair = blocks[i:i + 2]
            out = dot(tri, halves(jnp.concatenate(pair, 1) if len(pair) > 1 else pair[0]))
            for n in range(len(pair)):
                part = out[:, n * pack:(n + 1) * pack]
                made.append(jnp.where(left, part[:length], part[length:]))
        return made

    def twice(ref, r, u):
        v = ref[owner(r), u].astype(F32)
        return jnp.concatenate([v, v], 1)

    def ends(c):
        return jnp.where(left[:1], c[length - 1:length], c[0:1])

    def decays(todo):
        blocks = [jnp.concatenate([decay_v[0, owner(r), u], decay_v[1, owner(r), u]], 1) for r, u in todo]
        made = directed(sums, blocks)
        for (r, u), c in zip(todo, made):
            cum[slot(r, u)] = c
        for (r, u), c in zip(todo, made):
            e_out[owner(r), pl.ds(u, 1), :] = ends(c)

    def grads(todo):
        hats = [(twice(q_v, r, u) * jnp.exp(cum[slot(r, u)])).astype(BF16) for r, u in todo]
        made = [dot(cot_v[owner(r), u], hat, 0, 0).astype(BF16) for (r, u), hat in zip(todo, hats)]
        return hats, made

    def states(todo):
        keys = []
        for r, u in todo:
            c = cum[slot(r, u)]
            keys.append((twice(k_v, r, u) * jnp.exp(ends(c) - c)).astype(BF16))
        made = [dot(val[rows(r, u)], k_end, 0, 0).astype(BF16) for (r, u), k_end in zip(todo, keys)]
        return keys, made

    def place(kind, r, u, value):
        if r == 0:
            a_in[kind, u, 0] = value
        else:
            a_out[kind, u, r - 1] = value

    def emit(kind, todo):
        kept, made = (grads if kind == 0 else states)(todo)
        keep = q_hats if kind == 0 else k_ends
        for (r, u), value, block in zip(todo, kept, made):
            keep[slot(r, u)] = value
            place(kind, r, u, block)

    def values(u):
        at = rows(0, u, inner)
        val[at] = dot(hid_v[at], wgt_v[...]).astype(BF16)

    everyone, visitors = tuple(range(inner)), tuple(range(1, inner))

    def send(kind, u):
        for r in FAR_FIRST:
            a_copy(kind, r, u).start()

    loaded(0, 1)
    decays([(r, 0) for r in everyone])
    emit(GRAD, [(r, 0) for r in visitors])
    pl.semaphore_wait(barrier, sp + tp - 2)
    send(GRAD, 0)
    loaded(1, own - 1)
    decays([(r, u) for u in range(1, own) for r in everyone])
    for r in FAR_FIRST:
        e_copy(r).start()
    e_in[0] = e_out[y]
    for u in range(1, own):
        emit(GRAD, [(r, u) for r in visitors])
        send(GRAD, u)

    end = own - 1
    take(wgt_v, i_s.at[6])
    take(k_v, i_s.at[7])
    for u in range(own):
        take(hid_v.at[rows(0, u, inner)], h_s.at[u])
        values(u)
        emit(STATE, [(r, u) for r in visitors])
        if u < end:
            send(STATE, u)

    for r in range(1, tp):
        w_copy(r).start()
    w_in[tpi] = wgt_v[pl.ds(pl.multiple_of(tpi * feat, feat), feat), :]
    mine = [(0, u) for u in range(own)]
    emit(GRAD, mine)
    emit(STATE, mine)
    w_acc[...] = jnp.zeros((dv, width), F32)

    def offset(person):
        return lax.rem(y - person + inner, inner)

    def endings(u):
        return [e_in[offset(person), pl.ds(u, 1), :] for person in everyone]

    def pick(kind, ahead, behind):
        at = left_tall if ahead.shape[0] == dv else left[:1]
        return jnp.where(at, ahead, behind) if kind == STATE else jnp.where(at, behind, ahead)

    def running(blocks, factors, order):
        total, before = None, [None] * inner
        for person in order:
            before[person] = jnp.zeros((dv, pack), F32) if total is None else total
            total = blocks[person] if total is None else factors[person] * total + blocks[person]
        return before, total

    def combine_plane(kind, u):
        take(a_in.at[kind, u, pl.ds(1, inner - 1)], a_rs.at[kind, u])
        blocks = [a_in[kind, u, offset(person)].astype(F32) for person in everyone]
        ends_ = endings(u)
        factors = [jnp.exp(e) for e in ends_]
        before, total = running(blocks, factors, everyone)
        after, total_back = running(blocks, factors, everyone[::-1])
        for person in everyone:
            local[kind, u, person] = pick(kind, before[person], after[person])
        b_out[kind, u, pl.ds(0, dv)] = pick(kind, total, total_back).astype(BF16)
        if kind == GRAD:
            whole = sum(ends_[1:], ends_[0])
            high = whole.astype(BF16).astype(F32)
            tail = jnp.where(tail_row == 0, high, jnp.where(tail_row == 1, whole - high, 0.0))
            b_out[kind, u, pl.ds(dv, TAIL)] = tail.astype(BF16)
        for r in FAR_FIRST:
            b_copy(kind, r, u).start()

    def combine_all(kind, u):
        take(b_in.at[GRAD, u] if kind == GRAD else b_in.at[STATE, u, :, pl.ds(0, dv)], b_rs.at[kind, u])
        planes = [None]
        for r in range(1, outer):
            tail = b_in[GRAD, u, r - 1, pl.ds(dv, TAIL)].astype(F32)
            planes.append(tail[0:1] + tail[1:2])
        zero = jnp.zeros((1, pack), F32)
        carried = jnp.zeros((dv, pack), F32)
        for r in range(1, outer):
            q = outer - r
            ahead = jnp.where(z >= r, jnp.exp(sum(planes[1:r], zero)), 0.0)
            behind = jnp.where(z + q < outer, jnp.exp(sum(planes[r + 1:], zero)), 0.0)
            carried = carried + pick(kind, ahead, behind) * b_in[kind, u, r - 1, pl.ds(0, dv)].astype(F32)
        ends_ = endings(u)
        for person in everyone:
            factor = jnp.exp(pick(kind, sum(ends_[:person], zero), sum(ends_[person + 1:], zero)))
            c_out[kind, u, offset(person)] = (factor * carried + local[kind, u, person]).astype(BF16)
        for r in FAR_FIRST:
            c_copy(kind, r, u).start()

    def intra(todo):
        made = []
        for r, u in todo:
            s = slot(r, u)
            q_hat = q_hats[s]
            k_hat = (twice(k_v, r, u) * jnp.exp(-cum[s])).astype(BF16)
            v, seed = val[rows(r, u)], cot_v[owner(r), u]
            seed_scores = dot(seed, v, 1, 1)
            zero = jnp.zeros_like(q_hat)
            q_left, q_right = jnp.where(left, q_hat, zero), jnp.where(left, zero, q_hat)
            k_left, k_right = jnp.where(left, k_hat, zero), jnp.where(left, zero, k_hat)
            score = (jnp.where(lower, dot(q_left, k_hat, 1, 1), 0.0)
                     + jnp.where(upper, dot(q_right, k_hat, 1, 1), 0.0)).astype(BF16)
            seed_low = jnp.where(lower, seed_scores, 0.0).astype(BF16)
            seed_up = jnp.where(upper, seed_scores, 0.0).astype(BF16)
            made.append((dot(seed_low, k_left) + dot(seed_up, k_right),
                         dot(seed_low, q_left, 0, 0) + dot(seed_up, q_right, 0, 0),
                         dot(score, seed, 0, 0)))
        for (r, u), (for_q, for_k, for_v) in zip(todo, made):
            intra_q[slot(r, u)] = for_q
            intra_k[slot(r, u)] = for_k
            intra_v[slot(r, u)] = for_v

    def arrived(kind, r, u):
        return c_out[kind, u, 0] if r == 0 else c_in[kind, u, r - 1]

    def finish_values(todo):
        made = [intra_v[slot(r, u)] + dot(k_ends[slot(r, u)], arrived(GRAD, r, u), 1, 1) for r, u in todo]
        for (r, u), block in zip(todo, made):
            d_all[tpi, rows(r, u)] = block.astype(BF16)

    def finish_rest(todo):
        kept, terms = [], []
        for r, u in todo:
            s = slot(r, u)
            state, grad = arrived(STATE, r, u), arrived(GRAD, r, u)
            c = cum[s]
            end = ends(c)
            grow, shrink, to_end = jnp.exp(c), jnp.exp(-c), jnp.exp(end - c)
            q, k = twice(q_v, r, u), twice(k_v, r, u)
            cross = dot(cot_v[owner(r), u], state)
            dq = grow * (intra_q[s] + cross)
            dk_ = shrink * intra_k[s] + to_end * dot(val[rows(r, u)], grad)
            terms.append(q * dq - k * dk_)
            start = (jnp.sum(q * grow * cross, axis=0, keepdims=True)
                     + jnp.exp(end) * jnp.sum(state.astype(F32) * grad.astype(F32), axis=0, keepdims=True))
            kept.append((dq, dk_, start))
        for (r, u), (dq, dk_, start), sums_ in zip(todo, kept, directed(strict, terms)):
            b = batch_of(r, u)
            decay_grad = start - sums_
            o_q[b] = (dq[:, :dk] + dq[:, dk:]).astype(BF16)
            o_k[b] = (dk_[:, :dk] + dk_[:, dk:]).astype(BF16)
            o_f[b] = decay_grad[:, :dk]
            o_b[b] = decay_grad[:, dk:]

    def features(u):
        take(d_all.at[pl.ds(0, xs), rows(0, u, inner)], f_rs.at[u])
        at = rows(0, u, inner)
        wide = jnp.concatenate([d_all[t, at] for t in range(tp)], 1)
        weights = jnp.concatenate([w_in[t] for t in range(tp)], 1)
        out = dot(wide, weights, 1, 1).astype(BF16)
        for r in range(inner):
            o_h[batch_of(r, u)] = out[r * length:(r + 1) * length]

    def finish_own(u):
        finish_values([(0, u)])
        d_copies(0, u, 1)

    def finish_others(u):
        take(c_in.at[GRAD, u], c_rs.at[GRAD, u])
        finish_values([(r, u) for r in visitors])
        d_copies(1, u, inner - 1)

    def weight_terms(u):
        at = rows(0, u, inner)
        return dot(d_all[tpi, at], hid_v[at], 0, 0)

    def rest_others(u):
        take(c_in.at[STATE, u], c_rs.at[STATE, u])
        finish_rest([(r, u) for r in visitors])

    def loop(first, last, step):
        lax.fori_loop(first, last, lambda u, _: step(u) or 0, 0)

    def intra_all(u):
        intra([(r, u) for r in everyone])

    def first_steps(u):
        combine_plane(GRAD, u)
        intra_all(u)

    def second_steps(u):
        combine_all(GRAD, u)
        finish_own(u)
        combine_plane(STATE, u - 1)

    def weigh(u):
        finish_others(u)
        w_acc[...] += weight_terms(u)

    def pass_states(u):
        combine_all(STATE, u)
        finish_rest([(0, u)])

    def third_steps(u):
        weigh(u)
        pass_states(u)

    def fourth_steps(u):
        forward(u)
        rest_others(u)

    take(e_in.at[pl.ds(1, inner - 1)], e_rs.at[0])
    loop(0, end, first_steps)
    combine_plane(GRAD, end)
    combine_all(GRAD, 0)
    send(STATE, end)
    finish_own(0)
    intra_all(end)
    loop(1, own, second_steps)
    weigh(0)
    combine_plane(STATE, end)
    pass_states(0)
    loop(1, end, third_steps)

    finish_others(end)
    full = w_acc[...] + weight_terms(end)
    for p in range(0, sp, 2):
        block = full[:, p * rows_sp:(p + 2) * rows_sp].T.astype(BF16)
        g_out[p] = block[:rows_sp]
        g_out[p + 1] = block[rows_sp:]
    for away_by in OFFSETS:
        g_copy(*away_by).start()

    pass_states(end)
    loop(0, end, fourth_steps)
    forward(end)
    take(w_in.at[pl.ds(0, tp - 1)], w_rs.at[0])
    loop(0, end, features)
    rest_others(end)
    features(end)

    take(g_in, g_rs.at[0])
    acc = g_out[spi].astype(F32)
    for r in range(sp - 1):
        acc = acc + g_in[r].astype(F32)
    o_w[...] = acc

    take(w_in.at[pl.ds(0, tp - 1)], w_ss.at[0])
    take(e_in.at[pl.ds(1, inner - 1)], e_ss.at[0])
    take(a_out, a_ss.at[0])
    take(b_in.at[GRAD], b_ss.at[GRAD])
    take(b_in.at[STATE, :, :, pl.ds(0, dv)], b_ss.at[STATE])
    take(c_in, c_ss.at[0])
    take(d_all.at[pl.ds(0, xs - 1)], d_ss.at[0])
    take(d_all.at[pl.ds(0, xs)], f_ss.at[0])
    take(g_in, g_ss.at[0])


def store_kernel(*refs):
    n = len(refs) // 2
    copies = [pltpu.make_async_copy(refs[i], refs[n + i], refs[-1].at[i]) for i in range(n)]
    for copy in copies:
        copy.start()
    for copy in copies:
        copy.wait()


def store(arrays):
    n = len(arrays)
    return pl.pallas_call(
        store_kernel,
        out_shape=tuple(jax.ShapeDtypeStruct(a.shape, a.dtype) for a in arrays),
        in_specs=[pl.BlockSpec(memory_space=pltpu.VMEM)] * n,
        out_specs=(pl.BlockSpec(memory_space=pl.ANY),) * n,
        scratch_shapes=[pltpu.SemaphoreType.DMA((n,))],
        compiler_params=pltpu.CompilerParams(has_side_effects=True, vmem_limit_bytes=1024 * 1024),
    )(*arrays)


def shards(sp, tp, hidden, value_weight, queries, key_vectors, forward_decay, backward_decay, cotangent):
    batch, length, width = hidden.shape
    heads, dk = queries.shape[1], queries.shape[3]
    dv = value_weight.shape[1]
    assert heads == 1
    inner, outer, own, xs = INNER, sp // INNER, batch // INNER, tp // CORES
    pack, rows, feat, rows_sp = 2 * dk, batch * length, width // tp, width // sp
    dims = (sp, tp, batch, length, dk, dv, width)
    vmem, dma = pltpu.VMEM, pltpu.SemaphoreType.DMA
    scratch = [
        vmem((rows, width), BF16), vmem((width, dv), BF16),
        vmem((inner, own, length, dk), BF16), vmem((inner, own, length, dk), BF16),
        vmem((2, inner, own, length, dk), F32), vmem((inner, own, length, dv), BF16),
        vmem((rows, dv), BF16),
        vmem((batch, length, pack), F32),
        vmem((batch, length, pack), BF16), vmem((batch, length, pack), BF16),
        vmem((batch, length, pack), F32), vmem((batch, length, pack), F32),
        vmem((batch, length, dv), F32),
        vmem((2, own, inner - 1, dv, pack), BF16), vmem((2, own, inner, dv, pack), BF16),
        vmem((inner, own, pack), F32), vmem((inner, own, pack), F32),
        vmem((2, own, inner, dv, pack), F32),
        vmem((2, own, dv + TAIL, pack), BF16), vmem((2, own, outer - 1, dv + TAIL, pack), BF16),
        vmem((2, own, inner, dv, pack), BF16), vmem((2, own, inner - 1, dv, pack), BF16),
        vmem((tp, rows, dv), BF16), vmem((tp, feat, dv), BF16),
        vmem((dv, width), F32),
        vmem((sp, rows_sp, dv), BF16), vmem((sp - 1, rows_sp, dv), BF16),
        dma((8,)), dma((own,)),
        dma((1,)), dma((2, own)),
        dma((1,)), dma((1,)),
        dma((2,)), dma((2, own)),
        dma((1,)), dma((2, own)),
        dma((1,)), dma((own,)),
        dma((1,)), dma((own,)),
        dma((1,)), dma((1,)),
        dma((1,)), dma((1,)),
    ]
    whole = pl.BlockSpec(memory_space=vmem)
    flat, split = (batch, length, dk), (inner, own, length, dk)
    args = (hidden.reshape(inner, own, length, width), value_weight, queries.reshape(split),
            key_vectors.reshape(split), forward_decay.reshape(split), backward_decay.reshape(split),
            cotangent.reshape(inner, own, length, dv))
    outs = pl.pallas_call(
        functools.partial(kernel, dims),
        out_shape=(
            vmem(flat, BF16), vmem(flat, BF16), vmem(flat, F32), vmem(flat, F32),
            vmem((batch, length, feat), BF16), vmem((rows_sp, dv), F32),
        ),
        in_specs=[pl.BlockSpec(memory_space=pltpu.HBM)] * 7,
        out_specs=(whole,) * 6,
        scratch_shapes=scratch,
        compiler_params=pltpu.CompilerParams(
            collective_id=0, has_side_effects=True, vmem_limit_bytes=48 * 1024 * 1024
        ),
    )(*(pltpu.with_memory_space_constraint(a, pltpu.HBM) for a in args))
    outs = store(outs)
    return tuple(a.reshape(queries.shape) for a in outs[:4]) + tuple(outs[4:])


def solution(mesh):
    heads = P(None, "tp", "sp", None)
    return jax.shard_map(
        functools.partial(shards, mesh.shape["sp"], mesh.shape["tp"]),
        mesh=mesh,
        in_specs=(P(None, "sp", None), P(None, "tp"), heads, heads, heads, heads, P(None, "sp", "tp")),
        out_specs=(heads, heads, heads, heads, P(None, "sp", "tp"), P("sp", "tp")),
        check_vma=False,
    )
```

```python
import functools

import jax
import jax.numpy as jnp
from jax import lax
from jax.experimental import pallas as pl
from jax.experimental.pallas import tpu as pltpu
from jax.sharding import PartitionSpec as P

F32, BF16 = jnp.float32, jnp.bfloat16
MESH = pl.DeviceIdType.MESH
CORES = 2
INNER = 4
TAIL = 16
GRAD, STATE = 0, 1
FAR_FIRST = (2, 1, 3)
OFFSETS = sorted(((dz, dy) for dz in range(4) for dy in range(4) if dz or dy),
                 key=lambda d: -sum(min(v, 4 - v) for v in d))


def dot(a, b, ca=1, cb=0):
    return lax.dot_general(a, b, (((ca,), (cb,)), ((), ())), preferred_element_type=F32)


def halves(x):
    high = x.astype(BF16)
    return jnp.concatenate([high, (x - high.astype(F32)).astype(BF16)], 0)


def kernel(dims, hid, wgt, qry, key, fdec, bdec, cot,
           o_q, o_k, o_f, o_b, o_h, o_w,
           hid_v, wgt_v, q_v, k_v, decay_v, cot_v,
           val, cum, q_hats, k_ends, intra_q, intra_k, intra_v,
           a_out, a_in, e_out, e_in, local, b_out, b_in, c_out, c_in,
           d_all, w_in, w_acc, g_out, g_in,
           i_s, h_s, a_ss, a_rs, e_ss, e_rs, b_ss, b_rs, c_ss, c_rs,
           d_ss, d_rs, f_ss, f_rs, w_ss, w_rs, g_ss, g_rs):
    sp, tp, batch, length, dk, dv, width = dims
    inner, outer, own, xs = INNER, sp // INNER, batch // INNER, tp // CORES
    pack, feat, rows_sp, group = 2 * dk, width // tp, width // sp, INNER * length
    fold = dv // 2
    spi, tpi = lax.axis_index("sp"), lax.axis_index("tp")
    z, y = spi // inner, lax.rem(spi, inner)
    x, core = tpi // CORES, lax.rem(tpi, CORES)

    barrier = pltpu.get_barrier_semaphore()
    def owner(r):
        return lax.rem(y + r, inner)

    def batch_of(r, u):
        return owner(r) * own + u

    def slot(r, u):
        return u * inner + r

    def rows(r, u, count=1):
        return pl.ds(pl.multiple_of(slot(r, u) * length, length), count * length)

    def away(dz, dy):
        return lax.rem(z + dz, outer) * inner + lax.rem(y + dy, inner)

    def take(ref, sem):
        pltpu.make_async_copy(ref, ref, sem).wait()

    def load(first, count):
        at, n = pl.ds(first, count), min(first, 1)
        for i in range(2):
            pltpu.make_async_copy((fdec, bdec)[i].at[:, at], decay_v.at[i, :, at], i_s.at[n]).start()
        pltpu.make_async_copy(qry.at[:, at], q_v.at[:, at], i_s.at[2 + n]).start()
        pltpu.make_async_copy(cot.at[:, at], cot_v.at[:, at], i_s.at[4 + n]).start()

    def loaded(first, count):
        at, n = pl.ds(first, count), min(first, 1)
        take(decay_v.at[:, :, at], i_s.at[n])
        take(q_v.at[:, at], i_s.at[2 + n])
        take(cot_v.at[:, at], i_s.at[4 + n])

    def load_hidden(u):
        for r in range(inner):
            pltpu.make_async_copy(hid.at[owner(r), u], hid_v.at[rows(r, u)], h_s.at[u]).start()

    load(0, 1)
    for r in range(1, outer):
        pl.semaphore_signal(barrier, inc=1, device_id={"sp": away(r, 0)}, device_id_type=MESH)
    for r in range(1, inner):
        pl.semaphore_signal(barrier, inc=1, device_id={"sp": away(0, r)}, device_id_type=MESH)
    for r in range(1, tp):
        pl.semaphore_signal(barrier, inc=1, device_id={"tp": lax.rem(tpi + r, tp)}, device_id_type=MESH)

    pltpu.make_async_copy(wgt, wgt_v, i_s.at[6]).start()
    load_hidden(0)
    pltpu.make_async_copy(key, k_v, i_s.at[7]).start()
    load(1, own - 1)
    for u in range(1, own):
        load_hidden(u)

    def remote(src, dst, ss, rs, **where):
        return pltpu.make_async_remote_copy(src_ref=src, dst_ref=dst, send_sem=ss, recv_sem=rs,
                                            device_id=where, device_id_type=MESH)

    def w_copy(r):
        to = lax.rem(tpi + r, tp)
        return remote(wgt_v.at[pl.ds(pl.multiple_of(to * feat, feat), feat), :], w_in.at[tpi],
                      w_ss.at[0], w_rs.at[0], tp=to)

    def a_copy(kind, r, u):
        return remote(a_out.at[kind, u, r - 1], a_in.at[kind, u, r], a_ss.at[0], a_rs.at[kind, u],
                      sp=z * inner + owner(r))

    def e_copy(r):
        return remote(e_out.at[owner(r)], e_in.at[r], e_ss.at[0], e_rs.at[0], sp=z * inner + owner(r))

    def b_part(ref, kind):
        return ref if kind == GRAD else ref.at[pl.ds(0, fold)]

    def b_copy(kind, r, u):
        way = jnp.where(z + r < outer, 0, 1)
        return remote(b_part(b_out.at[kind, u, way], kind), b_part(b_in.at[kind, u, r - 1], kind),
                      b_ss.at[kind], b_rs.at[kind, u], sp=lax.rem(z + r, outer) * inner + y)

    def c_copy(kind, r, u):
        return remote(c_out.at[kind, u, r], c_in.at[kind, u, r - 1], c_ss.at[0], c_rs.at[kind, u],
                      sp=z * inner + lax.rem(y - r + inner, inner))

    mate = x * CORES + 1 - core

    def d_copies(r, u, count):
        at = rows(r, u, count)
        for k in FAR_FIRST:
            remote(d_all.at[tpi, at], d_all.at[tpi, at], d_ss.at[0], d_rs.at[u],
                   tp=lax.rem(x + k, xs) * CORES + core).start()
        remote(d_all.at[tpi, at], d_all.at[tpi, at], f_ss.at[0], f_rs.at[u], tp=mate).start()

    def forward(u):
        at = rows(0, u, inner)
        take(d_all.at[pl.ds(0, xs - 1), at], d_rs.at[u])
        for k in range(1, xs):
            mine = d_all.at[lax.rem(x - k + xs, xs) * CORES + core, at]
            remote(mine, mine, f_ss.at[0], f_rs.at[u], tp=mate).start()

    def g_copy(dz, dy):
        to = away(dz, dy)
        return remote(g_out.at[to], g_in.at[dz * inner + dy - 1], g_ss.at[0], g_rs.at[0], sp=to)

    row = lax.broadcasted_iota(jnp.int32, (length, length), 0)
    col = lax.broadcasted_iota(jnp.int32, (length, length), 1)
    lower, upper = row >= col, row <= col

    def matrix(first, second):
        both = jnp.concatenate([jnp.where(first, 1.0, 0.0), jnp.where(second, 1.0, 0.0)], 0)
        return jnp.concatenate([both, both], 1).astype(BF16)

    sums, strict = matrix(lower, upper), matrix(row > col, row < col)
    left = lax.broadcasted_iota(jnp.int32, (length, pack), 1) < dk
    left_fold = lax.broadcasted_iota(jnp.int32, (fold, pack), 1) < dk
    tail_row = lax.broadcasted_iota(jnp.int32, (TAIL, pack), 0)
    left_tall = lax.broadcasted_iota(jnp.int32, (dv, pack), 1) < dk

    def directed(tri, blocks):
        made = []
        for i in range(0, len(blocks), 2):
            pair = blocks[i:i + 2]
            out = dot(tri, halves(jnp.concatenate(pair, 1) if len(pair) > 1 else pair[0]))
            for n in range(len(pair)):
                part = out[:, n * pack:(n + 1) * pack]
                made.append(jnp.where(left, part[:length], part[length:]))
        return made

    def twice(ref, r, u):
        v = ref[owner(r), u].astype(F32)
        return jnp.concatenate([v, v], 1)

    def ends(c):
        return jnp.where(left[:1], c[length - 1:length], c[0:1])

    def decays(todo):
        blocks = [jnp.concatenate([decay_v[0, owner(r), u], decay_v[1, owner(r), u]], 1) for r, u in todo]
        made = directed(sums, blocks)
        for (r, u), c in zip(todo, made):
            cum[slot(r, u)] = c
        for (r, u), c in zip(todo, made):
            e_out[owner(r), pl.ds(u, 1), :] = ends(c)

    def grads(todo):
        hats = [(twice(q_v, r, u) * jnp.exp(cum[slot(r, u)])).astype(BF16) for r, u in todo]
        made = [dot(cot_v[owner(r), u], hat, 0, 0).astype(BF16) for (r, u), hat in zip(todo, hats)]
        return hats, made

    def states(todo):
        keys = []
        for r, u in todo:
            c = cum[slot(r, u)]
            keys.append((twice(k_v, r, u) * jnp.exp(ends(c) - c)).astype(BF16))
        made = [dot(val[rows(r, u)], k_end, 0, 0).astype(BF16) for (r, u), k_end in zip(todo, keys)]
        return keys, made

    def place(kind, r, u, value):
        if r == 0:
            a_in[kind, u, 0] = value
        else:
            a_out[kind, u, r - 1] = value

    def emit(kind, todo):
        kept, made = (grads if kind == 0 else states)(todo)
        keep = q_hats if kind == 0 else k_ends
        for (r, u), value, block in zip(todo, kept, made):
            keep[slot(r, u)] = value
            place(kind, r, u, block)

    def values(u):
        at = rows(0, u, inner)
        val[at] = dot(hid_v[at], wgt_v[...]).astype(BF16)

    everyone, visitors = tuple(range(inner)), tuple(range(1, inner))

    def send(kind, u):
        for r in FAR_FIRST:
            a_copy(kind, r, u).start()

    loaded(0, 1)
    decays([(r, 0) for r in everyone])
    emit(GRAD, [(r, 0) for r in visitors])
    pl.semaphore_wait(barrier, inner + outer + tp - 3)
    send(GRAD, 0)
    loaded(1, own - 1)
    decays([(r, u) for u in range(1, own) for r in everyone])
    for r in FAR_FIRST:
        e_copy(r).start()
    e_in[0] = e_out[y]
    for u in range(1, own):
        emit(GRAD, [(r, u) for r in visitors])
        send(GRAD, u)

    end = own - 1
    take(wgt_v, i_s.at[6])
    take(k_v, i_s.at[7])
    for u in range(own):
        take(hid_v.at[rows(0, u, inner)], h_s.at[u])
        values(u)
        emit(STATE, [(r, u) for r in visitors])
        if u < end:
            send(STATE, u)

    for r in range(1, tp):
        w_copy(r).start()
    w_in[tpi] = wgt_v[pl.ds(pl.multiple_of(tpi * feat, feat), feat), :]
    mine = [(0, u) for u in range(own)]
    emit(GRAD, mine)
    emit(STATE, mine)
    w_acc[...] = jnp.zeros((dv, width), F32)

    def offset(person):
        return lax.rem(y - person + inner, inner)

    def endings(u):
        return [e_in[offset(person), pl.ds(u, 1), :] for person in everyone]

    def pick(kind, ahead, behind):
        at = left_tall if ahead.shape[0] == dv else left[:1]
        return jnp.where(at, ahead, behind) if kind == STATE else jnp.where(at, behind, ahead)

    def turn(v):
        return pltpu.roll(v, dk, 1)

    def folded(v, first):
        if first:
            return jnp.where(left_fold, v[:fold], turn(v[fold:]))
        return jnp.where(left_fold, turn(v[:fold]), v[fold:])

    def unfolded(first, second):
        return jnp.concatenate([jnp.where(left_fold, first, turn(second)),
                                jnp.where(left_fold, turn(first), second)], 0)

    def running(blocks, factors, order):
        total, before = None, [None] * inner
        for person in order:
            before[person] = jnp.zeros((dv, pack), F32) if total is None else total
            total = blocks[person] if total is None else factors[person] * total + blocks[person]
        return before, total

    def combine_plane(kind, u):
        take(a_in.at[kind, u, pl.ds(1, inner - 1)], a_rs.at[kind, u])
        blocks = [a_in[kind, u, offset(person)].astype(F32) for person in everyone]
        ends_ = endings(u)
        factors = [jnp.exp(e) for e in ends_]
        before, total = running(blocks, factors, everyone)
        after, total_back = running(blocks, factors, everyone[::-1])
        for person in everyone:
            local[kind, u, person] = pick(kind, before[person], after[person])
        b_out[kind, u, 0, pl.ds(0, fold)] = folded(total, kind == STATE).astype(BF16)
        b_out[kind, u, 1, pl.ds(0, fold)] = folded(total_back, kind == GRAD).astype(BF16)
        if kind == GRAD:
            whole = sum(ends_[1:], ends_[0])
            high = whole.astype(BF16).astype(F32)
            tail = jnp.where(tail_row == 0, high, jnp.where(tail_row == 1, whole - high, 0.0)).astype(BF16)
            for way in range(2):
                b_out[kind, u, way, pl.ds(fold, TAIL)] = tail
        for r in FAR_FIRST:
            b_copy(kind, r, u).start()

    def combine_all(kind, u):
        take(b_in.at[GRAD, u] if kind == GRAD else b_in.at[STATE, u, :, pl.ds(0, fold)], b_rs.at[kind, u])
        planes = [None]
        for r in range(1, outer):
            tail = b_in[GRAD, u, r - 1, pl.ds(fold, TAIL)].astype(F32)
            planes.append(tail[0:1] + tail[1:2])
        zero = jnp.zeros((1, pack), F32)
        ahead, behind = jnp.zeros((fold, pack), F32), jnp.zeros((fold, pack), F32)
        for r in range(1, outer):
            block = b_in[kind, u, r - 1, pl.ds(0, fold)].astype(F32)
            passed, back = sum(planes[1:r], zero), sum(planes[r + 1:], zero)
            first = jnp.where(left[:1], passed, turn(passed)) if kind == STATE else jnp.where(left[:1], turn(passed), passed)
            second = jnp.where(left[:1], back, turn(back)) if kind == GRAD else jnp.where(left[:1], turn(back), back)
            ahead = ahead + jnp.where(z >= r, jnp.exp(first), 0.0) * block
            behind = behind + jnp.where(z + outer - r < outer, jnp.exp(second), 0.0) * block
        carried = unfolded(ahead, behind) if kind == STATE else unfolded(behind, ahead)
        ends_ = endings(u)
        for person in everyone:
            factor = jnp.exp(pick(kind, sum(ends_[:person], zero), sum(ends_[person + 1:], zero)))
            c_out[kind, u, offset(person)] = (factor * carried + local[kind, u, person]).astype(BF16)
        for r in FAR_FIRST:
            c_copy(kind, r, u).start()

    def intra(todo):
        made = []
        for r, u in todo:
            s = slot(r, u)
            q_hat = q_hats[s]
            k_hat = (twice(k_v, r, u) * jnp.exp(-cum[s])).astype(BF16)
            v, seed = val[rows(r, u)], cot_v[owner(r), u]
            seed_scores = dot(seed, v, 1, 1)
            zero = jnp.zeros_like(q_hat)
            q_left, q_right = jnp.where(left, q_hat, zero), jnp.where(left, zero, q_hat)
            k_left, k_right = jnp.where(left, k_hat, zero), jnp.where(left, zero, k_hat)
            score = (jnp.where(lower, dot(q_left, k_hat, 1, 1), 0.0)
                     + jnp.where(upper, dot(q_right, k_hat, 1, 1), 0.0)).astype(BF16)
            seed_low = jnp.where(lower, seed_scores, 0.0).astype(BF16)
            seed_up = jnp.where(upper, seed_scores, 0.0).astype(BF16)
            made.append((dot(seed_low, k_left) + dot(seed_up, k_right),
                         dot(seed_low, q_left, 0, 0) + dot(seed_up, q_right, 0, 0),
                         dot(score, seed, 0, 0)))
        for (r, u), (for_q, for_k, for_v) in zip(todo, made):
            intra_q[slot(r, u)] = for_q
            intra_k[slot(r, u)] = for_k
            intra_v[slot(r, u)] = for_v

    def arrived(kind, r, u):
        return c_out[kind, u, 0] if r == 0 else c_in[kind, u, r - 1]

    def finish_values(todo):
        made = [intra_v[slot(r, u)] + dot(k_ends[slot(r, u)], arrived(GRAD, r, u), 1, 1) for r, u in todo]
        for (r, u), block in zip(todo, made):
            d_all[tpi, rows(r, u)] = block.astype(BF16)

    def finish_rest(todo):
        kept, terms = [], []
        for r, u in todo:
            s = slot(r, u)
            state, grad = arrived(STATE, r, u), arrived(GRAD, r, u)
            c = cum[s]
            end = ends(c)
            grow, shrink, to_end = jnp.exp(c), jnp.exp(-c), jnp.exp(end - c)
            q, k = twice(q_v, r, u), twice(k_v, r, u)
            cross = dot(cot_v[owner(r), u], state)
            dq = grow * (intra_q[s] + cross)
            dk_ = shrink * intra_k[s] + to_end * dot(val[rows(r, u)], grad)
            terms.append(q * dq - k * dk_)
            start = (jnp.sum(q * grow * cross, axis=0, keepdims=True)
                     + jnp.exp(end) * jnp.sum(state.astype(F32) * grad.astype(F32), axis=0, keepdims=True))
            kept.append((dq, dk_, start))
        for (r, u), (dq, dk_, start), sums_ in zip(todo, kept, directed(strict, terms)):
            b = batch_of(r, u)
            decay_grad = start - sums_
            o_q[b] = (dq[:, :dk] + dq[:, dk:]).astype(BF16)
            o_k[b] = (dk_[:, :dk] + dk_[:, dk:]).astype(BF16)
            o_f[b] = decay_grad[:, :dk]
            o_b[b] = decay_grad[:, dk:]

    def features(u):
        take(d_all.at[pl.ds(0, xs), rows(0, u, inner)], f_rs.at[u])
        at = rows(0, u, inner)
        wide = jnp.concatenate([d_all[t, at] for t in range(tp)], 1)
        weights = jnp.concatenate([w_in[t] for t in range(tp)], 1)
        out = dot(wide, weights, 1, 1).astype(BF16)
        for r in range(inner):
            o_h[batch_of(r, u)] = out[r * length:(r + 1) * length]

    def finish_own(u):
        finish_values([(0, u)])
        d_copies(0, u, 1)

    def finish_others(u):
        take(c_in.at[GRAD, u], c_rs.at[GRAD, u])
        finish_values([(r, u) for r in visitors])
        d_copies(1, u, inner - 1)

    def weight_terms(u):
        at = rows(0, u, inner)
        return dot(d_all[tpi, at], hid_v[at], 0, 0)

    def rest_others(u):
        take(c_in.at[STATE, u], c_rs.at[STATE, u])
        finish_rest([(r, u) for r in visitors])

    def loop(first, last, step):
        lax.fori_loop(first, last, lambda u, _: step(u) or 0, 0)

    def intra_all(u):
        intra([(r, u) for r in everyone])

    def first_steps(u):
        combine_plane(GRAD, u)
        intra_all(u)

    def second_steps(u):
        combine_all(GRAD, u)
        finish_own(u)
        combine_plane(STATE, u - 1)

    def weigh(u):
        finish_others(u)
        w_acc[...] += weight_terms(u)

    def pass_states(u):
        combine_all(STATE, u)
        finish_rest([(0, u)])

    def third_steps(u):
        weigh(u)
        pass_states(u)

    def fourth_steps(u):
        forward(u)
        rest_others(u)

    take(e_in.at[pl.ds(1, inner - 1)], e_rs.at[0])
    loop(0, end, first_steps)
    combine_plane(GRAD, end)
    combine_all(GRAD, 0)
    finish_own(0)
    intra_all(end)
    loop(1, end, second_steps)
    send(STATE, end)
    second_steps(end)
    loop(0, end, third_steps)
    combine_plane(STATE, end)

    finish_others(end)
    full = w_acc[...] + weight_terms(end)
    for p in range(0, sp, 2):
        block = full[:, p * rows_sp:(p + 2) * rows_sp].T.astype(BF16)
        g_out[p] = block[:rows_sp]
        g_out[p + 1] = block[rows_sp:]
    for away_by in OFFSETS:
        g_copy(*away_by).start()
    loop(0, end - 1, fourth_steps)
    forward(end - 1)
    pass_states(end)
    forward(end)
    rest_others(end - 1)
    take(w_in.at[pl.ds(0, tp - 1)], w_rs.at[0])
    loop(0, own, features)
    rest_others(end)

    take(g_in, g_rs.at[0])
    acc = g_out[spi].astype(F32)
    for r in range(sp - 1):
        acc = acc + g_in[r].astype(F32)
    o_w[...] = acc

    take(w_in.at[pl.ds(0, tp - 1)], w_ss.at[0])
    take(e_in.at[pl.ds(1, inner - 1)], e_ss.at[0])
    take(a_out, a_ss.at[0])
    take(b_in.at[GRAD], b_ss.at[GRAD])
    take(b_in.at[STATE, :, :, pl.ds(0, fold)], b_ss.at[STATE])
    take(c_in, c_ss.at[0])
    take(d_all.at[pl.ds(0, xs - 1)], d_ss.at[0])
    take(d_all.at[pl.ds(0, xs)], f_ss.at[0])
    take(g_in, g_ss.at[0])


def store_kernel(*refs):
    n = len(refs) // 2
    copies = [pltpu.make_async_copy(refs[i], refs[n + i], refs[-1].at[i]) for i in range(n)]
    for copy in copies:
        copy.start()
    for copy in copies:
        copy.wait()


def store(arrays):
    n = len(arrays)
    return pl.pallas_call(
        store_kernel,
        out_shape=tuple(jax.ShapeDtypeStruct(a.shape, a.dtype) for a in arrays),
        in_specs=[pl.BlockSpec(memory_space=pltpu.VMEM)] * n,
        out_specs=(pl.BlockSpec(memory_space=pl.ANY),) * n,
        scratch_shapes=[pltpu.SemaphoreType.DMA((n,))],
        compiler_params=pltpu.CompilerParams(has_side_effects=True, vmem_limit_bytes=1024 * 1024),
    )(*arrays)


def shards(sp, tp, hidden, value_weight, queries, key_vectors, forward_decay, backward_decay, cotangent):
    batch, length, width = hidden.shape
    heads, dk = queries.shape[1], queries.shape[3]
    dv = value_weight.shape[1]
    assert heads == 1
    inner, outer, own, xs = INNER, sp // INNER, batch // INNER, tp // CORES
    pack, rows, feat, rows_sp = 2 * dk, batch * length, width // tp, width // sp
    dims = (sp, tp, batch, length, dk, dv, width)
    vmem, dma = pltpu.VMEM, pltpu.SemaphoreType.DMA
    scratch = [
        vmem((rows, width), BF16), vmem((width, dv), BF16),
        vmem((inner, own, length, dk), BF16), vmem((inner, own, length, dk), BF16),
        vmem((2, inner, own, length, dk), F32), vmem((inner, own, length, dv), BF16),
        vmem((rows, dv), BF16),
        vmem((batch, length, pack), F32),
        vmem((batch, length, pack), BF16), vmem((batch, length, pack), BF16),
        vmem((batch, length, pack), F32), vmem((batch, length, pack), F32),
        vmem((batch, length, dv), F32),
        vmem((2, own, inner - 1, dv, pack), BF16), vmem((2, own, inner, dv, pack), BF16),
        vmem((inner, own, pack), F32), vmem((inner, own, pack), F32),
        vmem((2, own, inner, dv, pack), F32),
        vmem((2, own, 2, dv // 2 + TAIL, pack), BF16), vmem((2, own, outer - 1, dv // 2 + TAIL, pack), BF16),
        vmem((2, own, inner, dv, pack), BF16), vmem((2, own, inner - 1, dv, pack), BF16),
        vmem((tp, rows, dv), BF16), vmem((tp, feat, dv), BF16),
        vmem((dv, width), F32),
        vmem((sp, rows_sp, dv), BF16), vmem((sp - 1, rows_sp, dv), BF16),
        dma((8,)), dma((own,)),
        dma((1,)), dma((2, own)),
        dma((1,)), dma((1,)),
        dma((2,)), dma((2, own)),
        dma((1,)), dma((2, own)),
        dma((1,)), dma((own,)),
        dma((1,)), dma((own,)),
        dma((1,)), dma((1,)),
        dma((1,)), dma((1,)),
    ]
    whole = pl.BlockSpec(memory_space=vmem)
    flat, split = (batch, length, dk), (inner, own, length, dk)
    args = (hidden.reshape(inner, own, length, width), value_weight, queries.reshape(split),
            key_vectors.reshape(split), forward_decay.reshape(split), backward_decay.reshape(split),
            cotangent.reshape(inner, own, length, dv))
    outs = pl.pallas_call(
        functools.partial(kernel, dims),
        out_shape=(
            vmem(flat, BF16), vmem(flat, BF16), vmem(flat, F32), vmem(flat, F32),
            vmem((batch, length, feat), BF16), vmem((rows_sp, dv), F32),
        ),
        in_specs=[pl.BlockSpec(memory_space=pltpu.HBM)] * 7,
        out_specs=(whole,) * 6,
        scratch_shapes=scratch,
        compiler_params=pltpu.CompilerParams(
            collective_id=0, has_side_effects=True, vmem_limit_bytes=48 * 1024 * 1024
        ),
    )(*(pltpu.with_memory_space_constraint(a, pltpu.HBM) for a in args))
    outs = store(outs)
    return tuple(a.reshape(queries.shape) for a in outs[:4]) + tuple(outs[4:])


def solution(mesh):
    heads = P(None, "tp", "sp", None)
    return jax.shard_map(
        functools.partial(shards, mesh.shape["sp"], mesh.shape["tp"]),
        mesh=mesh,
        in_specs=(P(None, "sp", None), P(None, "tp"), heads, heads, heads, heads, P(None, "sp", "tp")),
        out_specs=(heads, heads, heads, heads, P(None, "sp", "tp"), P("sp", "tp")),
        check_vma=False,
    )
```

```python
import functools

import jax
import jax.numpy as jnp
from jax import lax
from jax.experimental import pallas as pl
from jax.experimental.pallas import tpu as pltpu
from jax.sharding import PartitionSpec as P

F32, BF16 = jnp.float32, jnp.bfloat16
MESH = pl.DeviceIdType.MESH
CORES = 2
INNER = 4
TAIL = 16
GRAD, STATE = 0, 1
FAR_FIRST = (2, 1, 3)
OFFSETS = sorted(((dz, dy) for dz in range(4) for dy in range(4) if dz or dy),
                 key=lambda d: -sum(min(v, 4 - v) for v in d))


def dot(a, b, ca=1, cb=0):
    return lax.dot_general(a, b, (((ca,), (cb,)), ((), ())), preferred_element_type=F32)


def halves(x):
    high = x.astype(BF16)
    return jnp.concatenate([high, (x - high.astype(F32)).astype(BF16)], 0)


def kernel(dims, hid, wgt, qry, key, fdec, bdec, cot,
           o_q, o_k, o_f, o_b, o_h, o_w,
           hid_v, wgt_v, q_v, k_v, decay_v, cot_v,
           val, cum, q_hats, k_ends, intra_q, intra_k, intra_v,
           a_out, a_in, e_out, e_in, local, b_out, b_in, c_out, c_in,
           d_all, w_in, w_acc, g_out, g_in,
           i_s, h_s, a_ss, a_rs, e_ss, e_rs, b_ss, b_rs, c_ss, c_rs,
           d_ss, d_rs, f_ss, f_rs, w_ss, w_rs, g_ss, g_rs):
    sp, tp, batch, length, dk, dv, width = dims
    inner, outer, own, xs = INNER, sp // INNER, batch // INNER, tp // CORES
    pack, feat, rows_sp, group = 2 * dk, width // tp, width // sp, INNER * length
    fold = dv // 2
    spi, tpi = lax.axis_index("sp"), lax.axis_index("tp")
    z, y = spi // inner, lax.rem(spi, inner)
    x, core = tpi // CORES, lax.rem(tpi, CORES)

    barrier = pltpu.get_barrier_semaphore()
    mate = x * CORES + 1 - core
    inside = (x > 0) & (x < xs - 1)
    def owner(r):
        return lax.rem(y + r, inner)

    def batch_of(r, u):
        return owner(r) * own + u

    def slot(r, u):
        return u * inner + r

    def rows(r, u, count=1):
        return pl.ds(pl.multiple_of(slot(r, u) * length, length), count * length)

    def away(dz, dy):
        return lax.rem(z + dz, outer) * inner + lax.rem(y + dy, inner)

    def take(ref, sem):
        pltpu.make_async_copy(ref, ref, sem).wait()

    def load(first, count):
        at, n = pl.ds(first, count), min(first, 1)
        for i in range(2):
            pltpu.make_async_copy((fdec, bdec)[i].at[:, at], decay_v.at[i, :, at], i_s.at[n]).start()
        pltpu.make_async_copy(qry.at[:, at], q_v.at[:, at], i_s.at[2 + n]).start()
        pltpu.make_async_copy(cot.at[:, at], cot_v.at[:, at], i_s.at[4 + n]).start()

    def loaded(first, count):
        at, n = pl.ds(first, count), min(first, 1)
        take(decay_v.at[:, :, at], i_s.at[n])
        take(q_v.at[:, at], i_s.at[2 + n])
        take(cot_v.at[:, at], i_s.at[4 + n])

    def load_hidden(u):
        for r in range(inner):
            pltpu.make_async_copy(hid.at[owner(r), u], hid_v.at[rows(r, u)], h_s.at[u]).start()

    load(0, 1)
    for r in range(1, outer):
        pl.semaphore_signal(barrier, inc=1, device_id={"sp": away(r, 0)}, device_id_type=MESH)
    for r in range(1, inner):
        pl.semaphore_signal(barrier, inc=1, device_id={"sp": away(0, r)}, device_id_type=MESH)
    pl.semaphore_signal(barrier, inc=1, device_id={"tp": mate}, device_id_type=MESH)
    for step in (1, -1):
        @pl.when((x + step >= 0) & (x + step < xs))
        def _():
            for c in range(CORES):
                pl.semaphore_signal(barrier, inc=1, device_id={"tp": jnp.clip(x + step, 0, xs - 1) * CORES + c},
                                    device_id_type=MESH)

    pltpu.make_async_copy(wgt, wgt_v, i_s.at[6]).start()
    load_hidden(0)
    pltpu.make_async_copy(key, k_v, i_s.at[7]).start()
    load(1, own - 1)
    for u in range(1, own):
        load_hidden(u)

    def remote(src, dst, ss, rs, **where):
        return pltpu.make_async_remote_copy(src_ref=src, dst_ref=dst, send_sem=ss, recv_sem=rs,
                                            device_id=where, device_id_type=MESH)

    def w_copy(to, phase):
        return remote(wgt_v.at[pl.ds(pl.multiple_of(to * feat, feat), feat), :], w_in.at[tpi],
                      w_ss.at[0], w_rs.at[phase], tp=to)

    def w_near():
        w_copy(mate, 0).start()
        for step in (1, -1):
            @pl.when((x + step >= 0) & (x + step < xs))
            def _():
                for c in range(CORES):
                    w_copy(jnp.clip(x + step, 0, xs - 1) * CORES + c, 0).start()

    def w_across():
        for many in range(2):
            @pl.when(inside if many else jnp.logical_not(inside))
            def _():
                take(w_in.at[pl.ds(0, 1 + CORES * (1 + many))], w_rs.at[0])
        for c in range(CORES):
            w_copy(lax.rem(x + 2, xs) * CORES + c, 1).start()

    def w_ends():
        take(w_in.at[pl.ds(0, CORES)], w_rs.at[1])

        @pl.when(jnp.logical_not(inside))
        def _():
            for c in range(CORES):
                w_copy((xs - 1 - x) * CORES + c, 2).start()

    def a_copy(kind, r, u):
        return remote(a_out.at[kind, u, r - 1], a_in.at[kind, u, r], a_ss.at[0], a_rs.at[kind, u],
                      sp=z * inner + owner(r))

    def e_copy(r):
        return remote(e_out.at[owner(r)], e_in.at[r], e_ss.at[0], e_rs.at[0], sp=z * inner + owner(r))

    def b_part(ref, kind):
        return ref if kind == GRAD else ref.at[pl.ds(0, fold)]

    def b_copy(kind, r, u):
        way = jnp.where(z + r < outer, 0, 1)
        return remote(b_part(b_out.at[kind, u, way], kind), b_part(b_in.at[kind, u, r - 1], kind),
                      b_ss.at[kind], b_rs.at[kind, u], sp=lax.rem(z + r, outer) * inner + y)

    def c_copy(kind, r, u):
        return remote(c_out.at[kind, u, r], c_in.at[kind, u, r - 1], c_ss.at[0], c_rs.at[kind, u],
                      sp=z * inner + lax.rem(y - r + inner, inner))

    def d_copies(r, u, count):
        at = rows(r, u, count)
        for k in FAR_FIRST:
            remote(d_all.at[tpi, at], d_all.at[tpi, at], d_ss.at[0], d_rs.at[u],
                   tp=lax.rem(x + k, xs) * CORES + core).start()
        remote(d_all.at[tpi, at], d_all.at[tpi, at], f_ss.at[0], f_rs.at[u], tp=mate).start()

    def forward(u):
        at = rows(0, u, inner)
        take(d_all.at[pl.ds(0, xs - 1), at], d_rs.at[u])
        for k in range(1, xs):
            mine = d_all.at[lax.rem(x - k + xs, xs) * CORES + core, at]
            remote(mine, mine, f_ss.at[0], f_rs.at[u], tp=mate).start()

    def g_copy(dz, dy):
        to = away(dz, dy)
        return remote(g_out.at[to], g_in.at[dz * inner + dy - 1], g_ss.at[0], g_rs.at[0], sp=to)

    row = lax.broadcasted_iota(jnp.int32, (length, length), 0)
    col = lax.broadcasted_iota(jnp.int32, (length, length), 1)
    lower, upper = row >= col, row <= col

    def matrix(first, second):
        both = jnp.concatenate([jnp.where(first, 1.0, 0.0), jnp.where(second, 1.0, 0.0)], 0)
        return jnp.concatenate([both, both], 1).astype(BF16)

    sums, strict = matrix(lower, upper), matrix(row > col, row < col)
    left = lax.broadcasted_iota(jnp.int32, (length, pack), 1) < dk
    left_fold = lax.broadcasted_iota(jnp.int32, (fold, pack), 1) < dk
    tail_row = lax.broadcasted_iota(jnp.int32, (TAIL, pack), 0)
    left_tall = lax.broadcasted_iota(jnp.int32, (dv, pack), 1) < dk

    def directed(tri, blocks):
        made = []
        for i in range(0, len(blocks), 2):
            pair = blocks[i:i + 2]
            out = dot(tri, halves(jnp.concatenate(pair, 1) if len(pair) > 1 else pair[0]))
            for n in range(len(pair)):
                part = out[:, n * pack:(n + 1) * pack]
                made.append(jnp.where(left, part[:length], part[length:]))
        return made

    def twice(ref, r, u):
        v = ref[owner(r), u].astype(F32)
        return jnp.concatenate([v, v], 1)

    def ends(c):
        return jnp.where(left[:1], c[length - 1:length], c[0:1])

    def decays(todo):
        blocks = [jnp.concatenate([decay_v[0, owner(r), u], decay_v[1, owner(r), u]], 1) for r, u in todo]
        made = directed(sums, blocks)
        for (r, u), c in zip(todo, made):
            cum[slot(r, u)] = c
        for (r, u), c in zip(todo, made):
            e_out[owner(r), pl.ds(u, 1), :] = ends(c)

    def grads(todo):
        hats = [(twice(q_v, r, u) * jnp.exp(cum[slot(r, u)])).astype(BF16) for r, u in todo]
        made = [dot(cot_v[owner(r), u], hat, 0, 0).astype(BF16) for (r, u), hat in zip(todo, hats)]
        return hats, made

    def states(todo):
        keys = []
        for r, u in todo:
            c = cum[slot(r, u)]
            keys.append((twice(k_v, r, u) * jnp.exp(ends(c) - c)).astype(BF16))
        made = [dot(val[rows(r, u)], k_end, 0, 0).astype(BF16) for (r, u), k_end in zip(todo, keys)]
        return keys, made

    def place(kind, r, u, value):
        if r == 0:
            a_in[kind, u, 0] = value
        else:
            a_out[kind, u, r - 1] = value

    def emit(kind, todo):
        kept, made = (grads if kind == 0 else states)(todo)
        keep = q_hats if kind == 0 else k_ends
        for (r, u), value, block in zip(todo, kept, made):
            keep[slot(r, u)] = value
            place(kind, r, u, block)

    def values(u):
        at = rows(0, u, inner)
        val[at] = dot(hid_v[at], wgt_v[...]).astype(BF16)

    everyone, visitors = tuple(range(inner)), tuple(range(1, inner))

    def send(kind, u):
        for r in FAR_FIRST:
            a_copy(kind, r, u).start()

    loaded(0, 1)
    decays([(r, 0) for r in everyone])
    emit(GRAD, [(r, 0) for r in visitors])
    pl.semaphore_wait(barrier, inner + outer - 1 + jnp.where(inside, 2 * CORES, CORES))
    send(GRAD, 0)
    loaded(1, own - 1)
    decays([(r, u) for u in range(1, own) for r in everyone])
    for r in FAR_FIRST:
        e_copy(r).start()
    e_in[0] = e_out[y]
    for u in range(1, own):
        emit(GRAD, [(r, u) for r in visitors])
        send(GRAD, u)

    end = own - 1
    take(wgt_v, i_s.at[6])
    w_near()
    take(k_v, i_s.at[7])
    for u in range(own):
        take(hid_v.at[rows(0, u, inner)], h_s.at[u])
        values(u)
        emit(STATE, [(r, u) for r in visitors])
        if u < end:
            send(STATE, u)

    w_in[tpi] = wgt_v[pl.ds(pl.multiple_of(tpi * feat, feat), feat), :]
    mine = [(0, u) for u in range(own)]
    emit(GRAD, mine)
    emit(STATE, mine)
    w_acc[...] = jnp.zeros((dv, width), F32)
    w_across()

    def offset(person):
        return lax.rem(y - person + inner, inner)

    def endings(u):
        return [e_in[offset(person), pl.ds(u, 1), :] for person in everyone]

    def pick(kind, ahead, behind):
        at = left_tall if ahead.shape[0] == dv else left[:1]
        return jnp.where(at, ahead, behind) if kind == STATE else jnp.where(at, behind, ahead)

    def turn(v):
        return pltpu.roll(v, dk, 1)

    def folded(v, first):
        if first:
            return jnp.where(left_fold, v[:fold], turn(v[fold:]))
        return jnp.where(left_fold, turn(v[:fold]), v[fold:])

    def unfolded(first, second):
        return jnp.concatenate([jnp.where(left_fold, first, turn(second)),
                                jnp.where(left_fold, turn(first), second)], 0)

    def running(blocks, factors, order):
        total, before = None, [None] * inner
        for person in order:
            before[person] = jnp.zeros((dv, pack), F32) if total is None else total
            total = blocks[person] if total is None else factors[person] * total + blocks[person]
        return before, total

    def combine_plane(kind, u):
        take(a_in.at[kind, u, pl.ds(1, inner - 1)], a_rs.at[kind, u])
        blocks = [a_in[kind, u, offset(person)].astype(F32) for person in everyone]
        ends_ = endings(u)
        factors = [jnp.exp(e) for e in ends_]
        before, total = running(blocks, factors, everyone)
        after, total_back = running(blocks, factors, everyone[::-1])
        for person in everyone:
            local[kind, u, person] = pick(kind, before[person], after[person])
        b_out[kind, u, 0, pl.ds(0, fold)] = folded(total, kind == STATE).astype(BF16)
        b_out[kind, u, 1, pl.ds(0, fold)] = folded(total_back, kind == GRAD).astype(BF16)
        if kind == GRAD:
            whole = sum(ends_[1:], ends_[0])
            high = whole.astype(BF16).astype(F32)
            tail = jnp.where(tail_row == 0, high, jnp.where(tail_row == 1, whole - high, 0.0)).astype(BF16)
            for way in range(2):
                b_out[kind, u, way, pl.ds(fold, TAIL)] = tail
        for r in FAR_FIRST:
            b_copy(kind, r, u).start()

    def combine_all(kind, u):
        take(b_in.at[GRAD, u] if kind == GRAD else b_in.at[STATE, u, :, pl.ds(0, fold)], b_rs.at[kind, u])
        planes = [None]
        for r in range(1, outer):
            tail = b_in[GRAD, u, r - 1, pl.ds(fold, TAIL)].astype(F32)
            planes.append(tail[0:1] + tail[1:2])
        zero = jnp.zeros((1, pack), F32)
        ahead, behind = jnp.zeros((fold, pack), F32), jnp.zeros((fold, pack), F32)
        for r in range(1, outer):
            block = b_in[kind, u, r - 1, pl.ds(0, fold)].astype(F32)
            passed, back = sum(planes[1:r], zero), sum(planes[r + 1:], zero)
            first = jnp.where(left[:1], passed, turn(passed)) if kind == STATE else jnp.where(left[:1], turn(passed), passed)
            second = jnp.where(left[:1], back, turn(back)) if kind == GRAD else jnp.where(left[:1], turn(back), back)
            ahead = ahead + jnp.where(z >= r, jnp.exp(first), 0.0) * block
            behind = behind + jnp.where(z + outer - r < outer, jnp.exp(second), 0.0) * block
        carried = unfolded(ahead, behind) if kind == STATE else unfolded(behind, ahead)
        ends_ = endings(u)
        for person in everyone:
            factor = jnp.exp(pick(kind, sum(ends_[:person], zero), sum(ends_[person + 1:], zero)))
            c_out[kind, u, offset(person)] = (factor * carried + local[kind, u, person]).astype(BF16)
        for r in FAR_FIRST:
            c_copy(kind, r, u).start()

    def intra(todo):
        made = []
        for r, u in todo:
            s = slot(r, u)
            q_hat = q_hats[s]
            k_hat = (twice(k_v, r, u) * jnp.exp(-cum[s])).astype(BF16)
            v, seed = val[rows(r, u)], cot_v[owner(r), u]
            seed_scores = dot(seed, v, 1, 1)
            zero = jnp.zeros_like(q_hat)
            q_left, q_right = jnp.where(left, q_hat, zero), jnp.where(left, zero, q_hat)
            k_left, k_right = jnp.where(left, k_hat, zero), jnp.where(left, zero, k_hat)
            score = (jnp.where(lower, dot(q_left, k_hat, 1, 1), 0.0)
                     + jnp.where(upper, dot(q_right, k_hat, 1, 1), 0.0)).astype(BF16)
            seed_low = jnp.where(lower, seed_scores, 0.0).astype(BF16)
            seed_up = jnp.where(upper, seed_scores, 0.0).astype(BF16)
            made.append((dot(seed_low, k_left) + dot(seed_up, k_right),
                         dot(seed_low, q_left, 0, 0) + dot(seed_up, q_right, 0, 0),
                         dot(score, seed, 0, 0)))
        for (r, u), (for_q, for_k, for_v) in zip(todo, made):
            intra_q[slot(r, u)] = for_q
            intra_k[slot(r, u)] = for_k
            intra_v[slot(r, u)] = for_v

    def arrived(kind, r, u):
        return c_out[kind, u, 0] if r == 0 else c_in[kind, u, r - 1]

    def finish_values(todo):
        made = [intra_v[slot(r, u)] + dot(k_ends[slot(r, u)], arrived(GRAD, r, u), 1, 1) for r, u in todo]
        for (r, u), block in zip(todo, made):
            d_all[tpi, rows(r, u)] = block.astype(BF16)

    def finish_rest(todo):
        kept, terms = [], []
        for r, u in todo:
            s = slot(r, u)
            state, grad = arrived(STATE, r, u), arrived(GRAD, r, u)
            c = cum[s]
            end = ends(c)
            grow, shrink, to_end = jnp.exp(c), jnp.exp(-c), jnp.exp(end - c)
            q, k = twice(q_v, r, u), twice(k_v, r, u)
            cross = dot(cot_v[owner(r), u], state)
            dq = grow * (intra_q[s] + cross)
            dk_ = shrink * intra_k[s] + to_end * dot(val[rows(r, u)], grad)
            terms.append(q * dq - k * dk_)
            start = (jnp.sum(q * grow * cross, axis=0, keepdims=True)
                     + jnp.exp(end) * jnp.sum(state.astype(F32) * grad.astype(F32), axis=0, keepdims=True))
            kept.append((dq, dk_, start))
        for (r, u), (dq, dk_, start), sums_ in zip(todo, kept, directed(strict, terms)):
            b = batch_of(r, u)
            decay_grad = start - sums_
            o_q[b] = (dq[:, :dk] + dq[:, dk:]).astype(BF16)
            o_k[b] = (dk_[:, :dk] + dk_[:, dk:]).astype(BF16)
            o_f[b] = decay_grad[:, :dk]
            o_b[b] = decay_grad[:, dk:]

    def features(u):
        take(d_all.at[pl.ds(0, xs), rows(0, u, inner)], f_rs.at[u])
        at = rows(0, u, inner)
        wide = jnp.concatenate([d_all[t, at] for t in range(tp)], 1)
        weights = jnp.concatenate([w_in[t] for t in range(tp)], 1)
        out = dot(wide, weights, 1, 1).astype(BF16)
        for r in range(inner):
            o_h[batch_of(r, u)] = out[r * length:(r + 1) * length]

    def finish_own(u):
        finish_values([(0, u)])
        d_copies(0, u, 1)

    def finish_others(u):
        take(c_in.at[GRAD, u], c_rs.at[GRAD, u])
        finish_values([(r, u) for r in visitors])
        d_copies(1, u, inner - 1)

    def weight_terms(u):
        at = rows(0, u, inner)
        return dot(d_all[tpi, at], hid_v[at], 0, 0)

    def rest_others(u):
        take(c_in.at[STATE, u], c_rs.at[STATE, u])
        finish_rest([(r, u) for r in visitors])

    def loop(first, last, step):
        lax.fori_loop(first, last, lambda u, _: step(u) or 0, 0)

    def intra_all(u):
        intra([(r, u) for r in everyone])

    def first_steps(u):
        combine_plane(GRAD, u)
        intra_all(u)

    def second_steps(u):
        combine_all(GRAD, u)
        finish_own(u)
        combine_plane(STATE, u - 1)

    def weigh(u):
        finish_others(u)
        w_acc[...] += weight_terms(u)

    def pass_states(u):
        combine_all(STATE, u)
        finish_rest([(0, u)])

    def third_steps(u):
        weigh(u)
        pass_states(u)

    def fourth_steps(u):
        forward(u)
        rest_others(u)

    take(e_in.at[pl.ds(1, inner - 1)], e_rs.at[0])
    loop(0, end, first_steps)
    combine_plane(GRAD, end)
    combine_all(GRAD, 0)
    w_ends()
    finish_own(0)
    intra_all(end)
    loop(1, own, second_steps)
    send(STATE, end)
    loop(0, end - 1, third_steps)
    weigh(end - 1)

    finish_others(end)
    full = w_acc[...] + weight_terms(end)
    for p in range(0, sp, 2):
        block = full[:, p * rows_sp:(p + 2) * rows_sp].T.astype(BF16)
        g_out[p] = block[:rows_sp]
        g_out[p + 1] = block[rows_sp:]
    pass_states(end - 1)
    combine_plane(STATE, end)
    for away_by in OFFSETS:
        g_copy(*away_by).start()
    loop(0, end - 1, fourth_steps)
    forward(end - 1)
    pass_states(end)
    forward(end)
    rest_others(end - 1)

    @pl.when(jnp.logical_not(inside))
    def _():
        take(w_in.at[pl.ds(0, CORES)], w_rs.at[2])

    loop(0, own, features)
    rest_others(end)

    take(g_in, g_rs.at[0])
    acc = g_out[spi].astype(F32)
    for r in range(sp - 1):
        acc = acc + g_in[r].astype(F32)
    o_w[...] = acc

    take(w_in.at[pl.ds(0, tp - 1)], w_ss.at[0])
    take(e_in.at[pl.ds(1, inner - 1)], e_ss.at[0])
    take(a_out, a_ss.at[0])
    take(b_in.at[GRAD], b_ss.at[GRAD])
    take(b_in.at[STATE, :, :, pl.ds(0, fold)], b_ss.at[STATE])
    take(c_in, c_ss.at[0])
    take(d_all.at[pl.ds(0, xs - 1)], d_ss.at[0])
    take(d_all.at[pl.ds(0, xs)], f_ss.at[0])
    take(g_in, g_ss.at[0])


def store_kernel(*refs):
    n = len(refs) // 2
    copies = [pltpu.make_async_copy(refs[i], refs[n + i], refs[-1].at[i]) for i in range(n)]
    for copy in copies:
        copy.start()
    for copy in copies:
        copy.wait()


def store(arrays):
    n = len(arrays)
    return pl.pallas_call(
        store_kernel,
        out_shape=tuple(jax.ShapeDtypeStruct(a.shape, a.dtype) for a in arrays),
        in_specs=[pl.BlockSpec(memory_space=pltpu.VMEM)] * n,
        out_specs=(pl.BlockSpec(memory_space=pl.ANY),) * n,
        scratch_shapes=[pltpu.SemaphoreType.DMA((n,))],
        compiler_params=pltpu.CompilerParams(has_side_effects=True, vmem_limit_bytes=1024 * 1024),
    )(*arrays)


def shards(sp, tp, hidden, value_weight, queries, key_vectors, forward_decay, backward_decay, cotangent):
    batch, length, width = hidden.shape
    heads, dk = queries.shape[1], queries.shape[3]
    dv = value_weight.shape[1]
    assert heads == 1
    inner, outer, own, xs = INNER, sp // INNER, batch // INNER, tp // CORES
    pack, rows, feat, rows_sp = 2 * dk, batch * length, width // tp, width // sp
    dims = (sp, tp, batch, length, dk, dv, width)
    vmem, dma = pltpu.VMEM, pltpu.SemaphoreType.DMA
    scratch = [
        vmem((rows, width), BF16), vmem((width, dv), BF16),
        vmem((inner, own, length, dk), BF16), vmem((inner, own, length, dk), BF16),
        vmem((2, inner, own, length, dk), F32), vmem((inner, own, length, dv), BF16),
        vmem((rows, dv), BF16),
        vmem((batch, length, pack), F32),
        vmem((batch, length, pack), BF16), vmem((batch, length, pack), BF16),
        vmem((batch, length, pack), F32), vmem((batch, length, pack), F32),
        vmem((batch, length, dv), F32),
        vmem((2, own, inner - 1, dv, pack), BF16), vmem((2, own, inner, dv, pack), BF16),
        vmem((inner, own, pack), F32), vmem((inner, own, pack), F32),
        vmem((2, own, inner, dv, pack), F32),
        vmem((2, own, 2, dv // 2 + TAIL, pack), BF16), vmem((2, own, outer - 1, dv // 2 + TAIL, pack), BF16),
        vmem((2, own, inner, dv, pack), BF16), vmem((2, own, inner - 1, dv, pack), BF16),
        vmem((tp, rows, dv), BF16), vmem((tp, feat, dv), BF16),
        vmem((dv, width), F32),
        vmem((sp, rows_sp, dv), BF16), vmem((sp - 1, rows_sp, dv), BF16),
        dma((8,)), dma((own,)),
        dma((1,)), dma((2, own)),
        dma((1,)), dma((1,)),
        dma((2,)), dma((2, own)),
        dma((1,)), dma((2, own)),
        dma((1,)), dma((own,)),
        dma((1,)), dma((own,)),
        dma((1,)), dma((3,)),
        dma((1,)), dma((1,)),
    ]
    whole = pl.BlockSpec(memory_space=vmem)
    flat, split = (batch, length, dk), (inner, own, length, dk)
    args = (hidden.reshape(inner, own, length, width), value_weight, queries.reshape(split),
            key_vectors.reshape(split), forward_decay.reshape(split), backward_decay.reshape(split),
            cotangent.reshape(inner, own, length, dv))
    outs = pl.pallas_call(
        functools.partial(kernel, dims),
        out_shape=(
            vmem(flat, BF16), vmem(flat, BF16), vmem(flat, F32), vmem(flat, F32),
            vmem((batch, length, feat), BF16), vmem((rows_sp, dv), F32),
        ),
        in_specs=[pl.BlockSpec(memory_space=pltpu.HBM)] * 7,
        out_specs=(whole,) * 6,
        scratch_shapes=scratch,
        compiler_params=pltpu.CompilerParams(
            collective_id=0, has_side_effects=True, vmem_limit_bytes=48 * 1024 * 1024
        ),
    )(*(pltpu.with_memory_space_constraint(a, pltpu.HBM) for a in args))
    outs = store(outs)
    return tuple(a.reshape(queries.shape) for a in outs[:4]) + tuple(outs[4:])


def solution(mesh):
    heads = P(None, "tp", "sp", None)
    return jax.shard_map(
        functools.partial(shards, mesh.shape["sp"], mesh.shape["tp"]),
        mesh=mesh,
        in_specs=(P(None, "sp", None), P(None, "tp"), heads, heads, heads, heads, P(None, "sp", "tp")),
        out_specs=(heads, heads, heads, heads, P(None, "sp", "tp"), P("sp", "tp")),
        check_vma=False,
    )
```

```python
import functools

import jax
import jax.numpy as jnp
from jax import lax
from jax.experimental import pallas as pl
from jax.experimental.pallas import tpu as pltpu
from jax.sharding import PartitionSpec as P

F32, BF16 = jnp.float32, jnp.bfloat16
MESH = pl.DeviceIdType.MESH
CORES = 2
INNER = 4
TAIL = 16
GRAD, STATE = 0, 1
FAR_FIRST = (2, 1, 3)
OFFSETS = sorted(((dz, dy) for dz in range(4) for dy in range(4) if dz or dy),
                 key=lambda d: -sum(min(v, 4 - v) for v in d))


def dot(a, b, ca=1, cb=0):
    return lax.dot_general(a, b, (((ca,), (cb,)), ((), ())), preferred_element_type=F32)


def halves(x):
    high = x.astype(BF16)
    return jnp.concatenate([high, (x - high.astype(F32)).astype(BF16)], 0)


def kernel(dims, hid, wgt, qry, key, fdec, bdec, cot,
           o_q, o_k, o_f, o_b, o_h, o_w,
           hid_v, wgt_v, q_v, k_v, decay_v, cot_v,
           val, cum, q_hats, k_ends, intra_q, intra_k, intra_v,
           a_out, a_in, e_out, e_in, local, b_out, b_in, c_out, c_in,
           d_all, w_in, w_acc, g_out, g_in,
           i_s, h_s, x_ss, a_rs, e_ss, e_rs, b_ss, b_rs, c_rs,
           d_rs, f_ss, f_rs, w_ss, w_rs, g_ss, g_rs):
    sp, tp, batch, length, dk, dv, width = dims
    inner, outer, own, xs = INNER, sp // INNER, batch // INNER, tp // CORES
    pack, feat, rows_sp, group = 2 * dk, width // tp, width // sp, INNER * length
    fold = dv // 2
    spi, tpi = lax.axis_index("sp"), lax.axis_index("tp")
    z, y = spi // inner, lax.rem(spi, inner)
    x, core = tpi // CORES, lax.rem(tpi, CORES)

    barrier = pltpu.get_barrier_semaphore()
    mate = x * CORES + 1 - core
    inside = (x > 0) & (x < xs - 1)
    def owner(r):
        return lax.rem(y + r, inner)

    def batch_of(r, u):
        return owner(r) * own + u

    def slot(r, u):
        return u * inner + r

    def rows(r, u, count=1):
        return pl.ds(pl.multiple_of(slot(r, u) * length, length), count * length)

    def away(dz, dy):
        return lax.rem(z + dz, outer) * inner + lax.rem(y + dy, inner)

    def take(ref, sem):
        pltpu.make_async_copy(ref, ref, sem).wait()

    def load(first, count):
        at, n = pl.ds(first, count), min(first, 1)
        for i in range(2):
            pltpu.make_async_copy((fdec, bdec)[i].at[:, at], decay_v.at[i, :, at], i_s.at[n]).start()
        pltpu.make_async_copy(qry.at[:, at], q_v.at[:, at], i_s.at[2 + n]).start()
        pltpu.make_async_copy(cot.at[:, at], cot_v.at[:, at], i_s.at[4 + n]).start()

    def loaded(first, count):
        at, n = pl.ds(first, count), min(first, 1)
        take(decay_v.at[:, :, at], i_s.at[n])
        take(q_v.at[:, at], i_s.at[2 + n])
        take(cot_v.at[:, at], i_s.at[4 + n])

    def load_hidden(u):
        for r in range(inner):
            pltpu.make_async_copy(hid.at[owner(r), u], hid_v.at[rows(r, u)], h_s.at[u]).start()

    load(0, 1)
    for r in range(1, outer):
        pl.semaphore_signal(barrier, inc=1, device_id={"sp": away(r, 0)}, device_id_type=MESH)
    for r in range(1, inner):
        pl.semaphore_signal(barrier, inc=1, device_id={"sp": away(0, r)}, device_id_type=MESH)
    pl.semaphore_signal(barrier, inc=1, device_id={"tp": mate}, device_id_type=MESH)
    for step in (1, -1):
        @pl.when((x + step >= 0) & (x + step < xs))
        def _():
            for c in range(CORES):
                pl.semaphore_signal(barrier, inc=1, device_id={"tp": jnp.clip(x + step, 0, xs - 1) * CORES + c},
                                    device_id_type=MESH)

    pltpu.make_async_copy(wgt, wgt_v, i_s.at[6]).start()
    load_hidden(0)
    pltpu.make_async_copy(key, k_v, i_s.at[7]).start()
    load(1, own - 1)
    for u in range(1, own):
        load_hidden(u)

    def remote(src, dst, ss, rs, **where):
        return pltpu.make_async_remote_copy(src_ref=src, dst_ref=dst, send_sem=ss, recv_sem=rs,
                                            device_id=where, device_id_type=MESH)

    def w_copy(to, phase):
        return remote(wgt_v.at[pl.ds(pl.multiple_of(to * feat, feat), feat), :], w_in.at[tpi],
                      w_ss.at[0], w_rs.at[phase], tp=to)

    def w_near():
        w_copy(mate, 0).start()
        for step in (1, -1):
            @pl.when((x + step >= 0) & (x + step < xs))
            def _():
                for c in range(CORES):
                    w_copy(jnp.clip(x + step, 0, xs - 1) * CORES + c, 0).start()

    def w_across():
        for many in range(2):
            @pl.when(inside if many else jnp.logical_not(inside))
            def _():
                take(w_in.at[pl.ds(0, 1 + CORES * (1 + many))], w_rs.at[0])
        for c in range(CORES):
            w_copy(lax.rem(x + 2, xs) * CORES + c, 1).start()

    def w_ends():
        take(w_in.at[pl.ds(0, CORES)], w_rs.at[1])

        @pl.when(jnp.logical_not(inside))
        def _():
            for c in range(CORES):
                w_copy((xs - 1 - x) * CORES + c, 2).start()

    def a_copy(kind, r, u):
        return remote(a_out.at[kind, u, r - 1], a_in.at[kind, u, r], x_ss.at[0], a_rs.at[kind, u],
                      sp=z * inner + owner(r))

    def e_copy(r):
        return remote(e_out.at[owner(r)], e_in.at[r], e_ss.at[0], e_rs.at[0], sp=z * inner + owner(r))

    def b_part(ref, kind):
        return ref if kind == GRAD else ref.at[pl.ds(0, fold)]

    def b_copy(kind, r, u):
        way = jnp.where(z + r < outer, 0, 1)
        return remote(b_part(b_out.at[kind, u, way], kind), b_part(b_in.at[kind, u, r - 1], kind),
                      b_ss.at[kind], b_rs.at[kind, u], sp=lax.rem(z + r, outer) * inner + y)

    def c_copy(kind, r, u):
        return remote(c_out.at[kind, u, r], c_in.at[kind, u, r - 1], x_ss.at[0], c_rs.at[kind, u],
                      sp=z * inner + lax.rem(y - r + inner, inner))

    def d_copies(r, u, count):
        at = rows(r, u, count)
        for k in FAR_FIRST:
            remote(d_all.at[tpi, at], d_all.at[tpi, at], f_ss.at[0], d_rs.at[u],
                   tp=lax.rem(x + k, xs) * CORES + core).start()
        remote(d_all.at[tpi, at], d_all.at[tpi, at], f_ss.at[0], f_rs.at[u], tp=mate).start()

    def forward(u):
        at = rows(0, u, inner)
        take(d_all.at[pl.ds(0, xs - 1), at], d_rs.at[u])
        for k in range(1, xs):
            mine = d_all.at[lax.rem(x - k + xs, xs) * CORES + core, at]
            remote(mine, mine, f_ss.at[0], f_rs.at[u], tp=mate).start()

    def g_copy(dz, dy):
        to = away(dz, dy)
        return remote(g_out.at[to], g_in.at[dz * inner + dy - 1], g_ss.at[0], g_rs.at[0], sp=to)

    row = lax.broadcasted_iota(jnp.int32, (length, length), 0)
    col = lax.broadcasted_iota(jnp.int32, (length, length), 1)
    lower, upper = row >= col, row <= col

    def matrix(first, second):
        both = jnp.concatenate([jnp.where(first, 1.0, 0.0), jnp.where(second, 1.0, 0.0)], 0)
        return jnp.concatenate([both, both], 1).astype(BF16)

    sums, strict = matrix(lower, upper), matrix(row > col, row < col)
    left = lax.broadcasted_iota(jnp.int32, (length, pack), 1) < dk
    left_fold = lax.broadcasted_iota(jnp.int32, (fold, pack), 1) < dk
    tail_row = lax.broadcasted_iota(jnp.int32, (TAIL, pack), 0)
    left_tall = lax.broadcasted_iota(jnp.int32, (dv, pack), 1) < dk

    def directed(tri, blocks):
        made = []
        for i in range(0, len(blocks), 2):
            pair = blocks[i:i + 2]
            out = dot(tri, halves(jnp.concatenate(pair, 1) if len(pair) > 1 else pair[0]))
            for n in range(len(pair)):
                part = out[:, n * pack:(n + 1) * pack]
                made.append(jnp.where(left, part[:length], part[length:]))
        return made

    def twice(ref, r, u):
        v = ref[owner(r), u].astype(F32)
        return jnp.concatenate([v, v], 1)

    def ends(c):
        return jnp.where(left[:1], c[length - 1:length], c[0:1])

    def decays(todo):
        blocks = [jnp.concatenate([decay_v[0, owner(r), u], decay_v[1, owner(r), u]], 1) for r, u in todo]
        made = directed(sums, blocks)
        for (r, u), c in zip(todo, made):
            cum[slot(r, u)] = c
        for (r, u), c in zip(todo, made):
            e_out[owner(r), pl.ds(u, 1), :] = ends(c)

    def grads(todo):
        hats = [(twice(q_v, r, u) * jnp.exp(cum[slot(r, u)])).astype(BF16) for r, u in todo]
        made = [dot(cot_v[owner(r), u], hat, 0, 0).astype(BF16) for (r, u), hat in zip(todo, hats)]
        return hats, made

    def states(todo):
        keys = []
        for r, u in todo:
            c = cum[slot(r, u)]
            keys.append((twice(k_v, r, u) * jnp.exp(ends(c) - c)).astype(BF16))
        made = [dot(val[rows(r, u)], k_end, 0, 0).astype(BF16) for (r, u), k_end in zip(todo, keys)]
        return keys, made

    def place(kind, r, u, value):
        if r == 0:
            a_in[kind, u, 0] = value
        else:
            a_out[kind, u, r - 1] = value

    def emit(kind, todo):
        kept, made = (grads if kind == 0 else states)(todo)
        keep = q_hats if kind == 0 else k_ends
        for (r, u), value, block in zip(todo, kept, made):
            keep[slot(r, u)] = value
            place(kind, r, u, block)

    def values(u):
        at = rows(0, u, inner)
        val[at] = dot(hid_v[at], wgt_v[...]).astype(BF16)

    everyone, visitors = tuple(range(inner)), tuple(range(1, inner))

    def send(kind, u):
        for r in FAR_FIRST:
            a_copy(kind, r, u).start()

    loaded(0, 1)
    decays([(r, 0) for r in everyone])
    emit(GRAD, [(r, 0) for r in visitors])
    pl.semaphore_wait(barrier, inner + outer - 1 + jnp.where(inside, 2 * CORES, CORES))
    send(GRAD, 0)
    loaded(1, own - 1)
    decays([(r, u) for u in range(1, own) for r in everyone])
    for r in FAR_FIRST:
        e_copy(r).start()
    e_in[0] = e_out[y]
    for u in range(1, own):
        emit(GRAD, [(r, u) for r in visitors])
        send(GRAD, u)

    end = own - 1
    take(wgt_v, i_s.at[6])
    w_near()
    take(k_v, i_s.at[7])
    for u in range(own):
        take(hid_v.at[rows(0, u, inner)], h_s.at[u])
        values(u)
        emit(STATE, [(r, u) for r in visitors])
        if u < end:
            send(STATE, u)

    w_in[tpi] = wgt_v[pl.ds(pl.multiple_of(tpi * feat, feat), feat), :]
    mine = [(0, u) for u in range(own)]
    emit(GRAD, mine)
    emit(STATE, mine)
    w_acc[...] = jnp.zeros((dv, width), F32)
    w_across()

    def offset(person):
        return lax.rem(y - person + inner, inner)

    def endings(u):
        return [e_in[offset(person), pl.ds(u, 1), :] for person in everyone]

    def pick(kind, ahead, behind):
        at = left_tall if ahead.shape[0] == dv else left[:1]
        return jnp.where(at, ahead, behind) if kind == STATE else jnp.where(at, behind, ahead)

    def turn(v):
        return pltpu.roll(v, dk, 1)

    def folded(v, first):
        if first:
            return jnp.where(left_fold, v[:fold], turn(v[fold:]))
        return jnp.where(left_fold, turn(v[:fold]), v[fold:])

    def unfolded(first, second):
        return jnp.concatenate([jnp.where(left_fold, first, turn(second)),
                                jnp.where(left_fold, turn(first), second)], 0)

    def running(blocks, factors, order):
        total, before = None, [None] * inner
        for person in order:
            before[person] = jnp.zeros((dv, pack), F32) if total is None else total
            total = blocks[person] if total is None else factors[person] * total + blocks[person]
        return before, total

    def combine_plane(kind, u):
        take(a_in.at[kind, u, pl.ds(1, inner - 1)], a_rs.at[kind, u])
        blocks = [a_in[kind, u, offset(person)].astype(F32) for person in everyone]
        ends_ = endings(u)
        factors = [jnp.exp(e) for e in ends_]
        before, total = running(blocks, factors, everyone)
        after, total_back = running(blocks, factors, everyone[::-1])
        for person in everyone:
            local[kind, u, person] = pick(kind, before[person], after[person])
        b_out[kind, u, 0, pl.ds(0, fold)] = folded(total, kind == STATE).astype(BF16)
        b_out[kind, u, 1, pl.ds(0, fold)] = folded(total_back, kind == GRAD).astype(BF16)
        if kind == GRAD:
            whole = sum(ends_[1:], ends_[0])
            high = whole.astype(BF16).astype(F32)
            tail = jnp.where(tail_row == 0, high, jnp.where(tail_row == 1, whole - high, 0.0)).astype(BF16)
            for way in range(2):
                b_out[kind, u, way, pl.ds(fold, TAIL)] = tail
        for r in FAR_FIRST:
            b_copy(kind, r, u).start()

    def combine_all(kind, u):
        take(b_in.at[GRAD, u] if kind == GRAD else b_in.at[STATE, u, :, pl.ds(0, fold)], b_rs.at[kind, u])
        planes = [None]
        for r in range(1, outer):
            tail = b_in[GRAD, u, r - 1, pl.ds(fold, TAIL)].astype(F32)
            planes.append(tail[0:1] + tail[1:2])
        zero = jnp.zeros((1, pack), F32)
        ahead, behind = jnp.zeros((fold, pack), F32), jnp.zeros((fold, pack), F32)
        for r in range(1, outer):
            block = b_in[kind, u, r - 1, pl.ds(0, fold)].astype(F32)
            passed, back = sum(planes[1:r], zero), sum(planes[r + 1:], zero)
            first = jnp.where(left[:1], passed, turn(passed)) if kind == STATE else jnp.where(left[:1], turn(passed), passed)
            second = jnp.where(left[:1], back, turn(back)) if kind == GRAD else jnp.where(left[:1], turn(back), back)
            ahead = ahead + jnp.where(z >= r, jnp.exp(first), 0.0) * block
            behind = behind + jnp.where(z + outer - r < outer, jnp.exp(second), 0.0) * block
        carried = unfolded(ahead, behind) if kind == STATE else unfolded(behind, ahead)
        ends_ = endings(u)
        for person in everyone:
            factor = jnp.exp(pick(kind, sum(ends_[:person], zero), sum(ends_[person + 1:], zero)))
            c_out[kind, u, offset(person)] = (factor * carried + local[kind, u, person]).astype(BF16)
        for r in FAR_FIRST:
            c_copy(kind, r, u).start()

    def intra(todo):
        made = []
        for r, u in todo:
            s = slot(r, u)
            q_hat = q_hats[s]
            k_hat = (twice(k_v, r, u) * jnp.exp(-cum[s])).astype(BF16)
            v, seed = val[rows(r, u)], cot_v[owner(r), u]
            seed_scores = dot(seed, v, 1, 1)
            zero = jnp.zeros_like(q_hat)
            q_left, q_right = jnp.where(left, q_hat, zero), jnp.where(left, zero, q_hat)
            k_left, k_right = jnp.where(left, k_hat, zero), jnp.where(left, zero, k_hat)
            score = (jnp.where(lower, dot(q_left, k_hat, 1, 1), 0.0)
                     + jnp.where(upper, dot(q_right, k_hat, 1, 1), 0.0)).astype(BF16)
            seed_low = jnp.where(lower, seed_scores, 0.0).astype(BF16)
            seed_up = jnp.where(upper, seed_scores, 0.0).astype(BF16)
            made.append((dot(seed_low, k_left) + dot(seed_up, k_right),
                         dot(seed_low, q_left, 0, 0) + dot(seed_up, q_right, 0, 0),
                         dot(score, seed, 0, 0)))
        for (r, u), (for_q, for_k, for_v) in zip(todo, made):
            intra_q[slot(r, u)] = for_q
            intra_k[slot(r, u)] = for_k
            intra_v[slot(r, u)] = for_v

    def arrived(kind, r, u):
        return c_out[kind, u, 0] if r == 0 else c_in[kind, u, r - 1]

    def finish_values(todo):
        made = [intra_v[slot(r, u)] + dot(k_ends[slot(r, u)], arrived(GRAD, r, u), 1, 1) for r, u in todo]
        for (r, u), block in zip(todo, made):
            d_all[tpi, rows(r, u)] = block.astype(BF16)

    def finish_rest(todo):
        kept, terms = [], []
        for r, u in todo:
            s = slot(r, u)
            state, grad = arrived(STATE, r, u), arrived(GRAD, r, u)
            c = cum[s]
            end = ends(c)
            grow, shrink, to_end = jnp.exp(c), jnp.exp(-c), jnp.exp(end - c)
            q, k = twice(q_v, r, u), twice(k_v, r, u)
            cross = dot(cot_v[owner(r), u], state)
            dq = grow * (intra_q[s] + cross)
            dk_ = shrink * intra_k[s] + to_end * dot(val[rows(r, u)], grad)
            terms.append(q * dq - k * dk_)
            start = (jnp.sum(q * grow * cross, axis=0, keepdims=True)
                     + jnp.exp(end) * jnp.sum(state.astype(F32) * grad.astype(F32), axis=0, keepdims=True))
            kept.append((dq, dk_, start))
        for (r, u), (dq, dk_, start), sums_ in zip(todo, kept, directed(strict, terms)):
            b = batch_of(r, u)
            decay_grad = start - sums_
            o_q[b] = (dq[:, :dk] + dq[:, dk:]).astype(BF16)
            o_k[b] = (dk_[:, :dk] + dk_[:, dk:]).astype(BF16)
            o_f[b] = decay_grad[:, :dk]
            o_b[b] = decay_grad[:, dk:]

    def features(u):
        take(d_all.at[pl.ds(0, xs), rows(0, u, inner)], f_rs.at[u])
        at = rows(0, u, inner)
        wide = jnp.concatenate([d_all[t, at] for t in range(tp)], 1)
        weights = jnp.concatenate([w_in[t] for t in range(tp)], 1)
        out = dot(wide, weights, 1, 1).astype(BF16)
        for r in range(inner):
            o_h[batch_of(r, u)] = out[r * length:(r + 1) * length]

    def prepare_rest(todo):
        made = []
        for r, u in todo:
            b, at = batch_of(r, u), slot(r, u)
            c = cum[at]
            q, k = twice(q_v, r, u), twice(k_v, r, u)
            dk_ = (jnp.exp(-c) * intra_k[at]
                   + jnp.exp(ends(c) - c) * dot(val[rows(r, u)], arrived(GRAD, r, u)))
            o_k[b] = (dk_[:, :dk] + dk_[:, dk:]).astype(BF16)
            made.append(q * jnp.exp(c) * intra_q[at] - k * dk_)
        for (r, u), known in zip(todo, made):
            intra_k[slot(r, u)] = known

    def close_rest(todo):
        kept, terms = [], []
        for r, u in todo:
            at = slot(r, u)
            state, grad = arrived(STATE, r, u), arrived(GRAD, r, u)
            c = cum[at]
            grow = jnp.exp(c)
            cross = dot(cot_v[owner(r), u], state)
            far = twice(q_v, r, u) * grow * cross
            terms.append(intra_k[at] + far)
            start = (jnp.sum(far, axis=0, keepdims=True)
                     + jnp.exp(ends(c)) * jnp.sum(state.astype(F32) * grad.astype(F32), axis=0, keepdims=True))
            kept.append((grow * (intra_q[at] + cross), start))
        for (r, u), (dq, start), sums_ in zip(todo, kept, directed(strict, terms)):
            b = batch_of(r, u)
            decay_grad = start - sums_
            o_q[b] = (dq[:, :dk] + dq[:, dk:]).astype(BF16)
            o_f[b] = decay_grad[:, :dk]
            o_b[b] = decay_grad[:, dk:]

    def finish_own(u):
        finish_values([(0, u)])
        d_copies(0, u, 1)

    def finish_others(u):
        take(c_in.at[GRAD, u], c_rs.at[GRAD, u])
        finish_values([(r, u) for r in visitors])
        d_copies(1, u, inner - 1)

    def weight_terms(u):
        at = rows(0, u, inner)
        return dot(d_all[tpi, at], hid_v[at], 0, 0)

    def rest_others(u):
        take(c_in.at[STATE, u], c_rs.at[STATE, u])
        finish_rest([(r, u) for r in visitors])

    def loop(first, last, step):
        lax.fori_loop(first, last, lambda u, _: step(u) or 0, 0)

    def intra_all(u):
        intra([(r, u) for r in everyone])

    def first_steps(u):
        combine_plane(GRAD, u)
        intra_all(u)

    def second_steps(u):
        combine_all(GRAD, u)
        finish_own(u)
        combine_plane(STATE, u - 1)

    def weigh(u):
        finish_others(u)
        w_acc[...] += weight_terms(u)

    def pass_states(u):
        combine_all(STATE, u)
        finish_rest([(0, u)])

    def third_steps(u):
        weigh(u)
        pass_states(u)

    def fourth_steps(u):
        forward(u)
        rest_others(u)

    take(e_in.at[pl.ds(1, inner - 1)], e_rs.at[0])
    loop(0, end, first_steps)
    combine_plane(GRAD, end)
    combine_all(GRAD, 0)
    w_ends()
    finish_own(0)
    intra_all(end)
    loop(1, own, second_steps)
    send(STATE, end)
    loop(0, end - 1, third_steps)
    weigh(end - 1)

    finish_others(end)
    full = w_acc[...] + weight_terms(end)
    for p in range(0, sp, 2):
        block = full[:, p * rows_sp:(p + 2) * rows_sp].T.astype(BF16)
        g_out[p] = block[:rows_sp]
        g_out[p + 1] = block[rows_sp:]
    pass_states(end - 1)
    combine_plane(STATE, end)
    for away_by in OFFSETS:
        g_copy(*away_by).start()
    loop(0, end - 1, rest_others)
    combine_all(STATE, end)
    prepare_rest([(r, end) for r in visitors])
    loop(0, end, forward)
    finish_rest([(0, end)])
    forward(end)
    rest_others(end - 1)

    @pl.when(jnp.logical_not(inside))
    def _():
        take(w_in.at[pl.ds(0, CORES)], w_rs.at[2])

    loop(0, own, features)
    take(c_in.at[STATE, end], c_rs.at[STATE, end])
    close_rest([(r, end) for r in visitors])

    take(g_in, g_rs.at[0])
    acc = g_out[spi].astype(F32)
    for r in range(sp - 1):
        acc = acc + g_in[r].astype(F32)
    o_w[...] = acc

    take(w_in.at[pl.ds(0, tp - 1)], w_ss.at[0])
    take(e_in.at[pl.ds(1, inner - 1)], e_ss.at[0])
    take(d_all.at[pl.ds(0, tp - 2)], x_ss.at[0])
    take(b_in.at[GRAD], b_ss.at[GRAD])
    take(b_in.at[STATE, :, :, pl.ds(0, fold)], b_ss.at[STATE])
    take(d_all.at[pl.ds(0, tp - 1)], f_ss.at[0])
    take(g_in, g_ss.at[0])


def store_kernel(*refs):
    n = len(refs) // 2
    copies = [pltpu.make_async_copy(refs[i], refs[n + i], refs[-1].at[i]) for i in range(n)]
    for copy in copies:
        copy.start()
    for copy in copies:
        copy.wait()


def store(arrays):
    n = len(arrays)
    return pl.pallas_call(
        store_kernel,
        out_shape=tuple(jax.ShapeDtypeStruct(a.shape, a.dtype) for a in arrays),
        in_specs=[pl.BlockSpec(memory_space=pltpu.VMEM)] * n,
        out_specs=(pl.BlockSpec(memory_space=pl.ANY),) * n,
        scratch_shapes=[pltpu.SemaphoreType.DMA((n,))],
        compiler_params=pltpu.CompilerParams(has_side_effects=True, vmem_limit_bytes=1024 * 1024),
    )(*arrays)


def shards(sp, tp, hidden, value_weight, queries, key_vectors, forward_decay, backward_decay, cotangent):
    batch, length, width = hidden.shape
    heads, dk = queries.shape[1], queries.shape[3]
    dv = value_weight.shape[1]
    assert heads == 1
    inner, outer, own, xs = INNER, sp // INNER, batch // INNER, tp // CORES
    pack, rows, feat, rows_sp = 2 * dk, batch * length, width // tp, width // sp
    dims = (sp, tp, batch, length, dk, dv, width)
    vmem, dma = pltpu.VMEM, pltpu.SemaphoreType.DMA
    scratch = [
        vmem((rows, width), BF16), vmem((width, dv), BF16),
        vmem((inner, own, length, dk), BF16), vmem((inner, own, length, dk), BF16),
        vmem((2, inner, own, length, dk), F32), vmem((inner, own, length, dv), BF16),
        vmem((rows, dv), BF16),
        vmem((batch, length, pack), F32),
        vmem((batch, length, pack), BF16), vmem((batch, length, pack), BF16),
        vmem((batch, length, pack), F32), vmem((batch, length, pack), F32),
        vmem((batch, length, dv), F32),
        vmem((2, own, inner - 1, dv, pack), BF16), vmem((2, own, inner, dv, pack), BF16),
        vmem((inner, own, pack), F32), vmem((inner, own, pack), F32),
        vmem((2, own, inner, dv, pack), F32),
        vmem((2, own, 2, dv // 2 + TAIL, pack), BF16), vmem((2, own, outer - 1, dv // 2 + TAIL, pack), BF16),
        vmem((2, own, inner, dv, pack), BF16), vmem((2, own, inner - 1, dv, pack), BF16),
        vmem((tp, rows, dv), BF16), vmem((tp, feat, dv), BF16),
        vmem((dv, width), F32),
        vmem((sp, rows_sp, dv), BF16), vmem((sp - 1, rows_sp, dv), BF16),
        dma((8,)), dma((own,)),
        dma((1,)), dma((2, own)),
        dma((1,)), dma((1,)),
        dma((2,)), dma((2, own)),
        dma((2, own)),
        dma((own,)),
        dma((1,)), dma((own,)),
        dma((1,)), dma((3,)),
        dma((1,)), dma((1,)),
    ]
    whole = pl.BlockSpec(memory_space=vmem)
    flat, split = (batch, length, dk), (inner, own, length, dk)
    args = (hidden.reshape(inner, own, length, width), value_weight, queries.reshape(split),
            key_vectors.reshape(split), forward_decay.reshape(split), backward_decay.reshape(split),
            cotangent.reshape(inner, own, length, dv))
    outs = pl.pallas_call(
        functools.partial(kernel, dims),
        out_shape=(
            vmem(flat, BF16), vmem(flat, BF16), vmem(flat, F32), vmem(flat, F32),
            vmem((batch, length, feat), BF16), vmem((rows_sp, dv), F32),
        ),
        in_specs=[pl.BlockSpec(memory_space=pltpu.HBM)] * 7,
        out_specs=(whole,) * 6,
        scratch_shapes=scratch,
        compiler_params=pltpu.CompilerParams(
            collective_id=0, has_side_effects=True, vmem_limit_bytes=48 * 1024 * 1024
        ),
    )(*(pltpu.with_memory_space_constraint(a, pltpu.HBM) for a in args))
    outs = store(outs)
    return tuple(a.reshape(queries.shape) for a in outs[:4]) + tuple(outs[4:])


def solution(mesh):
    heads = P(None, "tp", "sp", None)
    return jax.shard_map(
        functools.partial(shards, mesh.shape["sp"], mesh.shape["tp"]),
        mesh=mesh,
        in_specs=(P(None, "sp", None), P(None, "tp"), heads, heads, heads, heads, P(None, "sp", "tp")),
        out_specs=(heads, heads, heads, heads, P(None, "sp", "tp"), P("sp", "tp")),
        check_vma=False,
    )
```

```python
import functools

import jax
import jax.numpy as jnp
from jax import lax
from jax.experimental import pallas as pl
from jax.experimental.pallas import tpu as pltpu
from jax.sharding import PartitionSpec as P

F32, BF16 = jnp.float32, jnp.bfloat16
MESH = pl.DeviceIdType.MESH
CORES = 2
INNER = 4
TAIL = 16
GRAD, STATE = 0, 1
FAR_FIRST = (2, 1, 3)
OFFSETS = sorted(((dz, dy) for dz in range(4) for dy in range(4) if dz or dy),
                 key=lambda d: (-min(d[1], 4 - d[1]), -min(d[0], 4 - d[0])))


def dot(a, b, ca=1, cb=0):
    return lax.dot_general(a, b, (((ca,), (cb,)), ((), ())), preferred_element_type=F32)


def halves(x):
    high = x.astype(BF16)
    return jnp.concatenate([high, (x - high.astype(F32)).astype(BF16)], 0)


def kernel(dims, hid, wgt, qry, key, fdec, bdec, cot,
           o_q, o_k, o_f, o_b, o_h, o_w,
           hid_v, wgt_v, q_v, k_v, decay_v, cot_v,
           val, cum, q_hats, k_ends, intra_q, intra_k, intra_v,
           a_out, a_in, e_out, e_in, local, b_out, b_in, c_out, c_in,
           d_all, w_in, w_acc, g_out, g_in,
           i_s, h_s, x_ss, a_rs, e_ss, e_rs, b_ss, b_rs, c_rs,
           d_rs, f_ss, f_rs, w_ss, w_rs, g_ss, g_rs):
    sp, tp, batch, length, dk, dv, width = dims
    inner, outer, own, xs = INNER, sp // INNER, batch // INNER, tp // CORES
    pack, feat, rows_sp, group = 2 * dk, width // tp, width // sp, INNER * length
    fold = dv // 2
    spi, tpi = lax.axis_index("sp"), lax.axis_index("tp")
    z, y = spi // inner, lax.rem(spi, inner)
    x, core = tpi // CORES, lax.rem(tpi, CORES)

    barrier = pltpu.get_barrier_semaphore()
    mate = x * CORES + 1 - core
    inside = (x > 0) & (x < xs - 1)
    def owner(r):
        return lax.rem(y + r, inner)

    def batch_of(r, u):
        return owner(r) * own + u

    def slot(r, u):
        return u * inner + r

    def rows(r, u, count=1):
        return pl.ds(pl.multiple_of(slot(r, u) * length, length), count * length)

    def away(dz, dy):
        return lax.rem(z + dz, outer) * inner + lax.rem(y + dy, inner)

    def take(ref, sem):
        pltpu.make_async_copy(ref, ref, sem).wait()

    def load(first, count):
        at, n = pl.ds(first, count), min(first, 1)
        for i in range(2):
            pltpu.make_async_copy((fdec, bdec)[i].at[:, at], decay_v.at[i, :, at], i_s.at[n]).start()
        pltpu.make_async_copy(qry.at[:, at], q_v.at[:, at], i_s.at[2 + n]).start()
        pltpu.make_async_copy(cot.at[:, at], cot_v.at[:, at], i_s.at[4 + n]).start()

    def loaded(first, count):
        at, n = pl.ds(first, count), min(first, 1)
        take(decay_v.at[:, :, at], i_s.at[n])
        take(q_v.at[:, at], i_s.at[2 + n])
        take(cot_v.at[:, at], i_s.at[4 + n])

    def load_hidden(u):
        for r in range(inner):
            pltpu.make_async_copy(hid.at[owner(r), u], hid_v.at[rows(r, u)], h_s.at[u]).start()

    load(0, 1)
    for r in range(1, outer):
        pl.semaphore_signal(barrier, inc=1, device_id={"sp": away(r, 0)}, device_id_type=MESH)
    for r in range(1, inner):
        pl.semaphore_signal(barrier, inc=1, device_id={"sp": away(0, r)}, device_id_type=MESH)
    pl.semaphore_signal(barrier, inc=1, device_id={"tp": mate}, device_id_type=MESH)
    for step in (1, -1):
        @pl.when((x + step >= 0) & (x + step < xs))
        def _():
            for c in range(CORES):
                pl.semaphore_signal(barrier, inc=1, device_id={"tp": jnp.clip(x + step, 0, xs - 1) * CORES + c},
                                    device_id_type=MESH)

    pltpu.make_async_copy(wgt, wgt_v, i_s.at[6]).start()
    load_hidden(0)
    pltpu.make_async_copy(key, k_v, i_s.at[7]).start()
    load(1, own - 1)
    for u in range(1, own):
        load_hidden(u)

    def remote(src, dst, ss, rs, **where):
        return pltpu.make_async_remote_copy(src_ref=src, dst_ref=dst, send_sem=ss, recv_sem=rs,
                                            device_id=where, device_id_type=MESH)

    def w_copy(to, phase):
        return remote(wgt_v.at[pl.ds(pl.multiple_of(to * feat, feat), feat), :], w_in.at[tpi],
                      w_ss.at[0], w_rs.at[phase], tp=to)

    def w_near():
        w_copy(mate, 0).start()
        for step in (1, -1):
            @pl.when((x + step >= 0) & (x + step < xs))
            def _():
                for c in range(CORES):
                    w_copy(jnp.clip(x + step, 0, xs - 1) * CORES + c, 0).start()

    def w_across():
        for many in range(2):
            @pl.when(inside if many else jnp.logical_not(inside))
            def _():
                take(w_in.at[pl.ds(0, 1 + CORES * (1 + many))], w_rs.at[0])
        for c in range(CORES):
            w_copy(lax.rem(x + 2, xs) * CORES + c, 1).start()

    def w_ends():
        take(w_in.at[pl.ds(0, CORES)], w_rs.at[1])

        @pl.when(jnp.logical_not(inside))
        def _():
            for c in range(CORES):
                w_copy((xs - 1 - x) * CORES + c, 2).start()

    def a_copy(kind, r, u):
        return remote(a_out.at[kind, u, r - 1], a_in.at[kind, u, r], x_ss.at[0], a_rs.at[kind, u],
                      sp=z * inner + owner(r))

    def e_copy(r):
        return remote(e_out.at[owner(r)], e_in.at[r], e_ss.at[0], e_rs.at[0], sp=z * inner + owner(r))

    def b_part(ref, kind):
        return ref if kind == GRAD else ref.at[pl.ds(0, fold)]

    def b_copy(kind, r, u):
        way = jnp.where(z + r < outer, 0, 1)
        return remote(b_part(b_out.at[kind, u, way], kind), b_part(b_in.at[kind, u, r - 1], kind),
                      b_ss.at[kind], b_rs.at[kind, u], sp=lax.rem(z + r, outer) * inner + y)

    def c_copy(kind, r, u):
        return remote(c_out.at[kind, u, r], c_in.at[kind, u, r - 1], x_ss.at[0], c_rs.at[kind, u],
                      sp=z * inner + lax.rem(y - r + inner, inner))

    def d_copies(r, u, count):
        at = rows(r, u, count)
        for k in FAR_FIRST:
            remote(d_all.at[tpi, at], d_all.at[tpi, at], f_ss.at[0], d_rs.at[u],
                   tp=lax.rem(x + k, xs) * CORES + core).start()
        remote(d_all.at[tpi, at], d_all.at[tpi, at], f_ss.at[0], f_rs.at[u], tp=mate).start()

    def forward(u):
        at = rows(0, u, inner)
        take(d_all.at[pl.ds(0, xs - 1), at], d_rs.at[u])
        for k in range(1, xs):
            mine = d_all.at[lax.rem(x - k + xs, xs) * CORES + core, at]
            remote(mine, mine, f_ss.at[0], f_rs.at[u], tp=mate).start()

    def g_copy(dz, dy):
        to = away(dz, dy)
        return remote(g_out.at[to], g_in.at[dz * inner + dy - 1], g_ss.at[0], g_rs.at[0], sp=to)

    row = lax.broadcasted_iota(jnp.int32, (length, length), 0)
    col = lax.broadcasted_iota(jnp.int32, (length, length), 1)
    lower, upper = row >= col, row <= col

    def matrix(first, second):
        both = jnp.concatenate([jnp.where(first, 1.0, 0.0), jnp.where(second, 1.0, 0.0)], 0)
        return jnp.concatenate([both, both], 1).astype(BF16)

    sums, strict = matrix(lower, upper), matrix(row > col, row < col)
    left = lax.broadcasted_iota(jnp.int32, (length, pack), 1) < dk
    left_fold = lax.broadcasted_iota(jnp.int32, (fold, pack), 1) < dk
    tail_row = lax.broadcasted_iota(jnp.int32, (TAIL, pack), 0)
    left_tall = lax.broadcasted_iota(jnp.int32, (dv, pack), 1) < dk

    def directed(tri, blocks):
        made = []
        for i in range(0, len(blocks), 2):
            pair = blocks[i:i + 2]
            out = dot(tri, halves(jnp.concatenate(pair, 1) if len(pair) > 1 else pair[0]))
            for n in range(len(pair)):
                part = out[:, n * pack:(n + 1) * pack]
                made.append(jnp.where(left, part[:length], part[length:]))
        return made

    def twice(ref, r, u):
        v = ref[owner(r), u].astype(F32)
        return jnp.concatenate([v, v], 1)

    def ends(c):
        return jnp.where(left[:1], c[length - 1:length], c[0:1])

    def decays(todo):
        blocks = [jnp.concatenate([decay_v[0, owner(r), u], decay_v[1, owner(r), u]], 1) for r, u in todo]
        made = directed(sums, blocks)
        for (r, u), c in zip(todo, made):
            cum[slot(r, u)] = c
        for (r, u), c in zip(todo, made):
            e_out[owner(r), pl.ds(u, 1), :] = ends(c)

    def grads(todo):
        hats = [(twice(q_v, r, u) * jnp.exp(cum[slot(r, u)])).astype(BF16) for r, u in todo]
        made = [dot(cot_v[owner(r), u], hat, 0, 0).astype(BF16) for (r, u), hat in zip(todo, hats)]
        return hats, made

    def states(todo):
        keys = []
        for r, u in todo:
            c = cum[slot(r, u)]
            keys.append((twice(k_v, r, u) * jnp.exp(ends(c) - c)).astype(BF16))
        made = [dot(val[rows(r, u)], k_end, 0, 0).astype(BF16) for (r, u), k_end in zip(todo, keys)]
        return keys, made

    def place(kind, r, u, value):
        if r == 0:
            a_in[kind, u, 0] = value
        else:
            a_out[kind, u, r - 1] = value

    def emit(kind, todo):
        kept, made = (grads if kind == 0 else states)(todo)
        keep = q_hats if kind == 0 else k_ends
        for (r, u), value, block in zip(todo, kept, made):
            keep[slot(r, u)] = value
            place(kind, r, u, block)

    def values(u):
        at = rows(0, u, inner)
        val[at] = dot(hid_v[at], wgt_v[...]).astype(BF16)

    everyone, visitors = tuple(range(inner)), tuple(range(1, inner))

    def send(kind, u):
        for r in FAR_FIRST:
            a_copy(kind, r, u).start()

    loaded(0, 1)
    decays([(r, 0) for r in everyone])
    emit(GRAD, [(r, 0) for r in visitors])
    pl.semaphore_wait(barrier, inner + outer - 1 + jnp.where(inside, 2 * CORES, CORES))
    send(GRAD, 0)
    loaded(1, own - 1)
    decays([(r, u) for u in range(1, own) for r in everyone])
    for r in FAR_FIRST:
        e_copy(r).start()
    e_in[0] = e_out[y]
    for u in range(1, own):
        emit(GRAD, [(r, u) for r in visitors])
        send(GRAD, u)

    end = own - 1
    take(wgt_v, i_s.at[6])
    w_near()
    take(k_v, i_s.at[7])
    for u in range(own):
        take(hid_v.at[rows(0, u, inner)], h_s.at[u])
        values(u)
        emit(STATE, [(r, u) for r in visitors])
        if u < end:
            send(STATE, u)

    w_in[tpi] = wgt_v[pl.ds(pl.multiple_of(tpi * feat, feat), feat), :]
    mine = [(0, u) for u in range(own)]
    emit(GRAD, mine)
    emit(STATE, mine)
    w_acc[...] = jnp.zeros((dv, width), F32)
    w_across()

    def offset(person):
        return lax.rem(y - person + inner, inner)

    def endings(u):
        return [e_in[offset(person), pl.ds(u, 1), :] for person in everyone]

    def pick(kind, ahead, behind):
        at = left_tall if ahead.shape[0] == dv else left[:1]
        return jnp.where(at, ahead, behind) if kind == STATE else jnp.where(at, behind, ahead)

    def turn(v):
        return pltpu.roll(v, dk, 1)

    def folded(v, first):
        if first:
            return jnp.where(left_fold, v[:fold], turn(v[fold:]))
        return jnp.where(left_fold, turn(v[:fold]), v[fold:])

    def unfolded(first, second):
        return jnp.concatenate([jnp.where(left_fold, first, turn(second)),
                                jnp.where(left_fold, turn(first), second)], 0)

    def running(blocks, factors, order):
        total, before = None, [None] * inner
        for person in order:
            before[person] = jnp.zeros((dv, pack), F32) if total is None else total
            total = blocks[person] if total is None else factors[person] * total + blocks[person]
        return before, total

    def combine_plane(kind, u):
        take(a_in.at[kind, u, pl.ds(1, inner - 1)], a_rs.at[kind, u])
        blocks = [a_in[kind, u, offset(person)].astype(F32) for person in everyone]
        ends_ = endings(u)
        factors = [jnp.exp(e) for e in ends_]
        before, total = running(blocks, factors, everyone)
        after, total_back = running(blocks, factors, everyone[::-1])
        for person in everyone:
            local[kind, u, person] = pick(kind, before[person], after[person])
        b_out[kind, u, 0, pl.ds(0, fold)] = folded(total, kind == STATE).astype(BF16)
        b_out[kind, u, 1, pl.ds(0, fold)] = folded(total_back, kind == GRAD).astype(BF16)
        if kind == GRAD:
            whole = sum(ends_[1:], ends_[0])
            high = whole.astype(BF16).astype(F32)
            tail = jnp.where(tail_row == 0, high, jnp.where(tail_row == 1, whole - high, 0.0)).astype(BF16)
            for way in range(2):
                b_out[kind, u, way, pl.ds(fold, TAIL)] = tail
        for r in FAR_FIRST:
            b_copy(kind, r, u).start()

    def combine_all(kind, u):
        take(b_in.at[GRAD, u] if kind == GRAD else b_in.at[STATE, u, :, pl.ds(0, fold)], b_rs.at[kind, u])
        planes = [None]
        for r in range(1, outer):
            tail = b_in[GRAD, u, r - 1, pl.ds(fold, TAIL)].astype(F32)
            planes.append(tail[0:1] + tail[1:2])
        zero = jnp.zeros((1, pack), F32)
        ahead, behind = jnp.zeros((fold, pack), F32), jnp.zeros((fold, pack), F32)
        for r in range(1, outer):
            block = b_in[kind, u, r - 1, pl.ds(0, fold)].astype(F32)
            passed, back = sum(planes[1:r], zero), sum(planes[r + 1:], zero)
            first = jnp.where(left[:1], passed, turn(passed)) if kind == STATE else jnp.where(left[:1], turn(passed), passed)
            second = jnp.where(left[:1], back, turn(back)) if kind == GRAD else jnp.where(left[:1], turn(back), back)
            ahead = ahead + jnp.where(z >= r, jnp.exp(first), 0.0) * block
            behind = behind + jnp.where(z + outer - r < outer, jnp.exp(second), 0.0) * block
        carried = unfolded(ahead, behind) if kind == STATE else unfolded(behind, ahead)
        ends_ = endings(u)
        for person in everyone:
            factor = jnp.exp(pick(kind, sum(ends_[:person], zero), sum(ends_[person + 1:], zero)))
            c_out[kind, u, offset(person)] = (factor * carried + local[kind, u, person]).astype(BF16)
        for r in FAR_FIRST:
            c_copy(kind, r, u).start()

    def intra(todo):
        made = []
        for r, u in todo:
            s = slot(r, u)
            q_hat = q_hats[s]
            k_hat = (twice(k_v, r, u) * jnp.exp(-cum[s])).astype(BF16)
            v, seed = val[rows(r, u)], cot_v[owner(r), u]
            seed_scores = dot(seed, v, 1, 1)
            zero = jnp.zeros_like(q_hat)
            q_left, q_right = jnp.where(left, q_hat, zero), jnp.where(left, zero, q_hat)
            k_left, k_right = jnp.where(left, k_hat, zero), jnp.where(left, zero, k_hat)
            score = (jnp.where(lower, dot(q_left, k_hat, 1, 1), 0.0)
                     + jnp.where(upper, dot(q_right, k_hat, 1, 1), 0.0)).astype(BF16)
            seed_low = jnp.where(lower, seed_scores, 0.0).astype(BF16)
            seed_up = jnp.where(upper, seed_scores, 0.0).astype(BF16)
            made.append((dot(seed_low, k_left) + dot(seed_up, k_right),
                         dot(seed_low, q_left, 0, 0) + dot(seed_up, q_right, 0, 0),
                         dot(score, seed, 0, 0)))
        for (r, u), (for_q, for_k, for_v) in zip(todo, made):
            intra_q[slot(r, u)] = for_q
            intra_k[slot(r, u)] = for_k
            intra_v[slot(r, u)] = for_v

    def arrived(kind, r, u):
        return c_out[kind, u, 0] if r == 0 else c_in[kind, u, r - 1]

    def finish_values(todo):
        made = [intra_v[slot(r, u)] + dot(k_ends[slot(r, u)], arrived(GRAD, r, u), 1, 1) for r, u in todo]
        for (r, u), block in zip(todo, made):
            d_all[tpi, rows(r, u)] = block.astype(BF16)

    def finish_rest(todo):
        kept, terms = [], []
        for r, u in todo:
            s = slot(r, u)
            state, grad = arrived(STATE, r, u), arrived(GRAD, r, u)
            c = cum[s]
            end = ends(c)
            grow, shrink, to_end = jnp.exp(c), jnp.exp(-c), jnp.exp(end - c)
            q, k = twice(q_v, r, u), twice(k_v, r, u)
            cross = dot(cot_v[owner(r), u], state)
            dq = grow * (intra_q[s] + cross)
            dk_ = shrink * intra_k[s] + to_end * dot(val[rows(r, u)], grad)
            terms.append(q * dq - k * dk_)
            start = (jnp.sum(q * grow * cross, axis=0, keepdims=True)
                     + jnp.exp(end) * jnp.sum(state.astype(F32) * grad.astype(F32), axis=0, keepdims=True))
            kept.append((dq, dk_, start))
        for (r, u), (dq, dk_, start), sums_ in zip(todo, kept, directed(strict, terms)):
            b = batch_of(r, u)
            decay_grad = start - sums_
            o_q[b] = (dq[:, :dk] + dq[:, dk:]).astype(BF16)
            o_k[b] = (dk_[:, :dk] + dk_[:, dk:]).astype(BF16)
            o_f[b] = decay_grad[:, :dk]
            o_b[b] = decay_grad[:, dk:]

    def features(u):
        take(d_all.at[pl.ds(0, xs), rows(0, u, inner)], f_rs.at[u])
        at = rows(0, u, inner)
        wide = jnp.concatenate([d_all[t, at] for t in range(tp)], 1)
        weights = jnp.concatenate([w_in[t] for t in range(tp)], 1)
        out = dot(wide, weights, 1, 1).astype(BF16)
        for r in range(inner):
            o_h[batch_of(r, u)] = out[r * length:(r + 1) * length]

    def prepare_rest(todo):
        made = []
        for r, u in todo:
            b, at = batch_of(r, u), slot(r, u)
            c = cum[at]
            q, k = twice(q_v, r, u), twice(k_v, r, u)
            dk_ = (jnp.exp(-c) * intra_k[at]
                   + jnp.exp(ends(c) - c) * dot(val[rows(r, u)], arrived(GRAD, r, u)))
            o_k[b] = (dk_[:, :dk] + dk_[:, dk:]).astype(BF16)
            made.append(q * jnp.exp(c) * intra_q[at] - k * dk_)
        for (r, u), known in zip(todo, made):
            intra_k[slot(r, u)] = known

    def close_rest(todo):
        kept, terms = [], []
        for r, u in todo:
            at = slot(r, u)
            state, grad = arrived(STATE, r, u), arrived(GRAD, r, u)
            c = cum[at]
            grow = jnp.exp(c)
            cross = dot(cot_v[owner(r), u], state)
            far = twice(q_v, r, u) * grow * cross
            terms.append(intra_k[at] + far)
            start = (jnp.sum(far, axis=0, keepdims=True)
                     + jnp.exp(ends(c)) * jnp.sum(state.astype(F32) * grad.astype(F32), axis=0, keepdims=True))
            kept.append((grow * (intra_q[at] + cross), start))
        for (r, u), (dq, start), sums_ in zip(todo, kept, directed(strict, terms)):
            b = batch_of(r, u)
            decay_grad = start - sums_
            o_q[b] = (dq[:, :dk] + dq[:, dk:]).astype(BF16)
            o_f[b] = decay_grad[:, :dk]
            o_b[b] = decay_grad[:, dk:]

    def finish_own(u):
        finish_values([(0, u)])
        d_copies(0, u, 1)

    def finish_others(u):
        take(c_in.at[GRAD, u], c_rs.at[GRAD, u])
        finish_values([(r, u) for r in visitors])
        d_copies(1, u, inner - 1)

    def weight_terms(u):
        at = rows(0, u, inner)
        return dot(d_all[tpi, at], hid_v[at], 0, 0)

    def rest_others(u):
        take(c_in.at[STATE, u], c_rs.at[STATE, u])
        finish_rest([(r, u) for r in visitors])

    def loop(first, last, step):
        lax.fori_loop(first, last, lambda u, _: step(u) or 0, 0)

    def intra_all(u):
        intra([(r, u) for r in everyone])

    def first_steps(u):
        combine_plane(GRAD, u)
        intra_all(u)

    def second_steps(u):
        combine_all(GRAD, u)
        finish_own(u)
        combine_plane(STATE, u - 1)

    def weigh(u):
        finish_others(u)
        w_acc[...] += weight_terms(u)

    def pass_states(u):
        combine_all(STATE, u)
        finish_rest([(0, u)])

    def third_steps(u):
        weigh(u)
        pass_states(u)

    def fourth_steps(u):
        forward(u)
        rest_others(u)

    take(e_in.at[pl.ds(1, inner - 1)], e_rs.at[0])
    loop(0, end, first_steps)
    combine_plane(GRAD, end)
    combine_all(GRAD, 0)
    w_ends()
    finish_own(0)
    intra_all(end)
    loop(1, own, second_steps)
    send(STATE, end)
    loop(0, end - 1, third_steps)
    weigh(end - 1)

    finish_others(end)
    full = w_acc[...] + weight_terms(end)
    for p in range(0, sp, 2):
        block = full[:, p * rows_sp:(p + 2) * rows_sp].T.astype(BF16)
        g_out[p] = block[:rows_sp]
        g_out[p + 1] = block[rows_sp:]
    pass_states(end - 1)
    combine_plane(STATE, end)
    for away_by in OFFSETS:
        g_copy(*away_by).start()
    loop(0, end - 1, rest_others)
    combine_all(STATE, end)
    prepare_rest([(r, end) for r in visitors])
    loop(0, end, forward)
    finish_rest([(0, end)])
    forward(end)
    rest_others(end - 1)

    @pl.when(jnp.logical_not(inside))
    def _():
        take(w_in.at[pl.ds(0, CORES)], w_rs.at[2])

    loop(0, own, features)
    take(c_in.at[STATE, end], c_rs.at[STATE, end])
    close_rest([(r, end) for r in visitors])

    take(g_in, g_rs.at[0])
    acc = g_out[spi].astype(F32)
    for r in range(sp - 1):
        acc = acc + g_in[r].astype(F32)
    o_w[...] = acc

    take(w_in.at[pl.ds(0, tp - 1)], w_ss.at[0])
    take(e_in.at[pl.ds(1, inner - 1)], e_ss.at[0])
    take(d_all.at[pl.ds(0, tp - 2)], x_ss.at[0])
    take(b_in.at[GRAD], b_ss.at[GRAD])
    take(b_in.at[STATE, :, :, pl.ds(0, fold)], b_ss.at[STATE])
    take(d_all.at[pl.ds(0, tp - 1)], f_ss.at[0])
    take(g_in, g_ss.at[0])


def store_kernel(*refs):
    n = len(refs) // 2
    copies = [pltpu.make_async_copy(refs[i], refs[n + i], refs[-1].at[i]) for i in range(n)]
    for copy in copies:
        copy.start()
    for copy in copies:
        copy.wait()


def store(arrays):
    n = len(arrays)
    return pl.pallas_call(
        store_kernel,
        out_shape=tuple(jax.ShapeDtypeStruct(a.shape, a.dtype) for a in arrays),
        in_specs=[pl.BlockSpec(memory_space=pltpu.VMEM)] * n,
        out_specs=(pl.BlockSpec(memory_space=pl.ANY),) * n,
        scratch_shapes=[pltpu.SemaphoreType.DMA((n,))],
        compiler_params=pltpu.CompilerParams(has_side_effects=True, vmem_limit_bytes=1024 * 1024),
    )(*arrays)


def shards(sp, tp, hidden, value_weight, queries, key_vectors, forward_decay, backward_decay, cotangent):
    batch, length, width = hidden.shape
    heads, dk = queries.shape[1], queries.shape[3]
    dv = value_weight.shape[1]
    assert heads == 1
    inner, outer, own, xs = INNER, sp // INNER, batch // INNER, tp // CORES
    pack, rows, feat, rows_sp = 2 * dk, batch * length, width // tp, width // sp
    dims = (sp, tp, batch, length, dk, dv, width)
    vmem, dma = pltpu.VMEM, pltpu.SemaphoreType.DMA
    scratch = [
        vmem((rows, width), BF16), vmem((width, dv), BF16),
        vmem((inner, own, length, dk), BF16), vmem((inner, own, length, dk), BF16),
        vmem((2, inner, own, length, dk), F32), vmem((inner, own, length, dv), BF16),
        vmem((rows, dv), BF16),
        vmem((batch, length, pack), F32),
        vmem((batch, length, pack), BF16), vmem((batch, length, pack), BF16),
        vmem((batch, length, pack), F32), vmem((batch, length, pack), F32),
        vmem((batch, length, dv), F32),
        vmem((2, own, inner - 1, dv, pack), BF16), vmem((2, own, inner, dv, pack), BF16),
        vmem((inner, own, pack), F32), vmem((inner, own, pack), F32),
        vmem((2, own, inner, dv, pack), F32),
        vmem((2, own, 2, dv // 2 + TAIL, pack), BF16), vmem((2, own, outer - 1, dv // 2 + TAIL, pack), BF16),
        vmem((2, own, inner, dv, pack), BF16), vmem((2, own, inner - 1, dv, pack), BF16),
        vmem((tp, rows, dv), BF16), vmem((tp, feat, dv), BF16),
        vmem((dv, width), F32),
        vmem((sp, rows_sp, dv), BF16), vmem((sp - 1, rows_sp, dv), BF16),
        dma((8,)), dma((own,)),
        dma((1,)), dma((2, own)),
        dma((1,)), dma((1,)),
        dma((2,)), dma((2, own)),
        dma((2, own)),
        dma((own,)),
        dma((1,)), dma((own,)),
        dma((1,)), dma((3,)),
        dma((1,)), dma((1,)),
    ]
    whole = pl.BlockSpec(memory_space=vmem)
    flat, split = (batch, length, dk), (inner, own, length, dk)
    args = (hidden.reshape(inner, own, length, width), value_weight, queries.reshape(split),
            key_vectors.reshape(split), forward_decay.reshape(split), backward_decay.reshape(split),
            cotangent.reshape(inner, own, length, dv))
    outs = pl.pallas_call(
        functools.partial(kernel, dims),
        out_shape=(
            vmem(flat, BF16), vmem(flat, BF16), vmem(flat, F32), vmem(flat, F32),
            vmem((batch, length, feat), BF16), vmem((rows_sp, dv), F32),
        ),
        in_specs=[pl.BlockSpec(memory_space=pltpu.HBM)] * 7,
        out_specs=(whole,) * 6,
        scratch_shapes=scratch,
        compiler_params=pltpu.CompilerParams(
            collective_id=0, has_side_effects=True, vmem_limit_bytes=48 * 1024 * 1024
        ),
    )(*(pltpu.with_memory_space_constraint(a, pltpu.HBM) for a in args))
    outs = store(outs)
    return tuple(a.reshape(queries.shape) for a in outs[:4]) + tuple(outs[4:])


def solution(mesh):
    heads = P(None, "tp", "sp", None)
    return jax.shard_map(
        functools.partial(shards, mesh.shape["sp"], mesh.shape["tp"]),
        mesh=mesh,
        in_specs=(P(None, "sp", None), P(None, "tp"), heads, heads, heads, heads, P(None, "sp", "tp")),
        out_specs=(heads, heads, heads, heads, P(None, "sp", "tp"), P("sp", "tp")),
        check_vma=False,
    )
```

```python
import functools

import jax
import jax.numpy as jnp
from jax import lax
from jax.experimental import pallas as pl
from jax.experimental.pallas import tpu as pltpu
from jax.sharding import PartitionSpec as P

F32, BF16 = jnp.float32, jnp.bfloat16
MESH = pl.DeviceIdType.MESH
CORES = 2
INNER = 4
TAIL = 16
GRAD, STATE = 0, 1
FAR_FIRST = (2, 1, 3)
OFFSETS = sorted(((dz, dy) for dz in range(4) for dy in range(4) if dz or dy),
                 key=lambda d: -sum(min(v, 4 - v) for v in d))


def dot(a, b, ca=1, cb=0):
    return lax.dot_general(a, b, (((ca,), (cb,)), ((), ())), preferred_element_type=F32)


def halves(x):
    high = x.astype(BF16)
    return jnp.concatenate([high, (x - high.astype(F32)).astype(BF16)], 0)


def kernel(dims, hid, wgt, qry, key, fdec, bdec, cot,
           o_q, o_k, o_f, o_b, o_h, o_w,
           hid_v, wgt_v, q_v, k_v, decay_v, cot_v,
           val, cum, q_hats, k_ends, intra_q, intra_k, intra_v,
           a_out, a_in, e_out, e_in, local, b_out, b_in, c_out, c_in,
           d_all, w_in, w_acc, g_out, g_in,
           i_s, h_s, x_ss, a_rs, e_ss, e_rs, b_ss, b_rs, c_rs,
           d_rs, f_ss, f_rs, w_ss, w_rs, g_ss, g_rs):
    sp, tp, batch, length, dk, dv, width = dims
    inner, outer, own, xs = INNER, sp // INNER, batch // INNER, tp // CORES
    pack, feat, rows_sp, group = 2 * dk, width // tp, width // sp, INNER * length
    fold = dv // 2
    spi, tpi = lax.axis_index("sp"), lax.axis_index("tp")
    z, y = spi // inner, lax.rem(spi, inner)
    x, core = tpi // CORES, lax.rem(tpi, CORES)

    barrier = pltpu.get_barrier_semaphore()
    mate = x * CORES + 1 - core
    inside = (x > 0) & (x < xs - 1)
    def owner(r):
        return lax.rem(y + r, inner)

    def batch_of(r, u):
        return owner(r) * own + u

    def slot(r, u):
        return u * inner + r

    def rows(r, u, count=1):
        return pl.ds(pl.multiple_of(slot(r, u) * length, length), count * length)

    def away(dz, dy):
        return lax.rem(z + dz, outer) * inner + lax.rem(y + dy, inner)

    def take(ref, sem):
        pltpu.make_async_copy(ref, ref, sem).wait()

    def load(first, count):
        at, n = pl.ds(first, count), min(first, 1)
        for i in range(2):
            pltpu.make_async_copy((fdec, bdec)[i].at[:, at], decay_v.at[i, :, at], i_s.at[n]).start()
        pltpu.make_async_copy(qry.at[:, at], q_v.at[:, at], i_s.at[2 + n]).start()
        pltpu.make_async_copy(cot.at[:, at], cot_v.at[:, at], i_s.at[4 + n]).start()

    def loaded(first, count):
        at, n = pl.ds(first, count), min(first, 1)
        take(decay_v.at[:, :, at], i_s.at[n])
        take(q_v.at[:, at], i_s.at[2 + n])
        take(cot_v.at[:, at], i_s.at[4 + n])

    def load_hidden(u):
        for r in range(inner):
            pltpu.make_async_copy(hid.at[owner(r), u], hid_v.at[rows(r, u)], h_s.at[u]).start()

    load(0, 1)
    for r in range(1, outer):
        pl.semaphore_signal(barrier, inc=1, device_id={"sp": away(r, 0)}, device_id_type=MESH)
    for r in range(1, inner):
        pl.semaphore_signal(barrier, inc=1, device_id={"sp": away(0, r)}, device_id_type=MESH)
    pl.semaphore_signal(barrier, inc=1, device_id={"tp": mate}, device_id_type=MESH)
    for step in (1, -1):
        @pl.when((x + step >= 0) & (x + step < xs))
        def _():
            for c in range(CORES):
                pl.semaphore_signal(barrier, inc=1, device_id={"tp": jnp.clip(x + step, 0, xs - 1) * CORES + c},
                                    device_id_type=MESH)

    pltpu.make_async_copy(wgt, wgt_v, i_s.at[6]).start()
    load_hidden(0)
    pltpu.make_async_copy(key, k_v, i_s.at[7]).start()
    load(1, own - 1)
    for u in range(1, own):
        load_hidden(u)

    def remote(src, dst, ss, rs, **where):
        return pltpu.make_async_remote_copy(src_ref=src, dst_ref=dst, send_sem=ss, recv_sem=rs,
                                            device_id=where, device_id_type=MESH)

    def w_copy(to, phase):
        return remote(wgt_v.at[pl.ds(pl.multiple_of(to * feat, feat), feat), :], w_in.at[tpi],
                      w_ss.at[0], w_rs.at[phase], tp=to)

    def w_near():
        w_copy(mate, 0).start()
        for step in (1, -1):
            @pl.when((x + step >= 0) & (x + step < xs))
            def _():
                for c in range(CORES):
                    w_copy(jnp.clip(x + step, 0, xs - 1) * CORES + c, 0).start()

    def w_across():
        for many in range(2):
            @pl.when(inside if many else jnp.logical_not(inside))
            def _():
                take(w_in.at[pl.ds(0, 1 + CORES * (1 + many))], w_rs.at[0])
        for c in range(CORES):
            w_copy(lax.rem(x + 2, xs) * CORES + c, 1).start()

    def w_ends():
        take(w_in.at[pl.ds(0, CORES)], w_rs.at[1])

        @pl.when(jnp.logical_not(inside))
        def _():
            for c in range(CORES):
                w_copy((xs - 1 - x) * CORES + c, 2).start()

    def a_copy(kind, r, u):
        return remote(a_out.at[kind, u, r - 1], a_in.at[kind, u, r], x_ss.at[0], a_rs.at[kind, u],
                      sp=z * inner + owner(r))

    def e_copy(r):
        return remote(e_out.at[owner(r)], e_in.at[r], e_ss.at[0], e_rs.at[0], sp=z * inner + owner(r))

    def b_part(ref, kind):
        return ref if kind == GRAD else ref.at[pl.ds(0, fold)]

    def b_copy(kind, r, u):
        way = jnp.where(z + r < outer, 0, 1)
        return remote(b_part(b_out.at[kind, u, way], kind), b_part(b_in.at[kind, u, r - 1], kind),
                      b_ss.at[kind], b_rs.at[kind, u], sp=lax.rem(z + r, outer) * inner + y)

    def c_copy(kind, r, u):
        return remote(c_out.at[kind, u, r], c_in.at[kind, u, r - 1], x_ss.at[0], c_rs.at[kind, u],
                      sp=z * inner + lax.rem(y - r + inner, inner))

    def d_copies(r, u, count):
        at = rows(r, u, count)
        for k in FAR_FIRST:
            remote(d_all.at[tpi, at], d_all.at[tpi, at], f_ss.at[0], d_rs.at[u],
                   tp=lax.rem(x + k, xs) * CORES + core).start()
        remote(d_all.at[tpi, at], d_all.at[tpi, at], f_ss.at[0], f_rs.at[u], tp=mate).start()

    def forward(u):
        at = rows(0, u, inner)
        take(d_all.at[pl.ds(0, xs - 1), at], d_rs.at[u])
        for k in range(1, xs):
            mine = d_all.at[lax.rem(x - k + xs, xs) * CORES + core, at]
            remote(mine, mine, f_ss.at[0], f_rs.at[u], tp=mate).start()

    def g_copy(dz, dy):
        to = away(dz, dy)
        return remote(g_out.at[to], g_in.at[dz * inner + dy - 1], g_ss.at[0], g_rs.at[0], sp=to)

    row = lax.broadcasted_iota(jnp.int32, (length, length), 0)
    col = lax.broadcasted_iota(jnp.int32, (length, length), 1)
    lower, upper = row >= col, row <= col

    def matrix(first, second):
        both = jnp.concatenate([jnp.where(first, 1.0, 0.0), jnp.where(second, 1.0, 0.0)], 0)
        return jnp.concatenate([both, both], 1).astype(BF16)

    sums, strict = matrix(lower, upper), matrix(row > col, row < col)
    left = lax.broadcasted_iota(jnp.int32, (length, pack), 1) < dk
    left_fold = lax.broadcasted_iota(jnp.int32, (fold, pack), 1) < dk
    tail_row = lax.broadcasted_iota(jnp.int32, (TAIL, pack), 0)
    left_tall = lax.broadcasted_iota(jnp.int32, (dv, pack), 1) < dk

    def directed(tri, blocks):
        made = []
        for i in range(0, len(blocks), 2):
            pair = blocks[i:i + 2]
            out = dot(tri, halves(jnp.concatenate(pair, 1) if len(pair) > 1 else pair[0]))
            for n in range(len(pair)):
                part = out[:, n * pack:(n + 1) * pack]
                made.append(jnp.where(left, part[:length], part[length:]))
        return made

    def twice(ref, r, u):
        v = ref[owner(r), u].astype(F32)
        return jnp.concatenate([v, v], 1)

    def ends(c):
        return jnp.where(left[:1], c[length - 1:length], c[0:1])

    def decays(todo):
        blocks = [jnp.concatenate([decay_v[0, owner(r), u], decay_v[1, owner(r), u]], 1) for r, u in todo]
        made = directed(sums, blocks)
        for (r, u), c in zip(todo, made):
            cum[slot(r, u)] = c
        for (r, u), c in zip(todo, made):
            e_out[owner(r), pl.ds(u, 1), :] = ends(c)

    def grads(todo):
        hats = [(twice(q_v, r, u) * jnp.exp(cum[slot(r, u)])).astype(BF16) for r, u in todo]
        made = [dot(cot_v[owner(r), u], hat, 0, 0).astype(BF16) for (r, u), hat in zip(todo, hats)]
        return hats, made

    def states(todo):
        keys = []
        for r, u in todo:
            c = cum[slot(r, u)]
            keys.append((twice(k_v, r, u) * jnp.exp(ends(c) - c)).astype(BF16))
        made = [dot(val[rows(r, u)], k_end, 0, 0).astype(BF16) for (r, u), k_end in zip(todo, keys)]
        return keys, made

    def place(kind, r, u, value):
        if r == 0:
            a_in[kind, u, 0] = value
        else:
            a_out[kind, u, r - 1] = value

    def emit(kind, todo):
        kept, made = (grads if kind == 0 else states)(todo)
        keep = q_hats if kind == 0 else k_ends
        for (r, u), value, block in zip(todo, kept, made):
            keep[slot(r, u)] = value
            place(kind, r, u, block)

    def values(u):
        at = rows(0, u, inner)
        val[at] = dot(hid_v[at], wgt_v[...]).astype(BF16)

    everyone, visitors = tuple(range(inner)), tuple(range(1, inner))

    def send(kind, u):
        for r in FAR_FIRST:
            a_copy(kind, r, u).start()

    loaded(0, 1)
    decays([(r, 0) for r in everyone])
    emit(GRAD, [(r, 0) for r in visitors])
    pl.semaphore_wait(barrier, inner + outer - 1 + jnp.where(inside, 2 * CORES, CORES))
    send(GRAD, 0)
    loaded(1, own - 1)
    decays([(r, u) for u in range(1, own) for r in everyone])
    for r in FAR_FIRST:
        e_copy(r).start()
    e_in[0] = e_out[y]
    for u in range(1, own):
        emit(GRAD, [(r, u) for r in visitors])
        send(GRAD, u)

    end = own - 1
    take(wgt_v, i_s.at[6])
    w_near()
    take(k_v, i_s.at[7])
    for u in range(own):
        take(hid_v.at[rows(0, u, inner)], h_s.at[u])
        values(u)
        emit(STATE, [(r, u) for r in visitors])
        if u < end:
            send(STATE, u)

    w_in[tpi] = wgt_v[pl.ds(pl.multiple_of(tpi * feat, feat), feat), :]
    mine = [(0, u) for u in range(own)]
    emit(GRAD, mine)
    emit(STATE, mine)
    w_acc[...] = jnp.zeros((dv, width), F32)
    w_across()

    def offset(person):
        return lax.rem(y - person + inner, inner)

    def endings(u):
        return [e_in[offset(person), pl.ds(u, 1), :] for person in everyone]

    def pick(kind, ahead, behind):
        at = left_tall if ahead.shape[0] == dv else left[:1]
        return jnp.where(at, ahead, behind) if kind == STATE else jnp.where(at, behind, ahead)

    def turn(v):
        return pltpu.roll(v, dk, 1)

    def folded(v, first):
        if first:
            return jnp.where(left_fold, v[:fold], turn(v[fold:]))
        return jnp.where(left_fold, turn(v[:fold]), v[fold:])

    def unfolded(first, second):
        return jnp.concatenate([jnp.where(left_fold, first, turn(second)),
                                jnp.where(left_fold, turn(first), second)], 0)

    def running(blocks, factors, order):
        total, before = None, [None] * inner
        for person in order:
            before[person] = jnp.zeros((dv, pack), F32) if total is None else total
            total = blocks[person] if total is None else factors[person] * total + blocks[person]
        return before, total

    def combine_plane(kind, u):
        take(a_in.at[kind, u, pl.ds(1, inner - 1)], a_rs.at[kind, u])
        blocks = [a_in[kind, u, offset(person)].astype(F32) for person in everyone]
        ends_ = endings(u)
        factors = [jnp.exp(e) for e in ends_]
        before, total = running(blocks, factors, everyone)
        after, total_back = running(blocks, factors, everyone[::-1])
        for person in everyone:
            local[kind, u, person] = pick(kind, before[person], after[person])
        b_out[kind, u, 0, pl.ds(0, fold)] = folded(total, kind == STATE).astype(BF16)
        b_out[kind, u, 1, pl.ds(0, fold)] = folded(total_back, kind == GRAD).astype(BF16)
        if kind == GRAD:
            whole = sum(ends_[1:], ends_[0])
            high = whole.astype(BF16).astype(F32)
            tail = jnp.where(tail_row == 0, high, jnp.where(tail_row == 1, whole - high, 0.0)).astype(BF16)
            for way in range(2):
                b_out[kind, u, way, pl.ds(fold, TAIL)] = tail
        for r in FAR_FIRST:
            b_copy(kind, r, u).start()

    def combine_all(kind, u):
        take(b_in.at[GRAD, u] if kind == GRAD else b_in.at[STATE, u, :, pl.ds(0, fold)], b_rs.at[kind, u])
        planes = [None]
        for r in range(1, outer):
            tail = b_in[GRAD, u, r - 1, pl.ds(fold, TAIL)].astype(F32)
            planes.append(tail[0:1] + tail[1:2])
        zero = jnp.zeros((1, pack), F32)
        ahead, behind = jnp.zeros((fold, pack), F32), jnp.zeros((fold, pack), F32)
        for r in range(1, outer):
            block = b_in[kind, u, r - 1, pl.ds(0, fold)].astype(F32)
            passed, back = sum(planes[1:r], zero), sum(planes[r + 1:], zero)
            first = jnp.where(left[:1], passed, turn(passed)) if kind == STATE else jnp.where(left[:1], turn(passed), passed)
            second = jnp.where(left[:1], back, turn(back)) if kind == GRAD else jnp.where(left[:1], turn(back), back)
            ahead = ahead + jnp.where(z >= r, jnp.exp(first), 0.0) * block
            behind = behind + jnp.where(z + outer - r < outer, jnp.exp(second), 0.0) * block
        carried = unfolded(ahead, behind) if kind == STATE else unfolded(behind, ahead)
        ends_ = endings(u)
        for person in everyone:
            factor = jnp.exp(pick(kind, sum(ends_[:person], zero), sum(ends_[person + 1:], zero)))
            c_out[kind, u, offset(person)] = (factor * carried + local[kind, u, person]).astype(BF16)
        for r in FAR_FIRST:
            c_copy(kind, r, u).start()

    def intra(todo):
        made = []
        for r, u in todo:
            s = slot(r, u)
            q_hat = q_hats[s]
            k_hat = (twice(k_v, r, u) * jnp.exp(-cum[s])).astype(BF16)
            v, seed = val[rows(r, u)], cot_v[owner(r), u]
            seed_scores = dot(seed, v, 1, 1)
            zero = jnp.zeros_like(q_hat)
            q_left, q_right = jnp.where(left, q_hat, zero), jnp.where(left, zero, q_hat)
            k_left, k_right = jnp.where(left, k_hat, zero), jnp.where(left, zero, k_hat)
            score = (jnp.where(lower, dot(q_left, k_hat, 1, 1), 0.0)
                     + jnp.where(upper, dot(q_right, k_hat, 1, 1), 0.0)).astype(BF16)
            seed_low = jnp.where(lower, seed_scores, 0.0).astype(BF16)
            seed_up = jnp.where(upper, seed_scores, 0.0).astype(BF16)
            made.append((dot(seed_low, k_left) + dot(seed_up, k_right),
                         dot(seed_low, q_left, 0, 0) + dot(seed_up, q_right, 0, 0),
                         dot(score, seed, 0, 0)))
        for (r, u), (for_q, for_k, for_v) in zip(todo, made):
            intra_q[slot(r, u)] = for_q
            intra_k[slot(r, u)] = for_k
            intra_v[slot(r, u)] = for_v

    def arrived(kind, r, u):
        return c_out[kind, u, 0] if r == 0 else c_in[kind, u, r - 1]

    def finish_values(todo):
        made = [intra_v[slot(r, u)] + dot(k_ends[slot(r, u)], arrived(GRAD, r, u), 1, 1) for r, u in todo]
        for (r, u), block in zip(todo, made):
            d_all[tpi, rows(r, u)] = block.astype(BF16)

    def finish_rest(todo):
        kept, terms = [], []
        for r, u in todo:
            s = slot(r, u)
            state, grad = arrived(STATE, r, u), arrived(GRAD, r, u)
            c = cum[s]
            end = ends(c)
            grow, shrink, to_end = jnp.exp(c), jnp.exp(-c), jnp.exp(end - c)
            q, k = twice(q_v, r, u), twice(k_v, r, u)
            cross = dot(cot_v[owner(r), u], state)
            dq = grow * (intra_q[s] + cross)
            dk_ = shrink * intra_k[s] + to_end * dot(val[rows(r, u)], grad)
            terms.append(q * dq - k * dk_)
            start = (jnp.sum(q * grow * cross, axis=0, keepdims=True)
                     + jnp.exp(end) * jnp.sum(state.astype(F32) * grad.astype(F32), axis=0, keepdims=True))
            kept.append((dq, dk_, start))
        for (r, u), (dq, dk_, start), sums_ in zip(todo, kept, directed(strict, terms)):
            b = batch_of(r, u)
            decay_grad = start - sums_
            o_q[b] = (dq[:, :dk] + dq[:, dk:]).astype(BF16)
            o_k[b] = (dk_[:, :dk] + dk_[:, dk:]).astype(BF16)
            o_f[b] = decay_grad[:, :dk]
            o_b[b] = decay_grad[:, dk:]

    def features(u):
        take(d_all.at[pl.ds(0, xs), rows(0, u, inner)], f_rs.at[u])
        at = rows(0, u, inner)
        wide = jnp.concatenate([d_all[t, at] for t in range(tp)], 1)
        weights = jnp.concatenate([w_in[t] for t in range(tp)], 1)
        out = dot(wide, weights, 1, 1).astype(BF16)
        for r in range(inner):
            o_h[batch_of(r, u)] = out[r * length:(r + 1) * length]

    def prepare_rest(todo):
        made = []
        for r, u in todo:
            b, at = batch_of(r, u), slot(r, u)
            c = cum[at]
            q, k = twice(q_v, r, u), twice(k_v, r, u)
            dk_ = (jnp.exp(-c) * intra_k[at]
                   + jnp.exp(ends(c) - c) * dot(val[rows(r, u)], arrived(GRAD, r, u)))
            o_k[b] = (dk_[:, :dk] + dk_[:, dk:]).astype(BF16)
            made.append(q * jnp.exp(c) * intra_q[at] - k * dk_)
        for (r, u), known in zip(todo, made):
            intra_k[slot(r, u)] = known

    def close_rest(todo):
        kept, terms = [], []
        for r, u in todo:
            at = slot(r, u)
            state, grad = arrived(STATE, r, u), arrived(GRAD, r, u)
            c = cum[at]
            grow = jnp.exp(c)
            cross = dot(cot_v[owner(r), u], state)
            far = twice(q_v, r, u) * grow * cross
            terms.append(intra_k[at] + far)
            start = (jnp.sum(far, axis=0, keepdims=True)
                     + jnp.exp(ends(c)) * jnp.sum(state.astype(F32) * grad.astype(F32), axis=0, keepdims=True))
            kept.append((grow * (intra_q[at] + cross), start))
        for (r, u), (dq, start), sums_ in zip(todo, kept, directed(strict, terms)):
            b = batch_of(r, u)
            decay_grad = start - sums_
            o_q[b] = (dq[:, :dk] + dq[:, dk:]).astype(BF16)
            o_f[b] = decay_grad[:, :dk]
            o_b[b] = decay_grad[:, dk:]

    def finish_own(u):
        finish_values([(0, u)])
        d_copies(0, u, 1)

    def finish_others(u):
        take(c_in.at[GRAD, u], c_rs.at[GRAD, u])
        finish_values([(r, u) for r in visitors])
        d_copies(1, u, inner - 1)

    def weight_terms(u):
        at = rows(0, u, inner)
        return dot(d_all[tpi, at], hid_v[at], 0, 0)

    def rest_others(u):
        take(c_in.at[STATE, u], c_rs.at[STATE, u])
        finish_rest([(r, u) for r in visitors])

    def loop(first, last, step):
        lax.fori_loop(first, last, lambda u, _: step(u) or 0, 0)

    def intra_all(u):
        intra([(r, u) for r in everyone])

    def first_steps(u):
        combine_plane(GRAD, u)
        intra_all(u)

    def second_steps(u):
        combine_all(GRAD, u)
        combine_plane(STATE, u - 1)
        finish_own(u)

    def weigh(u):
        finish_others(u)
        w_acc[...] += weight_terms(u)

    def pass_states(u):
        combine_all(STATE, u)
        finish_rest([(0, u)])

    def third_steps(u):
        weigh(u)
        pass_states(u)

    def fourth_steps(u):
        forward(u)
        rest_others(u)

    take(e_in.at[pl.ds(1, inner - 1)], e_rs.at[0])
    loop(0, end, first_steps)
    combine_plane(GRAD, end)
    combine_all(GRAD, 0)
    w_ends()
    finish_own(0)
    intra_all(end)
    loop(1, own, second_steps)
    send(STATE, end)
    loop(0, end - 1, third_steps)
    weigh(end - 1)

    finish_others(end)
    full = w_acc[...] + weight_terms(end)
    for p in range(0, sp, 2):
        block = full[:, p * rows_sp:(p + 2) * rows_sp].T.astype(BF16)
        g_out[p] = block[:rows_sp]
        g_out[p + 1] = block[rows_sp:]
    pass_states(end - 1)
    combine_plane(STATE, end)
    for away_by in OFFSETS:
        g_copy(*away_by).start()
    loop(0, end - 1, rest_others)
    combine_all(STATE, end)
    prepare_rest([(r, end) for r in visitors])
    loop(0, end, forward)
    finish_rest([(0, end)])
    forward(end)
    rest_others(end - 1)

    @pl.when(jnp.logical_not(inside))
    def _():
        take(w_in.at[pl.ds(0, CORES)], w_rs.at[2])

    loop(0, own, features)
    take(c_in.at[STATE, end], c_rs.at[STATE, end])
    close_rest([(r, end) for r in visitors])

    take(g_in, g_rs.at[0])
    acc = g_out[spi].astype(F32)
    for r in range(sp - 1):
        acc = acc + g_in[r].astype(F32)
    o_w[...] = acc

    take(w_in.at[pl.ds(0, tp - 1)], w_ss.at[0])
    take(e_in.at[pl.ds(1, inner - 1)], e_ss.at[0])
    take(d_all.at[pl.ds(0, tp - 2)], x_ss.at[0])
    take(b_in.at[GRAD], b_ss.at[GRAD])
    take(b_in.at[STATE, :, :, pl.ds(0, fold)], b_ss.at[STATE])
    take(d_all.at[pl.ds(0, tp - 1)], f_ss.at[0])
    take(g_in, g_ss.at[0])


def store_kernel(*refs):
    n = len(refs) // 2
    copies = [pltpu.make_async_copy(refs[i], refs[n + i], refs[-1].at[i]) for i in range(n)]
    for copy in copies:
        copy.start()
    for copy in copies:
        copy.wait()


def store(arrays):
    n = len(arrays)
    return pl.pallas_call(
        store_kernel,
        out_shape=tuple(jax.ShapeDtypeStruct(a.shape, a.dtype) for a in arrays),
        in_specs=[pl.BlockSpec(memory_space=pltpu.VMEM)] * n,
        out_specs=(pl.BlockSpec(memory_space=pl.ANY),) * n,
        scratch_shapes=[pltpu.SemaphoreType.DMA((n,))],
        compiler_params=pltpu.CompilerParams(has_side_effects=True, vmem_limit_bytes=1024 * 1024),
    )(*arrays)


def shards(sp, tp, hidden, value_weight, queries, key_vectors, forward_decay, backward_decay, cotangent):
    batch, length, width = hidden.shape
    heads, dk = queries.shape[1], queries.shape[3]
    dv = value_weight.shape[1]
    assert heads == 1
    inner, outer, own, xs = INNER, sp // INNER, batch // INNER, tp // CORES
    pack, rows, feat, rows_sp = 2 * dk, batch * length, width // tp, width // sp
    dims = (sp, tp, batch, length, dk, dv, width)
    vmem, dma = pltpu.VMEM, pltpu.SemaphoreType.DMA
    scratch = [
        vmem((rows, width), BF16), vmem((width, dv), BF16),
        vmem((inner, own, length, dk), BF16), vmem((inner, own, length, dk), BF16),
        vmem((2, inner, own, length, dk), F32), vmem((inner, own, length, dv), BF16),
        vmem((rows, dv), BF16),
        vmem((batch, length, pack), F32),
        vmem((batch, length, pack), BF16), vmem((batch, length, pack), BF16),
        vmem((batch, length, pack), F32), vmem((batch, length, pack), F32),
        vmem((batch, length, dv), F32),
        vmem((2, own, inner - 1, dv, pack), BF16), vmem((2, own, inner, dv, pack), BF16),
        vmem((inner, own, pack), F32), vmem((inner, own, pack), F32),
        vmem((2, own, inner, dv, pack), F32),
        vmem((2, own, 2, dv // 2 + TAIL, pack), BF16), vmem((2, own, outer - 1, dv // 2 + TAIL, pack), BF16),
        vmem((2, own, inner, dv, pack), BF16), vmem((2, own, inner - 1, dv, pack), BF16),
        vmem((tp, rows, dv), BF16), vmem((tp, feat, dv), BF16),
        vmem((dv, width), F32),
        vmem((sp, rows_sp, dv), BF16), vmem((sp - 1, rows_sp, dv), BF16),
        dma((8,)), dma((own,)),
        dma((1,)), dma((2, own)),
        dma((1,)), dma((1,)),
        dma((2,)), dma((2, own)),
        dma((2, own)),
        dma((own,)),
        dma((1,)), dma((own,)),
        dma((1,)), dma((3,)),
        dma((1,)), dma((1,)),
    ]
    whole = pl.BlockSpec(memory_space=vmem)
    flat, split = (batch, length, dk), (inner, own, length, dk)
    args = (hidden.reshape(inner, own, length, width), value_weight, queries.reshape(split),
            key_vectors.reshape(split), forward_decay.reshape(split), backward_decay.reshape(split),
            cotangent.reshape(inner, own, length, dv))
    outs = pl.pallas_call(
        functools.partial(kernel, dims),
        out_shape=(
            vmem(flat, BF16), vmem(flat, BF16), vmem(flat, F32), vmem(flat, F32),
            vmem((batch, length, feat), BF16), vmem((rows_sp, dv), F32),
        ),
        in_specs=[pl.BlockSpec(memory_space=pltpu.HBM)] * 7,
        out_specs=(whole,) * 6,
        scratch_shapes=scratch,
        compiler_params=pltpu.CompilerParams(
            collective_id=0, has_side_effects=True, vmem_limit_bytes=48 * 1024 * 1024
        ),
    )(*(pltpu.with_memory_space_constraint(a, pltpu.HBM) for a in args))
    outs = store(outs)
    return tuple(a.reshape(queries.shape) for a in outs[:4]) + tuple(outs[4:])


def solution(mesh):
    heads = P(None, "tp", "sp", None)
    return jax.shard_map(
        functools.partial(shards, mesh.shape["sp"], mesh.shape["tp"]),
        mesh=mesh,
        in_specs=(P(None, "sp", None), P(None, "tp"), heads, heads, heads, heads, P(None, "sp", "tp")),
        out_specs=(heads, heads, heads, heads, P(None, "sp", "tp"), P("sp", "tp")),
        check_vma=False,
    )
```
